32 devices in a mesh: grp: 1, sp: 16 (over z, y, core), tp: 2 (over x).
Axes of the slice: x: 2, y: 2, z: 4, core: 2. Of those that a mesh axis runs over, the one named last changes fastest.
Arguments:
- residual_in: bfloat16 [2048, 2048], P(('grp', 'sp'), 'tp'), may hold values from -16 to 16
- query_pre: bfloat16 [2048, 512], P(('grp', 'sp'), 'tp'), may hold values from -6 to 6
- forget_pre: bfloat16 [2048, 512], P(('grp', 'sp'), 'tp'), may hold values from -9 to 9
- value_pre: bfloat16 [2048, 512], P(('grp', 'sp'), 'tp'), may hold values from -6 to 6
- gate_pre: bfloat16 [2048, 512], P(('grp', 'sp'), 'tp'), may hold values from -6 to 6
- floor_gap: float32 [512], P('tp'), may hold values from 0 to 1, as said below
- head_gain: float32 [64], replicated, may hold values from 0.1 to 1.9
- out_weight: bfloat16 [512, 2048], P(None, 'tp'), may hold values from -0.25 to 0.25
- norm_gain: float32 [2048], P('tp'), may hold values from 0.1 to 1.9
- value_weight: bfloat16 [2048, 5632], P('sp', 'tp'), may hold values from -0.125 to 0.125
- gate_weight: bfloat16 [2048, 5632], P('sp', 'tp'), may hold values from -0.125 to 0.125
- value_taps: float32 [3, 5632], P(None, 'tp'), may hold values from -3 to 3
- gate_taps: float32 [3, 5632], P(None, 'tp'), may hold values from -3 to 3
- down_weight: bfloat16 [5632, 2048], P('tp', 'sp'), may hold values from -0.078125 to 0.078125
Outputs:
- mixed: bfloat16 [2048, 2048], P(('grp', 'sp'), 'tp')
The draws below stay inside these ranges and needn't reach their ends.
Inputs may be any that keep to these rules, and one draw needn't show every extreme that they name: `floor_gap`: each channel's value lies strictly between 0 and 1.
All inputs are finite; a program needn't handle non-finite values.
Results may differ from the reference program's by a relative error of at most 0.0085.
Values may be sent and summed in bfloat16 or wider, within the bound.
A program may use at most 128 MiB of HBM per device.

```python
import jax
import jax.numpy as jnp
from jax import lax

D = 2048
H = 8
DK = 64
DV = 64
FF = 5632
TAPS = 3
BLOCK = 64
TOK_DEV = 128
TOKENS = 2048


def draw_residual_in(key, part):
    noise_key, order_key = jax.random.split(jax.random.fold_in(key, 11))
    base = jax.random.normal(noise_key, (TOKENS, D), jnp.float32)
    ranking = jax.random.permutation(order_key, 4).astype(jnp.float32)
    scales = 0.35 * 6.0 ** (ranking / 3.0)
    return (base.reshape(TOKENS, 4, D // 4) * scales[None, :, None]).reshape(TOKENS, D).astype(jnp.bfloat16)


def draw_forget_pre(key, part):
    noise_key, offset_key = jax.random.split(jax.random.fold_in(key, 17))
    base = jnp.clip(jax.random.normal(noise_key, (TOKENS, H * DK), jnp.float32), -6.0, 6.0)
    offsets = jax.random.uniform(offset_key, (TOKENS // TOK_DEV, 1, H * DK), jnp.float32, -1.5, 1.5)
    return (base.reshape(TOKENS // TOK_DEV, TOK_DEV, H * DK) + offsets).reshape(TOKENS, H * DK).astype(jnp.bfloat16)


def draw_floor_gap(key, part):
    order_key, slow_key, fast_key = jax.random.split(jax.random.fold_in(key, 23), 3)
    ranking = jax.random.permutation(order_key, H)
    quick = ranking < H // 2
    slow_values = jnp.exp(jax.random.uniform(slow_key, (H, DK), jnp.float32, jnp.log(0.3 / TOKENS), jnp.log(2.5 / TOKENS)))
    fast_values = jnp.exp(jax.random.uniform(fast_key, (H, DK), jnp.float32, jnp.log(0.02), jnp.log(0.06)))
    return jnp.where(quick[:, None], fast_values, slow_values).reshape(H * DK)


def shard_levels(rng, dims, cuts, least, largest):
    gain, own = 1.0, jax.random.fold_in(rng, 6)
    for dim, blocks in cuts:
        heights = jnp.exp(jax.random.uniform(jax.random.fold_in(own, dim), (blocks,), jnp.float32, least / len(cuts), largest / len(cuts)))
        gain = gain * jnp.repeat(heights, dims[dim] // blocks).reshape([-1 if axis == dim else 1 for axis in range(len(dims))])
    return gain


def centred(rng, extent, scale, reach, shards=(), kind=jnp.bfloat16):
    factor_of = shard_levels(rng, extent, shards, -0.22, 0.18) if shards else 1.0
    values = jax.random.normal(rng, extent, jnp.float32) * scale * factor_of
    return jnp.minimum(jnp.maximum(values, -reach), reach).astype(kind)


def setup_inputs(seed: int = 0, part: int = 0) -> dict:
    streams_of = jax.random.split(jax.random.key(seed), 15)
    part_keys = jax.random.split(jax.random.fold_in(streams_of[14], part), 15)
    return {
        "residual_in": draw_residual_in(jax.random.fold_in(jax.random.fold_in(streams_of[14], part), 71), part),
        "query_pre": centred(part_keys[1], (TOKENS, H * DK), 1.0, 6.0, ((0, 16), (1, 2))),
        "forget_pre": draw_forget_pre(jax.random.fold_in(jax.random.fold_in(streams_of[14], part), 71), part),
        "value_pre": centred(part_keys[3], (TOKENS, H * DV), 1.0, 6.0, ((0, 16), (1, 2))),
        "gate_pre": centred(part_keys[4], (TOKENS, H * DV), 1.0, 6.0, ((0, 16), (1, 2))),
        "floor_gap": draw_floor_gap(jax.random.fold_in(streams_of[14], 71), part),
        "head_gain": jnp.clip(1.0 + 0.18 * jax.random.normal(streams_of[6], (DV,), jnp.float32), 0.1, 1.9),
        "out_weight": centred(streams_of[7], (H * DV, D), (H * DV) ** -0.5, 0.25, ((1, 2),)),
        "norm_gain": jnp.clip(1.0 + 0.18 * jax.random.normal(streams_of[8], (D,), jnp.float32), 0.1, 1.9),
        "value_weight": centred(streams_of[9], (D, FF), D ** -0.5, 0.125, ((0, 16), (1, 2))),
        "gate_weight": centred(streams_of[10], (D, FF), D ** -0.5, 0.125, ((0, 16), (1, 2))),
        "value_taps": centred(streams_of[11], (TAPS, FF), 0.577, 3.0, ((1, 2),), jnp.float32),
        "gate_taps": centred(streams_of[12], (TAPS, FF), 0.577, 3.0, ((1, 2),), jnp.float32),
        "down_weight": centred(streams_of[13], (FF, D), FF ** -0.5, 0.078125, ((0, 2), (1, 16))),
    }


epsilon = 1e-06
highest_precision = lax.Precision.HIGHEST

def split_heads(matrix, head_count):
    return matrix.reshape(matrix.shape[0], head_count, -1).transpose(1, 0, 2)

def recurrence(query_rows, gate_keys, values, log_decay, block_size, start_state):
    head_count, seq_length, key_width = query_rows.shape
    block_count = seq_length // block_size

    def to_blocks(tensor):
        return tensor.reshape(head_count, block_count, block_size, tensor.shape[-1]).transpose(1, 0, 2, 3)
    causal = jnp.tril(jnp.ones((block_size, block_size), dtype=bool))

    def advance(current_state, inputs):
        block_queries, block_keys, block_values, decay_block = inputs
        running_state = jnp.cumsum(decay_block, axis=1)
        carried_state = jnp.einsum('pen,pnd->ped', block_queries * jnp.exp(running_state), current_state, precision=highest_precision)
        spread = jnp.where(causal[None, :, :, None], running_state[:, :, None, :] - running_state[:, None, :, :], -jnp.inf)
        scores = jnp.einsum('htk,hsk,htsk->hts', block_queries, block_keys, jnp.exp(spread), precision=highest_precision)
        inner = jnp.einsum('hts,hsv->htv', scores, block_values, precision=highest_precision)
        ending_state = running_state[:, -1, :]
        fresh_update = jnp.einsum('bia,big->bag', block_keys * jnp.exp(ending_state[:, None, :] - running_state), block_values, precision=highest_precision)
        return (jnp.exp(ending_state)[:, :, None] * current_state + fresh_update, carried_state + inner)
    final_state, outputs = lax.scan(advance, start_state, (to_blocks(query_rows), to_blocks(gate_keys), to_blocks(values), to_blocks(log_decay)))
    return (final_state, outputs.transpose(1, 0, 2, 3).reshape(head_count, seq_length, values.shape[-1]))

def mixer_inputs(query_pre, forget_pre, value_pre, floor_gap, head_count):
    gate_keys = floor_gap.astype(jnp.float32) * jax.nn.sigmoid(-forget_pre.astype(jnp.float32))
    log_decay = jnp.log1p(-gate_keys)
    query_rows = jax.nn.silu(query_pre.astype(jnp.float32))
    return (split_heads(query_rows, head_count), split_heads(gate_keys, head_count), split_heads(value_pre.astype(jnp.float32), head_count), split_heads(log_decay, head_count))

def head_output(recurrent, head_gain, gate_pre):
    ordered = recurrent.transpose(1, 0, 2)
    scaled = ordered * lax.rsqrt(lax.optimization_barrier(jnp.mean(ordered * ordered, axis=-1, keepdims=True)) + epsilon) * head_gain
    gating = jax.nn.silu(gate_pre.astype(jnp.float32)).reshape(ordered.shape)
    return (scaled * gating).reshape(ordered.shape[0], -1).astype(jnp.bfloat16)

def causal_taps(padded, taps, row_count):
    return taps[0] * padded[0:row_count] + taps[1] * padded[1:row_count + 1] + taps[2] * padded[2:row_count + 2]

def reference(residual_in, query_pre, forget_pre, value_pre, gate_pre, floor_gap, head_gain, out_weight, norm_gain, value_weight, gate_weight, value_taps, gate_taps, down_weight):
    row_count = residual_in.shape[0]
    query_rows, gate_keys, values, log_decay = mixer_inputs(query_pre, forget_pre, value_pre, floor_gap, H)
    start_state = jnp.zeros((H, DK, DV), jnp.float32)
    final_state, recurrent = recurrence(query_rows, gate_keys, values, log_decay, BLOCK, start_state)
    head_out = head_output(recurrent, head_gain, gate_pre)
    stream = residual_in.astype(jnp.float32) + jnp.dot(head_out, out_weight, preferred_element_type=jnp.float32)
    normed = (stream * lax.rsqrt(lax.optimization_barrier(jnp.mean(stream * stream, axis=1, keepdims=True)) + epsilon) * norm_gain).astype(jnp.bfloat16)
    up_value = jnp.dot(normed, value_weight, preferred_element_type=jnp.float32).astype(jnp.bfloat16)
    up_gate = jnp.dot(normed, gate_weight, preferred_element_type=jnp.float32).astype(jnp.bfloat16)
    zero_rows = jnp.zeros((2, up_value.shape[1]), jnp.float32)
    conv_value = causal_taps(jnp.concatenate([zero_rows, up_value.astype(jnp.float32)], axis=0), value_taps, row_count)
    conv_gate = causal_taps(jnp.concatenate([zero_rows, up_gate.astype(jnp.float32)], axis=0), gate_taps, row_count)
    hidden = (jax.nn.silu(conv_gate) * conv_value).astype(jnp.bfloat16)
    return (stream + jnp.dot(hidden, down_weight, preferred_element_type=jnp.float32)).astype(jnp.bfloat16)
```

```python
import functools

import jax
import jax.numpy as jnp
from jax import lax
from jax.experimental import pallas as pl
from jax.experimental.pallas import tpu as pltpu
from jax.sharding import PartitionSpec as P

DK = 64
SUB = 16
LANES = 128
INNER = 4
OUTER = 4
epsilon = 1e-06
highest = lax.Precision.HIGHEST
f32 = jnp.float32
bf16 = jnp.bfloat16
MESH = pl.DeviceIdType.MESH


def dot_nt(a, b):
    return lax.dot_general(
        a, b, (((1,), (1,)), ((), ())), precision=highest, preferred_element_type=f32
    )


def dot_hi(a, b):
    return jnp.dot(a, b, precision=highest, preferred_element_type=f32)


def layer_kernel(
    full,
    extra,
    up_in,
    dn_in,
    keys_ref,
    logd_ref,
    query_ref,
    values_ref,
    gating_ref,
    head_gain_ref,
    residual_ref,
    out_weight_ref,
    norm_gain_ref,
    taps_ref,
    out_ref,
    up,
    dn,
    st,
    zt,
    inner_buf,
    start_buf,
    ho,
    sq,
    stream,
    nb,
    ubuf,
    tail_s,
    tail_r,
    hid,
    acc,
    xs,
    xr,
    zs,
    zr,
    ssem,
    up_r,
    dn_r,
    st_r,
    zt_r,
    nb_r,
    xr_r,
    zr_r,
    misc_r,
):
    s = lax.axis_index("sp")
    x = lax.axis_index("tp")
    z = s // INNER
    i = s % INNER
    c = s % 2
    ox = 1 - x
    ic = i + 1 - 2 * c
    iy = (i + 2) % INNER
    idg = (ic + 2) % INNER
    z1 = z + 1 - 2 * (z % 2)
    z2 = (z + 2) % OUTER
    z3 = OUTER - 1 - z
    chunk = full + extra
    rows = keys_ref.shape[0]
    width = keys_ref.shape[1]
    pairs = width // LANES
    pending = []

    def at(zz, ii, xx=x):
        return {"sp": zz * INNER + ii, "tp": xx}

    def send(src, dst, rsem, device):
        copy = pltpu.make_async_remote_copy(
            src_ref=src,
            dst_ref=dst,
            send_sem=ssem.at[len(pending)],
            recv_sem=rsem,
            device_id=device,
            device_id_type=MESH,
        )
        copy.start()
        pending.append(copy)

    def arrived(dst, rsem):
        pltpu.make_async_remote_copy(
            src_ref=dst,
            dst_ref=dst,
            send_sem=ssem.at[0],
            recv_sem=rsem,
            device_id=at(z, ic),
            device_id_type=MESH,
        ).wait_recv()

    barrier = pltpu.get_barrier_semaphore()
    peers = [at((z + k) % OUTER, i) for k in range(1, OUTER)]
    peers += [at(z, ic), at(z, iy), at(z, idg), at(z, i, ox)]
    for peer in peers:
        pl.semaphore_signal(barrier, inc=1, device_id=peer, device_id_type=MESH)
    pl.semaphore_wait(barrier, len(peers))

    def up_slot(zz, ii):
        return up.at[zz * INNER + ii], up_r.at[zz * INNER + ii]

    def dn_slot(zz, ii):
        slot = dn.at[zz * INNER + ii, pl.ds(0, chunk)]
        return slot, dn_r.at[zz * INNER + ii]

    def send_z(source, slot, k):
        dst, sem = slot(z, i)
        send(source.at[(z + k) % OUTER], dst, sem, at((z + k) % OUTER, i))

    def forward_yc(slot, zz, source=None):
        dst, sem = slot(zz, i)
        if source is None:
            arrived(dst, sem)
            source = dst
        send(source, dst, sem, at(z, iy))
        send(source, dst, sem, at(z, ic))

    def forward_c(slot, zz):
        dst, sem = slot(zz, iy)
        arrived(dst, sem)
        send(dst, dst, sem, at(z, ic))

    send_z(up_in, up_slot, 2)

    keys = keys_ref[...]
    position = lax.broadcasted_iota(jnp.int32, (rows, rows), 0)
    earlier = lax.broadcasted_iota(jnp.int32, (rows, rows), 1)
    running = dot_hi((position >= earlier).astype(f32), logd_ref[...])
    ending = running[rows - 1 : rows]
    kept = keys * jnp.exp(ending - running)
    turned = values_ref[...].T
    low = lax.broadcasted_iota(jnp.int32, (1, LANES), 1) < DK
    for p in range(pairs):
        lanes = slice(p * LANES, (p + 1) * LANES)
        both = dot_hi(turned[lanes], kept[:, lanes])
        st[i, 0:DK, lanes] = jnp.where(low, both[:DK], both[DK:])
    st[i, DK : DK + 8] = jnp.broadcast_to(jnp.exp(ending), (8, width))
    for ii in (ic, iy, idg):
        send(st.at[i], st.at[i], st_r.at[i], at(z, ii))
    forward_yc(up_slot, z, up_in.at[z])
    forward_yc(dn_slot, z, dn_in.at[z])

    up[s] = up_in[z]
    dn[s, 0:chunk] = dn_in[z]
    spare = dn.shape[1] - chunk
    if spare:
        for b in range(INNER * OUTER):
            dn[b, chunk:] = jnp.zeros((spare, dn.shape[2]), bf16)
    start_buf[...] = query_ref[...] * jnp.exp(running)

    for ii in (ic, iy, idg):
        arrived(st.at[ii], st_r.at[ii])
    total = jnp.zeros((DK, width), f32)
    mine = jnp.zeros((DK, width), f32)
    total_decay = jnp.ones((1, width), f32)
    my_decay = jnp.ones((1, width), f32)
    for j in range(INNER):
        decay = st[j, DK : DK + 1]
        fresh = st[j, 0:DK]
        mine = jnp.where(j < i, mine * decay + fresh, mine)
        my_decay = jnp.where(j < i, my_decay * decay, my_decay)
        total = total * decay + fresh
        total_decay = total_decay * decay
    zt[z, 0:DK] = total
    zt[z, DK : DK + 8] = jnp.broadcast_to(total_decay, (8, width))
    for k in range(1, OUTER):
        send(zt.at[z], zt.at[z], zt_r.at[z], at((z + k) % OUTER, i))
    send_z(up_in, up_slot, 1)
    send_z(up_in, up_slot, 3)

    cells = [[] for _ in range(pairs)]
    row_of = lax.broadcasted_iota(jnp.int32, (rows, width), 0)
    column = lax.broadcasted_iota(jnp.int32, (2 * SUB, rows), 1)
    stacked = lax.broadcasted_iota(jnp.int32, (2 * SUB, rows), 0) % SUB
    for n in range(rows // SUB):
        part = slice(n * SUB, (n + 1) * SUB)
        middle = running[n * SUB + SUB // 2 - 1 : n * SUB + SUB // 2]
        query_part = query_ref[part] * jnp.exp(running[part] - middle)
        reach = jnp.where(row_of < (n + 1) * SUB, middle - running, -jnp.inf)
        key_part = keys * jnp.exp(reach)
        for p in range(pairs):
            lanes = slice(p * LANES, (p + 1) * LANES)
            piece = query_part[:, lanes]
            piece = jnp.concatenate(
                [jnp.where(low, piece, 0.0), jnp.where(low, 0.0, piece)], axis=0
            )
            score = dot_nt(piece, key_part[:, lanes])
            score = jnp.where(stacked + n * SUB >= column, score, 0.0)
            cells[p].append(score)
    for p in range(pairs):
        lanes = slice(p * LANES, (p + 1) * LANES)
        scores = jnp.concatenate(
            [cell[:SUB] for cell in cells[p]] + [cell[SUB:] for cell in cells[p]],
            axis=0,
        )
        result = dot_hi(scores, values_ref[:, lanes])
        inner_buf[:, lanes] = jnp.where(low, result[:rows], result[rows:])

    for k in range(1, OUTER):
        zz = (z + k) % OUTER
        arrived(zt.at[zz], zt_r.at[zz])
    entering = jnp.zeros((DK, width), f32)
    for j in range(OUTER - 1):
        entering = jnp.where(
            j < z, entering * zt[j, DK : DK + 1] + zt[j, 0:DK], entering
        )
    entering = entering * my_decay + mine
    same_head = (
        lax.broadcasted_iota(jnp.int32, (LANES, LANES), 0) // DK
        == lax.broadcasted_iota(jnp.int32, (LANES, LANES), 1) // DK
    ).astype(f32)
    for p in range(pairs):
        lanes = slice(p * LANES, (p + 1) * LANES)
        piece = entering[:, lanes]
        piece = jnp.concatenate(
            [jnp.where(low, piece, 0.0), jnp.where(low, 0.0, piece)], axis=0
        )
        recurrent = inner_buf[:, lanes] + dot_nt(start_buf[:, lanes], piece)
        squares = dot_hi(recurrent * recurrent, same_head) * (1.0 / DK)
        scaled = recurrent * lax.rsqrt(squares + epsilon) * head_gain_ref[:, lanes]
        ho[x, :, lanes] = (scaled * gating_ref[:, lanes]).astype(bf16)
    send(ho.at[x], ho.at[x], misc_r.at[0], at(z, i, ox))

    forward_yc(up_slot, z2)
    forward_c(up_slot, z)

    arrived(ho.at[ox], misc_r.at[0])
    heads = jnp.concatenate([ho[0], ho[1]], axis=1)
    stream[...] = residual_ref[...].astype(f32) + jnp.dot(
        heads, out_weight_ref[...], preferred_element_type=f32
    )
    partial = jnp.sum(stream[...] * stream[...], axis=1, keepdims=True)
    sq[x] = jnp.broadcast_to(partial, (rows, LANES))
    send(sq.at[x], sq.at[x], misc_r.at[1], at(z, i, ox))
    forward_c(dn_slot, z)
    arrived(sq.at[ox], misc_r.at[1])
    channels = 2 * stream.shape[1]
    mean = (sq[0][:, 0:1] + sq[1][:, 0:1]) * (1.0 / channels)
    normed = stream[...] * lax.rsqrt(mean + epsilon) * norm_gain_ref[...]
    nb[z, x] = normed.astype(bf16)

    def nb_slot(zz, xx):
        return nb.at[zz, xx], nb_r.at[zz * 2 + xx]

    def share(zz, devices):
        dst, sem = nb_slot(zz, x)
        for device in devices:
            send(dst, dst, sem, device)

    share(z, [at(z2, i), at(z1, i), at(z, i, ox)])
    for k in (2, 1, 3):
        send_z(dn_in, dn_slot, k)

    forward_yc(up_slot, (z + 1) % OUTER)
    forward_yc(up_slot, (z + 3) % OUTER)
    forward_c(up_slot, z2)
    arrived(*nb_slot(z1, x))
    share(z1, [at(z, i, ox)])
    arrived(*nb_slot(z2, x))
    share(z2, [at(z1, i), at(z, i, ox)])
    forward_yc(dn_slot, z2)
    forward_c(up_slot, (z + 1) % OUTER)
    forward_c(up_slot, (z + 3) % OUTER)
    arrived(*nb_slot(z3, x))
    share(z3, [at(z, i, ox)])

    for zz in range(OUTER):
        arrived(*up_slot(zz, ic))
        arrived(*up_slot(zz, idg))
        arrived(*nb_slot(zz, ox))

    forward_yc(dn_slot, (z + 1) % OUTER)

    count = OUTER * rows
    half = nb.shape[3]
    deep = half // up.shape[1]
    first = nb[:, 0].reshape(count, half)
    second = nb[:, 1].reshape(count, half)
    span = up.shape[2]
    step = 2 * LANES
    for low_lane in range(0, span, step):
        lanes = slice(low_lane, min(span, low_lane + step))
        size = lanes.stop - lanes.start
        product = jnp.dot(
            first, up[0:deep, :, lanes].reshape(half, size), preferred_element_type=f32
        ) + jnp.dot(
            second,
            up[deep : 2 * deep, :, lanes].reshape(half, size),
            preferred_element_type=f32,
        )
        ubuf[:, 8:, lanes] = (
            product.astype(bf16).astype(f32).reshape(OUTER, rows, size)
        )
    for b in range(OUTER):
        tail_s[2 * b : 2 * b + 2] = ubuf[b, rows + 6 : rows + 8]
    after = z * INNER + (i + 1) % INNER
    send(tail_s, tail_r, misc_r.at[2], {"sp": after, "tp": x})

    forward_c(dn_slot, z2)
    forward_yc(dn_slot, (z + 3) % OUTER)

    arrived(tail_r, misc_r.at[2])
    for b in range(OUTER):
        wrapped = tail_r[2 * b - 2 : 2 * b] if b else jnp.zeros((2, span), f32)
        ubuf[b, 6:8] = jnp.where(i == 0, wrapped, tail_r[2 * b : 2 * b + 2])

    def conv(b, lanes):
        return (
            taps_ref[z, 0:1, lanes] * ubuf[b, pl.ds(6, rows), lanes]
            + taps_ref[z, 1:2, lanes] * ubuf[b, pl.ds(7, rows), lanes]
            + taps_ref[z, 2:3, lanes] * ubuf[b, pl.ds(8, rows), lanes]
        )

    def gate(v):
        return v / (1.0 + jnp.exp(-v))

    @pl.loop(0, OUTER)
    def _(b):
        for t in range(full // LANES):
            lanes = slice(t * LANES, (t + 1) * LANES)
            other = slice(full + t * LANES, full + (t + 1) * LANES)
            hid[b, :, lanes] = (gate(conv(b, other)) * conv(b, lanes)).astype(bf16)
        if extra:
            mixed = conv(b, slice(2 * full, 2 * full + LANES))
            turned_half = pltpu.roll(mixed, LANES // 2, 1)
            last = jnp.where(low, gate(turned_half) * mixed, 0.0)
            hid[b, :, full : full + LANES] = last.astype(bf16)

    forward_c(dn_slot, (z + 1) % OUTER)
    forward_c(dn_slot, (z + 3) % OUTER)
    for zz in range(OUTER):
        arrived(*dn_slot(zz, ic))
        arrived(*dn_slot(zz, idg))

    hidden = hid[...].reshape(count, hid.shape[2])

    def columns(base, store):
        for j in range(deep // 2):
            weight = jnp.concatenate(
                [dn[base + 2 * j], dn[base + 2 * j + 1]], axis=1
            )
            product = jnp.dot(hidden, weight, preferred_element_type=f32)
            store(slice(j * step, (j + 1) * step), product.reshape(OUTER, rows, step))

    def store_other(lanes, value):
        xs[:, :, lanes] = value.astype(bf16)

    def store_own(lanes, value):
        acc[:, :, lanes] = value

    columns(ox * deep, store_other)
    for zz in (z3, z1, z2, z):
        send(xs.at[zz], xr.at[zz], xr_r.at[zz], at(z, i, ox))
    columns(x * deep, store_own)

    def summed(zz):
        arrived(xr.at[zz], xr_r.at[zz])
        return acc[zz] + xr[zz].astype(f32)

    zs[0] = summed(z3).astype(bf16)
    send(zs.at[0], zr.at[0], zr_r.at[0], at(z1, i))
    zs[1] = summed(z1).astype(bf16)
    send(zs.at[1], zr.at[1], zr_r.at[1], at(z1, i))
    partial_sum = summed(z2)
    arrived(zr.at[0], zr_r.at[0])
    zs[2] = (partial_sum + zr[0].astype(f32)).astype(bf16)
    send(zs.at[2], zr.at[2], zr_r.at[2], at(z2, i))
    own = summed(z)
    arrived(zr.at[1], zr_r.at[1])
    own = own + zr[1].astype(f32)
    arrived(zr.at[2], zr_r.at[2])
    out_ref[...] = (stream[...] + (own + zr[2].astype(f32))).astype(bf16)

    for copy in pending:
        copy.wait_send()


def fused_layer(
    residual_in,
    query_pre,
    forget_pre,
    value_pre,
    gate_pre,
    floor_gap,
    head_gain,
    out_weight,
    norm_gain,
    value_weight,
    gate_weight,
    value_taps,
    gate_taps,
    down_weight,
):
    rows, my_width = residual_in.shape
    depth, half = value_weight.shape
    width = query_pre.shape[1]
    blocks = INNER * OUTER
    full = half // LANES // OUTER * LANES
    extra = half // OUTER - full
    chunk = full + extra
    padded = full + (LANES if extra else 0)

    def arrange(value, gate):
        parts = []
        for o in range(OUTER):
            main = slice(o * full, (o + 1) * full)
            rest = slice(OUTER * full + o * extra, OUTER * full + (o + 1) * extra)
            pieces = [value[:, main], gate[:, main]]
            if extra:
                pieces += [value[:, rest], gate[:, rest]]
            parts.append(jnp.concatenate(pieces, axis=1))
        return jnp.stack(parts)

    up_parts = arrange(value_weight, gate_weight)
    taps = arrange(value_taps, gate_taps)
    main = down_weight[: OUTER * full].reshape(OUTER, full, depth)
    rest = down_weight[OUTER * full :].reshape(OUTER, extra, depth)
    dn_parts = jnp.concatenate([main, rest], axis=1)
    keys = floor_gap * jax.nn.sigmoid(-forget_pre.astype(f32))
    log_decay = jnp.log1p(-keys)
    query = jax.nn.silu(query_pre.astype(f32))
    gating = jax.nn.silu(gate_pre.astype(f32))
    values = value_pre.astype(f32)
    gain = jnp.tile(head_gain, width // DK)[None]

    dma = pltpu.SemaphoreType.DMA
    vmem = pl.BlockSpec(memory_space=pltpu.VMEM)
    span = 2 * chunk
    return pl.pallas_call(
        functools.partial(layer_kernel, full, extra),
        out_shape=jax.ShapeDtypeStruct((rows, my_width), bf16),
        in_specs=[vmem] * 12,
        out_specs=vmem,
        scratch_shapes=[
            pltpu.VMEM((blocks, depth, span), bf16),
            pltpu.VMEM((blocks, padded, depth), bf16),
            pltpu.VMEM((INNER, DK + 8, width), f32),
            pltpu.VMEM((OUTER, DK + 8, width), f32),
            pltpu.VMEM((rows, width), f32),
            pltpu.VMEM((rows, width), f32),
            pltpu.VMEM((2, rows, width), bf16),
            pltpu.VMEM((2, rows, LANES), f32),
            pltpu.VMEM((rows, my_width), f32),
            pltpu.VMEM((OUTER, 2, rows, my_width), bf16),
            pltpu.VMEM((OUTER, rows + 8, span), f32),
            pltpu.VMEM((2 * OUTER, span), f32),
            pltpu.VMEM((2 * OUTER, span), f32),
            pltpu.VMEM((OUTER, rows, padded), bf16),
            pltpu.VMEM((OUTER, rows, my_width), f32),
            pltpu.VMEM((OUTER, rows, my_width), bf16),
            pltpu.VMEM((OUTER, rows, my_width), bf16),
            pltpu.VMEM((3, rows, my_width), bf16),
            pltpu.VMEM((3, rows, my_width), bf16),
            dma((80,)),
            dma((blocks,)),
            dma((blocks,)),
            dma((INNER,)),
            dma((OUTER,)),
            dma((2 * OUTER,)),
            dma((OUTER,)),
            dma((3,)),
            dma((3,)),
        ],
        compiler_params=pltpu.CompilerParams(
            collective_id=0, has_side_effects=True, vmem_limit_bytes=56 * 2**20
        ),
        name="layer",
    )(
        up_parts,
        dn_parts,
        keys,
        log_decay,
        query,
        values,
        gating,
        gain,
        residual_in,
        out_weight,
        norm_gain[None],
        taps,
    )


def local_recurrence(query_pre, forget_pre, value_pre, floor_gap):
    rows, width = query_pre.shape
    heads = width // DK
    subs = rows // SUB
    keys = floor_gap * jax.nn.sigmoid(-forget_pre.astype(f32))
    log_decay = jnp.log1p(-keys)
    query = jax.nn.silu(query_pre.astype(f32))
    values = value_pre.astype(f32)
    position = lax.iota(jnp.int32, rows)
    lower = (position[:, None] >= position[None, :]).astype(f32)
    running = jnp.dot(lower, log_decay, precision=highest)
    middle = running.reshape(subs, SUB, width)[:, SUB // 2 - 1, :]
    query_part = query * jnp.exp(running - jnp.repeat(middle, SUB, axis=0))
    reach = (lax.iota(jnp.int32, subs) + 1) * SUB
    seen = position[None, :, None] < reach[:, None, None]
    key_part = keys[None] * jnp.exp(
        jnp.where(seen, middle[:, None, :] - running[None], -jnp.inf)
    )
    scores = jnp.einsum(
        "ithk,ishk->hits",
        query_part.reshape(subs, SUB, heads, DK),
        key_part.reshape(subs, rows, heads, DK),
        precision=highest,
    ).reshape(heads, rows, rows)
    scores = jnp.where(position[None, :, None] >= position[None, None, :], scores, 0.0)
    value_heads = values.reshape(rows, heads, DK)
    inner = jnp.einsum("hts,shv->htv", scores, value_heads, precision=highest)
    ending = running[-1]
    state = jnp.einsum(
        "shv,shk->vhk",
        value_heads,
        (keys * jnp.exp(ending - running)).reshape(rows, heads, DK),
        precision=highest,
    ).reshape(DK, width)
    from_start = (query * jnp.exp(running)).reshape(rows, heads, DK)
    return inner, state, jnp.exp(ending), from_start


def causal_taps(before, current, taps):
    padded = jnp.concatenate([before, current], axis=1).astype(f32)
    rows = current.shape[1]
    return (
        taps[0] * padded[:, 0:rows]
        + taps[1] * padded[:, 1 : rows + 1]
        + taps[2] * padded[:, 2 : rows + 2]
    )


def on_device(
    residual_in,
    query_pre,
    forget_pre,
    value_pre,
    gate_pre,
    floor_gap,
    head_gain,
    out_weight,
    norm_gain,
    value_weight,
    gate_weight,
    value_taps,
    gate_taps,
    down_weight,
):
    sp = lax.axis_size("sp")
    tp = lax.axis_size("tp")
    inner_size = 4 if sp % 4 == 0 else 1
    outer = sp // inner_size
    me = lax.axis_index("sp")
    my_outer = me // inner_size
    my_inner = me % inner_size
    outer_groups = [[o * inner_size + i for o in range(outer)] for i in range(inner_size)]
    inner_groups = [[o * inner_size + i for i in range(inner_size)] for o in range(outer)]
    rows, my_width = residual_in.shape
    width = my_width * tp
    depth, half = value_weight.shape
    chunk = half // outer

    wide_groups = [
        [s * tp + t for s in group for t in range(tp)] for group in outer_groups
    ]

    def exchange(array):
        return lax.all_to_all(
            array, "sp", 0, 0, axis_index_groups=outer_groups, tiled=True
        )

    def gather_inner(array):
        return lax.all_gather(array, "sp", axis_index_groups=inner_groups)

    def gather_wide(array):
        gathered = lax.all_gather(array, ("sp", "tp"), axis_index_groups=wide_groups)
        gathered = gathered.reshape(outer, tp, *array.shape)
        return [gathered[:, t].reshape(-1, array.shape[1]) for t in range(tp)]

    def reorder(pieces):
        span = pieces[0].shape[-1]
        blocks = []
        for i in range(inner_size):
            for o in range(outer):
                start = (o * inner_size + i) * depth
                low = start % span
                blocks.append(pieces[start // span][..., low : low + depth])
        return lax.optimization_barrier(jnp.concatenate(blocks, axis=-1))

    up_parts = jnp.stack(
        [
            jnp.concatenate(
                [
                    value_weight[:, o * chunk : (o + 1) * chunk],
                    gate_weight[:, o * chunk : (o + 1) * chunk],
                ],
                axis=1,
            )
            for o in range(outer)
        ]
    )
    up_chunk = gather_inner(exchange(up_parts)).reshape(width, 2 * chunk)
    down_parts = down_weight.reshape(outer, chunk, depth)
    down_mine = gather_inner(exchange(down_parts))
    down_chunk = down_mine.transpose(2, 1, 0, 3).reshape(chunk, width)

    out_full = reorder(list(lax.all_gather(out_weight, "tp")))
    gain_full = reorder(list(lax.all_gather(norm_gain, "tp")))
    residual_group = reorder(gather_wide(residual_in))

    inner, state, total_decay, from_start = local_recurrence(
        query_pre, forget_pre, value_pre, floor_gap
    )
    heads = inner.shape[0]
    first = total_decay.astype(bf16)
    rest = total_decay - first.astype(f32)
    second = rest.astype(bf16)
    third = (rest - second.astype(f32)).astype(bf16)
    spare = jnp.zeros((13, heads * DK), bf16)
    packed = jnp.concatenate(
        [state.astype(bf16), first[None], second[None], third[None], spare], axis=0
    )
    everyone = lax.all_gather(packed, "sp").astype(f32)
    decays = everyone[:, DK] + everyone[:, DK + 1] + everyone[:, DK + 2]
    entering = jnp.zeros_like(state)
    for j in range(sp - 1):
        advanced = entering * decays[j] + everyone[j, :DK]
        entering = jnp.where(j < me, advanced, entering)
    carried = jnp.einsum(
        "thk,vhk->htv", from_start, entering.reshape(DK, heads, DK), precision=highest
    )
    recurrent = (inner + carried).transpose(1, 0, 2)
    scaled = (
        recurrent
        * lax.rsqrt(jnp.mean(recurrent * recurrent, axis=-1, keepdims=True) + epsilon)
        * head_gain
    )
    gating = jax.nn.silu(gate_pre.astype(f32)).reshape(recurrent.shape)
    head_out = (scaled * gating).reshape(rows, heads * DK).astype(bf16)

    head_out, out_full = lax.optimization_barrier((head_out, out_full))
    head_group = jnp.concatenate(gather_wide(head_out), axis=1)
    stream = residual_group.astype(f32) + jnp.dot(
        head_group, out_full, preferred_element_type=f32
    )
    squares = jnp.mean(stream * stream, axis=1, keepdims=True)
    normed = (stream * lax.rsqrt(squares + epsilon) * gain_full).astype(bf16)
    up = jnp.dot(normed, up_chunk, preferred_element_type=f32).astype(bf16)
    up = up.reshape(outer, rows, 2 * chunk)
    tails = up[:, rows - 2 :]
    pairs = [
        (o * inner_size + i, o * inner_size + (i + 1) % inner_size)
        for o in range(outer)
        for i in range(inner_size)
    ]
    arrived = lax.ppermute(tails, "sp", pairs) if inner_size > 1 else tails
    wrapped = jnp.concatenate([jnp.zeros_like(arrived[:1]), arrived[:-1]], axis=0)
    before = jnp.where(my_inner == 0, wrapped, arrived)

    taps = jnp.concatenate(
        [
            lax.dynamic_slice_in_dim(value_taps, my_outer * chunk, chunk, axis=1),
            lax.dynamic_slice_in_dim(gate_taps, my_outer * chunk, chunk, axis=1),
        ],
        axis=1,
    )
    conv = causal_taps(before, up, taps)
    hidden = (jax.nn.silu(conv[:, :, chunk:]) * conv[:, :, :chunk]).astype(bf16)
    terms = jnp.dot(
        hidden.reshape(outer * rows, chunk), down_chunk, preferred_element_type=f32
    ).astype(bf16)
    summed = lax.psum_scatter(
        terms, "sp", scatter_dimension=0, tiled=True, axis_index_groups=outer_groups
    )
    summed = lax.psum_scatter(summed, "tp", scatter_dimension=1, tiled=True)
    my_heads = lax.dynamic_slice_in_dim(head_group, my_outer * rows, rows, axis=0)
    own = residual_in.astype(f32) + jnp.dot(
        my_heads, out_weight, preferred_element_type=f32
    )
    return (own + summed.astype(f32)).astype(bf16)


def fits(mesh, residual_in, query_pre, *arrays):
    depth, half = arrays[7].shape
    extra = half // OUTER % LANES
    return (
        mesh.shape["sp"] == INNER * OUTER
        and mesh.shape["tp"] == 2
        and depth == LANES
        and residual_in.shape == (LANES, depth * INNER * OUTER // 2)
        and query_pre.shape[1] % LANES == 0
        and half % LANES == 0
        and extra in (0, LANES // 2)
    )


def solution(mesh):
    rows = P(("grp", "sp"), "tp")

    def layer(*arrays):
        return (fused_layer if fits(mesh, *arrays) else on_device)(*arrays)

    return jax.shard_map(
        layer,
        mesh=mesh,
        in_specs=(
            rows,
            rows,
            rows,
            rows,
            rows,
            P("tp"),
            P(),
            P(None, "tp"),
            P("tp"),
            P("sp", "tp"),
            P("sp", "tp"),
            P(None, "tp"),
            P(None, "tp"),
            P("tp", "sp"),
        ),
        out_specs=rows,
        check_vma=False,
    )
```

```python
import functools

import jax
import jax.numpy as jnp
from jax import lax
from jax.experimental import pallas as pl
from jax.experimental.pallas import tpu as pltpu
from jax.sharding import PartitionSpec as P

DK = 64
SUB = 16
LANES = 128
INNER = 4
OUTER = 4
epsilon = 1e-06
highest = lax.Precision.HIGHEST
f32 = jnp.float32
bf16 = jnp.bfloat16
MESH = pl.DeviceIdType.MESH


def dot_nt(a, b):
    return lax.dot_general(
        a, b, (((1,), (1,)), ((), ())), precision=highest, preferred_element_type=f32
    )


def dot_hi(a, b):
    return jnp.dot(a, b, precision=highest, preferred_element_type=f32)


def gate(v):
    return v / (1.0 + jnp.exp(-v))


def turn(v):
    return jnp.concatenate([v[:, DK:], v[:, :DK]], axis=1)


def layer_kernel(
    full,
    extra,
    residual_ref,
    query_ref,
    forget_ref,
    value_ref,
    gate_ref,
    floor_ref,
    head_gain_ref,
    out_weight_ref,
    norm_gain_ref,
    value_weight_ref,
    gate_weight_ref,
    value_taps_ref,
    gate_taps_ref,
    down_ref,
    out_ref,
    up_in,
    dn_in,
    taps,
    up,
    dn,
    st,
    zt,
    inner_buf,
    start_buf,
    ho,
    sq,
    stream,
    nb,
    ubuf,
    tail_s,
    tail_r,
    hid,
    acc,
    xs,
    xr,
    zs,
    zr,
    ssem,
    up_r,
    dn_r,
    st_r,
    zt_r,
    nb_r,
    xr_r,
    zr_r,
    misc_r,
):
    s = lax.axis_index("sp")
    x = lax.axis_index("tp")
    z = s // INNER
    i = s % INNER
    c = s % 2
    ox = 1 - x
    ic = i + 1 - 2 * c
    iy = (i + 2) % INNER
    idg = (ic + 2) % INNER
    z1 = z + 1 - 2 * (z % 2)
    z2 = (z + 2) % OUTER
    z3 = OUTER - 1 - z
    chunk = full + extra
    rows = query_ref.shape[0]
    width = query_ref.shape[1]
    pairs = width // LANES
    pending = []

    def at(zz, ii, xx=x):
        return {"sp": zz * INNER + ii, "tp": xx}

    def send(src, dst, rsem, device):
        copy = pltpu.make_async_remote_copy(
            src_ref=src,
            dst_ref=dst,
            send_sem=ssem.at[len(pending)],
            recv_sem=rsem,
            device_id=device,
            device_id_type=MESH,
        )
        copy.start()
        pending.append(copy)

    def arrived(dst, rsem):
        pltpu.make_async_remote_copy(
            src_ref=dst,
            dst_ref=dst,
            send_sem=ssem.at[0],
            recv_sem=rsem,
            device_id=at(z, ic),
            device_id_type=MESH,
        ).wait_recv()

    barrier = pltpu.get_barrier_semaphore()
    peers = [at((z + k) % OUTER, i) for k in range(1, OUTER)]
    peers += [at(z, ic), at(z, iy), at(z, idg), at(z, i, ox)]
    for peer in peers:
        pl.semaphore_signal(barrier, inc=1, device_id=peer, device_id_type=MESH)
    pl.semaphore_wait(barrier, len(peers))

    def up_slot(zz, ii):
        return up.at[zz * INNER + ii], up_r.at[zz * INNER + ii]

    def dn_slot(zz, ii):
        slot = dn.at[zz * INNER + ii, pl.ds(0, chunk)]
        return slot, dn_r.at[zz * INNER + ii]

    def send_z(source, slot, zz):
        dst, sem = slot(z, i)
        send(source.at[zz], dst, sem, at(zz, i))

    def forward_yc(slot, zz, source=None):
        dst, sem = slot(zz, i)
        if source is None:
            arrived(dst, sem)
            source = dst
        send(source, dst, sem, at(z, iy))
        send(source, dst, sem, at(z, ic))

    def forward_c(slot, zz):
        dst, sem = slot(zz, iy)
        arrived(dst, sem)
        send(dst, dst, sem, at(z, ic))

    keys = floor_ref[...] * jax.nn.sigmoid(-forget_ref[...].astype(f32))
    query = gate(query_ref[...].astype(f32))
    values = value_ref[...].astype(f32)
    position = lax.broadcasted_iota(jnp.int32, (rows, rows), 0)
    earlier = lax.broadcasted_iota(jnp.int32, (rows, rows), 1)
    running = dot_hi((position >= earlier).astype(f32), jnp.log1p(-keys))
    ending = running[rows - 1 : rows]
    kept = keys * jnp.exp(ending - running)
    turned = values.T
    low = lax.broadcasted_iota(jnp.int32, (1, LANES), 1) < DK
    part_row = lax.broadcasted_iota(jnp.int32, (SUB, width), 0)

    def store_state(ref, state, decay):
        ref[0:DK] = state.astype(bf16)
        one = decay.astype(bf16).astype(f32)
        two = (decay - one).astype(bf16).astype(f32)
        three = decay - one - two
        parts = jnp.where(part_row == 1, two, jnp.where(part_row == 2, three, 0.0))
        ref[DK : DK + SUB] = jnp.where(part_row == 0, one, parts).astype(bf16)

    def load_state(ref):
        parts = ref[DK : DK + SUB].astype(f32)
        return ref[0:DK].astype(f32), parts[0:1] + parts[1:2] + parts[2:3]

    states = []
    for p in range(pairs):
        lanes = slice(p * LANES, (p + 1) * LANES)
        both = dot_hi(turned[lanes], kept[:, lanes])
        states.append(jnp.where(low, both[:DK], both[DK:]))
    store_state(st.at[i], jnp.concatenate(states, axis=1), jnp.exp(ending))
    for ii in (ic, iy, idg):
        send(st.at[i], st.at[i], st_r.at[i], at(z, ii))

    for o in range(OUTER):
        main = slice(o * full, (o + 1) * full)
        up_in[o, :, 0:full] = value_weight_ref[:, main]
        up_in[o, :, full : 2 * full] = gate_weight_ref[:, main]
        dn_in[o, 0:full] = down_ref[main]
        if extra:
            start = OUTER * full + o * extra
            dn_in[o, full:chunk] = down_ref[start : start + extra]
    if extra:
        for o in range(0, OUTER, 2):
            start = OUTER * full + o * extra
            tile = slice(start, start + LANES)
            v = value_weight_ref[:, tile].astype(f32)
            g = gate_weight_ref[:, tile].astype(f32)
            end = slice(2 * full, 2 * full + LANES)
            up_in[o, :, end] = jnp.where(low, v, turn(g)).astype(bf16)
            up_in[o + 1, :, end] = jnp.where(low, turn(v), g).astype(bf16)

    forward_yc(up_slot, z, up_in.at[z])
    send_z(dn_in, dn_slot, z1)
    forward_yc(dn_slot, z, dn_in.at[z])
    up[s] = up_in[z]
    dn[s, 0:chunk] = dn_in[z]
    spare = dn.shape[1] - chunk
    if spare:
        for b in range(INNER * OUTER):
            dn[b, chunk:] = jnp.zeros((spare, dn.shape[2]), bf16)
    start_buf[...] = query * jnp.exp(running)

    for ii in (ic, iy, idg):
        arrived(st.at[ii], st_r.at[ii])
    total = jnp.zeros((DK, width), f32)
    mine = jnp.zeros((DK, width), f32)
    total_decay = jnp.ones((1, width), f32)
    my_decay = jnp.ones((1, width), f32)
    for j in range(INNER):
        fresh, decay = load_state(st.at[j])
        mine = jnp.where(j < i, mine * decay + fresh, mine)
        my_decay = jnp.where(j < i, my_decay * decay, my_decay)
        total = total * decay + fresh
        total_decay = total_decay * decay
    store_state(zt.at[z], total, total_decay)
    for k in range(1, OUTER):
        send(zt.at[z], zt.at[z], zt_r.at[z], at((z + k) % OUTER, i))
    send_z(up_in, up_slot, z2)
    send_z(up_in, up_slot, z1)

    cells = [[] for _ in range(pairs)]
    row_of = lax.broadcasted_iota(jnp.int32, (rows, width), 0)
    column = lax.broadcasted_iota(jnp.int32, (2 * SUB, rows), 1)
    stacked = lax.broadcasted_iota(jnp.int32, (2 * SUB, rows), 0) % SUB
    for n in range(rows // SUB):
        part = slice(n * SUB, (n + 1) * SUB)
        middle = running[n * SUB + SUB // 2 - 1 : n * SUB + SUB // 2]
        query_part = query[part] * jnp.exp(running[part] - middle)
        reach = jnp.where(row_of < (n + 1) * SUB, middle - running, -jnp.inf)
        key_part = keys * jnp.exp(reach)
        for p in range(pairs):
            lanes = slice(p * LANES, (p + 1) * LANES)
            piece = query_part[:, lanes]
            piece = jnp.concatenate(
                [jnp.where(low, piece, 0.0), jnp.where(low, 0.0, piece)], axis=0
            )
            score = dot_nt(piece, key_part[:, lanes])
            score = jnp.where(stacked + n * SUB >= column, score, 0.0)
            cells[p].append(score)
    for p in range(pairs):
        lanes = slice(p * LANES, (p + 1) * LANES)
        scores = jnp.concatenate(
            [cell[:SUB] for cell in cells[p]] + [cell[SUB:] for cell in cells[p]],
            axis=0,
        )
        result = dot_hi(scores, values[:, lanes])
        inner_buf[:, lanes] = jnp.where(low, result[:rows], result[rows:])

    gain = jnp.concatenate([head_gain_ref[...]] * (LANES // DK), axis=1)
    gating = gate(gate_ref[...].astype(f32))
    for k in range(1, OUTER):
        zz = (z + k) % OUTER
        arrived(zt.at[zz], zt_r.at[zz])
    entering = jnp.zeros((DK, width), f32)
    for j in range(OUTER - 1):
        fresh, decay = load_state(zt.at[j])
        entering = jnp.where(j < z, entering * decay + fresh, entering)
    entering = entering * my_decay + mine
    same_head = (
        lax.broadcasted_iota(jnp.int32, (LANES, LANES), 0) // DK
        == lax.broadcasted_iota(jnp.int32, (LANES, LANES), 1) // DK
    ).astype(f32)
    for p in range(pairs):
        lanes = slice(p * LANES, (p + 1) * LANES)
        piece = entering[:, lanes]
        piece = jnp.concatenate(
            [jnp.where(low, piece, 0.0), jnp.where(low, 0.0, piece)], axis=0
        )
        recurrent = inner_buf[:, lanes] + dot_nt(start_buf[:, lanes], piece)
        squares = dot_hi(recurrent * recurrent, same_head) * (1.0 / DK)
        scaled = recurrent * lax.rsqrt(squares + epsilon) * gain
        ho[x, :, lanes] = (scaled * gating[:, lanes]).astype(bf16)
    send(ho.at[x], ho.at[x], misc_r.at[0], at(z, i, ox))

    forward_c(up_slot, z)

    arrived(ho.at[ox], misc_r.at[0])
    heads = jnp.concatenate([ho[0], ho[1]], axis=1)
    stream[...] = residual_ref[...].astype(f32) + jnp.dot(
        heads, out_weight_ref[...], preferred_element_type=f32
    )
    partial = jnp.sum(stream[...] * stream[...], axis=1, keepdims=True)
    sq[x] = jnp.broadcast_to(partial, (rows, LANES))
    send(sq.at[x], sq.at[x], misc_r.at[1], at(z, i, ox))
    arrived(sq.at[ox], misc_r.at[1])
    channels = 2 * stream.shape[1]
    mean = (sq[0][:, 0:1] + sq[1][:, 0:1]) * (1.0 / channels)
    normed = stream[...] * lax.rsqrt(mean + epsilon) * norm_gain_ref[...]
    nb[z, x] = normed.astype(bf16)

    def nb_slot(zz, xx):
        return nb.at[zz, xx], nb_r.at[zz * 2 + xx]

    def share(zz, devices):
        dst, sem = nb_slot(zz, x)
        for device in devices:
            send(dst, dst, sem, device)

    share(z, [at(z2, i), at(z1, i), at(z, i, ox)])
    forward_c(dn_slot, z)
    forward_yc(up_slot, z2)
    forward_yc(up_slot, z1)
    arrived(*nb_slot(z2, x))
    share(z2, [at(z1, i), at(z, i, ox)])
    send_z(up_in, up_slot, z3)
    arrived(*nb_slot(z1, x))
    share(z1, [at(z, i, ox)])
    forward_c(up_slot, z2)
    forward_c(up_slot, z1)
    forward_yc(dn_slot, z1)
    arrived(*nb_slot(z3, x))
    share(z3, [at(z, i, ox)])
    forward_yc(up_slot, z3)
    forward_c(dn_slot, z1)
    forward_c(up_slot, z3)
    send_z(dn_in, dn_slot, z2)
    send_z(dn_in, dn_slot, z3)

    for zz in range(OUTER):
        arrived(*up_slot(zz, ic))
        arrived(*up_slot(zz, idg))
        arrived(*nb_slot(zz, ox))

    mine_at = pl.ds(pl.multiple_of(z * full, LANES), full)
    taps[:, 0:full] = value_taps_ref[:, mine_at]
    taps[:, full : 2 * full] = gate_taps_ref[:, mine_at]
    if extra:
        tile = pl.ds(pl.multiple_of(OUTER * full + z // 2 * LANES, LANES), LANES)
        v = value_taps_ref[:, tile]
        g = gate_taps_ref[:, tile]
        v = jnp.where(z % 2 == 0, v, turn(v))
        g = jnp.where(z % 2 == 0, turn(g), g)
        taps[:, 2 * full : 2 * full + LANES] = jnp.where(low, v, g)

    count = OUTER * rows
    half = nb.shape[3]
    deep = half // up.shape[1]
    first = nb[:, 0].reshape(count, half)
    second = nb[:, 1].reshape(count, half)
    span = up.shape[2]
    step = 2 * LANES
    for low_lane in range(0, span, step):
        lanes = slice(low_lane, min(span, low_lane + step))
        size = lanes.stop - lanes.start
        product = jnp.dot(
            first, up[0:deep, :, lanes].reshape(half, size), preferred_element_type=f32
        ) + jnp.dot(
            second,
            up[deep : 2 * deep, :, lanes].reshape(half, size),
            preferred_element_type=f32,
        )
        ubuf[:, 8:, lanes] = (
            product.astype(bf16).astype(f32).reshape(OUTER, rows, size)
        )
    for b in range(OUTER):
        tail_s[2 * b : 2 * b + 2] = ubuf[b, rows + 6 : rows + 8]
    after = z * INNER + (i + 1) % INNER
    send(tail_s, tail_r, misc_r.at[2], {"sp": after, "tp": x})

    forward_yc(dn_slot, z2)
    forward_yc(dn_slot, z3)

    arrived(tail_r, misc_r.at[2])
    for b in range(OUTER):
        wrapped = tail_r[2 * b - 2 : 2 * b] if b else jnp.zeros((2, span), f32)
        ubuf[b, 6:8] = jnp.where(i == 0, wrapped, tail_r[2 * b : 2 * b + 2])

    def conv(b, lanes):
        return (
            taps[0:1, lanes] * ubuf[b, pl.ds(6, rows), lanes]
            + taps[1:2, lanes] * ubuf[b, pl.ds(7, rows), lanes]
            + taps[2:3, lanes] * ubuf[b, pl.ds(8, rows), lanes]
        )

    @pl.loop(0, OUTER)
    def _(b):
        for t in range(full // LANES):
            lanes = slice(t * LANES, (t + 1) * LANES)
            other = slice(full + t * LANES, full + (t + 1) * LANES)
            hid[b, :, lanes] = (gate(conv(b, other)) * conv(b, lanes)).astype(bf16)
        if extra:
            mixed = conv(b, slice(2 * full, 2 * full + LANES))
            turned_half = turn(mixed)
            last = jnp.where(low, gate(turned_half) * mixed, 0.0)
            hid[b, :, full : full + LANES] = last.astype(bf16)

    forward_c(dn_slot, z2)
    forward_c(dn_slot, z3)
    for zz in range(OUTER):
        arrived(*dn_slot(zz, ic))
        arrived(*dn_slot(zz, idg))

    def columns(zz, base, store):
        for j in range(deep // 2):
            weight = jnp.concatenate(
                [dn[base + 2 * j], dn[base + 2 * j + 1]], axis=1
            )
            product = jnp.dot(hid[zz], weight, preferred_element_type=f32)
            store[zz, :, j * step : (j + 1) * step] = product.astype(store.dtype)

    for zz in (z3, z1, z2, z):
        columns(zz, ox * deep, xs)
        send(xs.at[zz], xr.at[zz], xr_r.at[zz], at(z, i, ox))
    for zz in (z3, z1, z2, z):
        columns(zz, x * deep, acc)

    def summed(zz):
        arrived(xr.at[zz], xr_r.at[zz])
        return acc[zz] + xr[zz].astype(f32)

    zs[0] = summed(z3).astype(bf16)
    send(zs.at[0], zr.at[0], zr_r.at[0], at(z1, i))
    zs[1] = summed(z1).astype(bf16)
    send(zs.at[1], zr.at[1], zr_r.at[1], at(z1, i))
    partial_sum = summed(z2)
    arrived(zr.at[0], zr_r.at[0])
    zs[2] = (partial_sum + zr[0].astype(f32)).astype(bf16)
    send(zs.at[2], zr.at[2], zr_r.at[2], at(z2, i))
    own = summed(z)
    arrived(zr.at[1], zr_r.at[1])
    own = own + zr[1].astype(f32)
    arrived(zr.at[2], zr_r.at[2])
    out_ref[...] = (stream[...] + (own + zr[2].astype(f32))).astype(bf16)

    for copy in pending:
        copy.wait_send()


def fused_layer(
    residual_in,
    query_pre,
    forget_pre,
    value_pre,
    gate_pre,
    floor_gap,
    head_gain,
    out_weight,
    norm_gain,
    value_weight,
    gate_weight,
    value_taps,
    gate_taps,
    down_weight,
):
    rows, my_width = residual_in.shape
    depth, half = value_weight.shape
    width = query_pre.shape[1]
    blocks = INNER * OUTER
    full = half // LANES // OUTER * LANES
    extra = half // OUTER - full
    chunk = full + extra
    padded = full + (LANES if extra else 0)

    dma = pltpu.SemaphoreType.DMA
    vmem = pl.BlockSpec(memory_space=pltpu.VMEM)
    span = 2 * chunk
    return pl.pallas_call(
        functools.partial(layer_kernel, full, extra),
        out_shape=jax.ShapeDtypeStruct((rows, my_width), bf16),
        in_specs=[vmem] * 14,
        out_specs=vmem,
        scratch_shapes=[
            pltpu.VMEM((OUTER, depth, span), bf16),
            pltpu.VMEM((OUTER, chunk, depth), bf16),
            pltpu.VMEM((value_taps.shape[0], span), f32),
            pltpu.VMEM((blocks, depth, span), bf16),
            pltpu.VMEM((blocks, padded, depth), bf16),
            pltpu.VMEM((INNER, DK + SUB, width), bf16),
            pltpu.VMEM((OUTER, DK + SUB, width), bf16),
            pltpu.VMEM((rows, width), f32),
            pltpu.VMEM((rows, width), f32),
            pltpu.VMEM((2, rows, width), bf16),
            pltpu.VMEM((2, rows, LANES), f32),
            pltpu.VMEM((rows, my_width), f32),
            pltpu.VMEM((OUTER, 2, rows, my_width), bf16),
            pltpu.VMEM((OUTER, rows + 8, span), f32),
            pltpu.VMEM((2 * OUTER, span), f32),
            pltpu.VMEM((2 * OUTER, span), f32),
            pltpu.VMEM((OUTER, rows, padded), bf16),
            pltpu.VMEM((OUTER, rows, my_width), f32),
            pltpu.VMEM((OUTER, rows, my_width), bf16),
            pltpu.VMEM((OUTER, rows, my_width), bf16),
            pltpu.VMEM((3, rows, my_width), bf16),
            pltpu.VMEM((3, rows, my_width), bf16),
            dma((80,)),
            dma((blocks,)),
            dma((blocks,)),
            dma((INNER,)),
            dma((OUTER,)),
            dma((2 * OUTER,)),
            dma((OUTER,)),
            dma((3,)),
            dma((3,)),
        ],
        compiler_params=pltpu.CompilerParams(
            collective_id=0, has_side_effects=True, vmem_limit_bytes=56 * 2**20
        ),
        name="layer",
    )(
        residual_in,
        query_pre,
        forget_pre,
        value_pre,
        gate_pre,
        floor_gap[None],
        head_gain[None],
        out_weight,
        norm_gain[None],
        value_weight,
        gate_weight,
        value_taps,
        gate_taps,
        down_weight,
    )


def local_recurrence(query_pre, forget_pre, value_pre, floor_gap):
    rows, width = query_pre.shape
    heads = width // DK
    subs = rows // SUB
    keys = floor_gap * jax.nn.sigmoid(-forget_pre.astype(f32))
    log_decay = jnp.log1p(-keys)
    query = jax.nn.silu(query_pre.astype(f32))
    values = value_pre.astype(f32)
    position = lax.iota(jnp.int32, rows)
    lower = (position[:, None] >= position[None, :]).astype(f32)
    running = jnp.dot(lower, log_decay, precision=highest)
    middle = running.reshape(subs, SUB, width)[:, SUB // 2 - 1, :]
    query_part = query * jnp.exp(running - jnp.repeat(middle, SUB, axis=0))
    reach = (lax.iota(jnp.int32, subs) + 1) * SUB
    seen = position[None, :, None] < reach[:, None, None]
    key_part = keys[None] * jnp.exp(
        jnp.where(seen, middle[:, None, :] - running[None], -jnp.inf)
    )
    scores = jnp.einsum(
        "ithk,ishk->hits",
        query_part.reshape(subs, SUB, heads, DK),
        key_part.reshape(subs, rows, heads, DK),
        precision=highest,
    ).reshape(heads, rows, rows)
    scores = jnp.where(position[None, :, None] >= position[None, None, :], scores, 0.0)
    value_heads = values.reshape(rows, heads, DK)
    inner = jnp.einsum("hts,shv->htv", scores, value_heads, precision=highest)
    ending = running[-1]
    state = jnp.einsum(
        "shv,shk->vhk",
        value_heads,
        (keys * jnp.exp(ending - running)).reshape(rows, heads, DK),
        precision=highest,
    ).reshape(DK, width)
    from_start = (query * jnp.exp(running)).reshape(rows, heads, DK)
    return inner, state, jnp.exp(ending), from_start


def causal_taps(before, current, taps):
    padded = jnp.concatenate([before, current], axis=1).astype(f32)
    rows = current.shape[1]
    return (
        taps[0] * padded[:, 0:rows]
        + taps[1] * padded[:, 1 : rows + 1]
        + taps[2] * padded[:, 2 : rows + 2]
    )


def on_device(
    residual_in,
    query_pre,
    forget_pre,
    value_pre,
    gate_pre,
    floor_gap,
    head_gain,
    out_weight,
    norm_gain,
    value_weight,
    gate_weight,
    value_taps,
    gate_taps,
    down_weight,
):
    sp = lax.axis_size("sp")
    tp = lax.axis_size("tp")
    inner_size = 4 if sp % 4 == 0 else 1
    outer = sp // inner_size
    me = lax.axis_index("sp")
    my_outer = me // inner_size
    my_inner = me % inner_size
    outer_groups = [[o * inner_size + i for o in range(outer)] for i in range(inner_size)]
    inner_groups = [[o * inner_size + i for i in range(inner_size)] for o in range(outer)]
    rows, my_width = residual_in.shape
    width = my_width * tp
    depth, half = value_weight.shape
    chunk = half // outer

    wide_groups = [
        [s * tp + t for s in group for t in range(tp)] for group in outer_groups
    ]

    def exchange(array):
        return lax.all_to_all(
            array, "sp", 0, 0, axis_index_groups=outer_groups, tiled=True
        )

    def gather_inner(array):
        return lax.all_gather(array, "sp", axis_index_groups=inner_groups)

    def gather_wide(array):
        gathered = lax.all_gather(array, ("sp", "tp"), axis_index_groups=wide_groups)
        gathered = gathered.reshape(outer, tp, *array.shape)
        return [gathered[:, t].reshape(-1, array.shape[1]) for t in range(tp)]

    def reorder(pieces):
        span = pieces[0].shape[-1]
        blocks = []
        for i in range(inner_size):
            for o in range(outer):
                start = (o * inner_size + i) * depth
                low = start % span
                blocks.append(pieces[start // span][..., low : low + depth])
        return lax.optimization_barrier(jnp.concatenate(blocks, axis=-1))

    up_parts = jnp.stack(
        [
            jnp.concatenate(
                [
                    value_weight[:, o * chunk : (o + 1) * chunk],
                    gate_weight[:, o * chunk : (o + 1) * chunk],
                ],
                axis=1,
            )
            for o in range(outer)
        ]
    )
    up_chunk = gather_inner(exchange(up_parts)).reshape(width, 2 * chunk)
    down_parts = down_weight.reshape(outer, chunk, depth)
    down_mine = gather_inner(exchange(down_parts))
    down_chunk = down_mine.transpose(2, 1, 0, 3).reshape(chunk, width)

    out_full = reorder(list(lax.all_gather(out_weight, "tp")))
    gain_full = reorder(list(lax.all_gather(norm_gain, "tp")))
    residual_group = reorder(gather_wide(residual_in))

    inner, state, total_decay, from_start = local_recurrence(
        query_pre, forget_pre, value_pre, floor_gap
    )
    heads = inner.shape[0]
    first = total_decay.astype(bf16)
    rest = total_decay - first.astype(f32)
    second = rest.astype(bf16)
    third = (rest - second.astype(f32)).astype(bf16)
    spare = jnp.zeros((13, heads * DK), bf16)
    packed = jnp.concatenate(
        [state.astype(bf16), first[None], second[None], third[None], spare], axis=0
    )
    everyone = lax.all_gather(packed, "sp").astype(f32)
    decays = everyone[:, DK] + everyone[:, DK + 1] + everyone[:, DK + 2]
    entering = jnp.zeros_like(state)
    for j in range(sp - 1):
        advanced = entering * decays[j] + everyone[j, :DK]
        entering = jnp.where(j < me, advanced, entering)
    carried = jnp.einsum(
        "thk,vhk->htv", from_start, entering.reshape(DK, heads, DK), precision=highest
    )
    recurrent = (inner + carried).transpose(1, 0, 2)
    scaled = (
        recurrent
        * lax.rsqrt(jnp.mean(recurrent * recurrent, axis=-1, keepdims=True) + epsilon)
        * head_gain
    )
    gating = jax.nn.silu(gate_pre.astype(f32)).reshape(recurrent.shape)
    head_out = (scaled * gating).reshape(rows, heads * DK).astype(bf16)

    head_out, out_full = lax.optimization_barrier((head_out, out_full))
    head_group = jnp.concatenate(gather_wide(head_out), axis=1)
    stream = residual_group.astype(f32) + jnp.dot(
        head_group, out_full, preferred_element_type=f32
    )
    squares = jnp.mean(stream * stream, axis=1, keepdims=True)
    normed = (stream * lax.rsqrt(squares + epsilon) * gain_full).astype(bf16)
    up = jnp.dot(normed, up_chunk, preferred_element_type=f32).astype(bf16)
    up = up.reshape(outer, rows, 2 * chunk)
    tails = up[:, rows - 2 :]
    pairs = [
        (o * inner_size + i, o * inner_size + (i + 1) % inner_size)
        for o in range(outer)
        for i in range(inner_size)
    ]
    arrived = lax.ppermute(tails, "sp", pairs) if inner_size > 1 else tails
    wrapped = jnp.concatenate([jnp.zeros_like(arrived[:1]), arrived[:-1]], axis=0)
    before = jnp.where(my_inner == 0, wrapped, arrived)

    taps = jnp.concatenate(
        [
            lax.dynamic_slice_in_dim(value_taps, my_outer * chunk, chunk, axis=1),
            lax.dynamic_slice_in_dim(gate_taps, my_outer * chunk, chunk, axis=1),
        ],
        axis=1,
    )
    conv = causal_taps(before, up, taps)
    hidden = (jax.nn.silu(conv[:, :, chunk:]) * conv[:, :, :chunk]).astype(bf16)
    terms = jnp.dot(
        hidden.reshape(outer * rows, chunk), down_chunk, preferred_element_type=f32
    ).astype(bf16)
    summed = lax.psum_scatter(
        terms, "sp", scatter_dimension=0, tiled=True, axis_index_groups=outer_groups
    )
    summed = lax.psum_scatter(summed, "tp", scatter_dimension=1, tiled=True)
    my_heads = lax.dynamic_slice_in_dim(head_group, my_outer * rows, rows, axis=0)
    own = residual_in.astype(f32) + jnp.dot(
        my_heads, out_weight, preferred_element_type=f32
    )
    return (own + summed.astype(f32)).astype(bf16)


def fits(mesh, residual_in, query_pre, *arrays):
    depth, half = arrays[7].shape
    extra = half // OUTER % LANES
    return (
        mesh.shape["sp"] == INNER * OUTER
        and mesh.shape["tp"] == 2
        and depth == LANES
        and residual_in.shape == (LANES, depth * INNER * OUTER // 2)
        and query_pre.shape[1] % LANES == 0
        and half % LANES == 0
        and extra in (0, LANES // 2)
    )


def solution(mesh):
    rows = P(("grp", "sp"), "tp")

    def layer(*arrays):
        return (fused_layer if fits(mesh, *arrays) else on_device)(*arrays)

    return jax.shard_map(
        layer,
        mesh=mesh,
        in_specs=(
            rows,
            rows,
            rows,
            rows,
            rows,
            P("tp"),
            P(),
            P(None, "tp"),
            P("tp"),
            P("sp", "tp"),
            P("sp", "tp"),
            P(None, "tp"),
            P(None, "tp"),
            P("tp", "sp"),
        ),
        out_specs=rows,
        check_vma=False,
    )
```

```python
import functools

import jax
import jax.numpy as jnp
from jax import lax
from jax.experimental import pallas as pl
from jax.experimental.pallas import tpu as pltpu
from jax.sharding import PartitionSpec as P

DK = 64
SUB = 16
LANES = 128
INNER = 4
OUTER = 4
epsilon = 1e-06
highest = lax.Precision.HIGHEST
f32 = jnp.float32
bf16 = jnp.bfloat16
MESH = pl.DeviceIdType.MESH


def dot_nt(a, b):
    return lax.dot_general(
        a, b, (((1,), (1,)), ((), ())), precision=highest, preferred_element_type=f32
    )


def dot_hi(a, b):
    return jnp.dot(a, b, precision=highest, preferred_element_type=f32)


def gate(v):
    return v / (1.0 + jnp.exp(-v))


def turn(v):
    return jnp.concatenate([v[:, DK:], v[:, :DK]], axis=1)


def layer_kernel(
    full,
    extra,
    residual_ref,
    query_ref,
    forget_ref,
    value_ref,
    gate_ref,
    floor_ref,
    head_gain_ref,
    out_weight_ref,
    norm_gain_ref,
    value_weight_ref,
    gate_weight_ref,
    value_taps_ref,
    gate_taps_ref,
    down_ref,
    out_ref,
    up_in,
    dn_in,
    taps,
    up,
    dn,
    st,
    zt,
    inner_buf,
    start_buf,
    ho,
    sq,
    stream,
    nb,
    ubuf,
    tail_s,
    tail_r,
    hid,
    acc,
    xs,
    xr,
    zs,
    zr,
    ssem,
    up_r,
    dn_r,
    st_r,
    zt_r,
    zt_s,
    go,
    nb_r,
    xr_r,
    zr_r,
    misc_r,
):
    s = lax.axis_index("sp")
    x = lax.axis_index("tp")
    z = s // INNER
    i = s % INNER
    c = s % 2
    ox = 1 - x
    ic = i + 1 - 2 * c
    iy = (i + 2) % INNER
    idg = (ic + 2) % INNER
    z1 = z + 1 - 2 * (z % 2)
    z2 = (z + 2) % OUTER
    z3 = OUTER - 1 - z
    chunk = full + extra
    depth = up.shape[1]
    rows = query_ref.shape[0]
    width = query_ref.shape[1]
    pairs = width // LANES
    pending = []

    def at(zz, ii, xx=x):
        return {"sp": zz * INNER + ii, "tp": xx}

    def send(src, dst, rsem, device, first=None):
        copy = pltpu.make_async_remote_copy(
            src_ref=src,
            dst_ref=dst,
            send_sem=ssem.at[len(pending)],
            recv_sem=rsem,
            device_id=device,
            device_id_type=MESH,
        )
        pending.append(copy)
        if first is None:
            copy.start()
        elif first is not False:
            pl.when(first)(copy.start)
        return copy

    def arrived(dst, rsem):
        pltpu.make_async_remote_copy(
            src_ref=dst,
            dst_ref=dst,
            send_sem=ssem.at[0],
            recv_sem=rsem,
            device_id=at(z, ic),
            device_id_type=MESH,
        ).wait_recv()

    barrier = pltpu.get_barrier_semaphore()
    peers = [at((z + k) % OUTER, i) for k in range(1, OUTER)]
    peers += [at(z, ic), at(z, iy), at(z, idg), at(z, i, ox)]
    for peer in peers:
        pl.semaphore_signal(barrier, inc=1, device_id=peer, device_id_type=MESH)

    def up_slot(zz, ii):
        return up.at[zz * INNER + ii], up_r.at[zz * INNER + ii]

    def dn_slot(zz, ii):
        slot = dn.at[zz * INNER + ii, pl.ds(0, chunk)]
        return slot, dn_r.at[zz * INNER + ii]

    def send_z(source, slot, zz, first=None):
        dst, sem = slot(z, i)
        return send(source.at[zz], dst, sem, at(zz, i), first)

    def forward_yc(slot, zz, source=None):
        dst, sem = slot(zz, i)
        if source is None:
            arrived(dst, sem)
            source = dst
        send(source, dst, sem, at(z, iy))
        send(source, dst, sem, at(z, ic))

    def prepare_yc(slot, zz):
        dst, sem = slot(zz, i)
        copies = [send(dst, dst, sem, at(z, ii), False) for ii in (iy, ic)]

        def run():
            arrived(dst, sem)
            for copy in copies:
                copy.start()

        return run

    def forward_c(slot, zz):
        dst, sem = slot(zz, iy)
        arrived(dst, sem)
        send(dst, dst, sem, at(z, ic))

    keys = floor_ref[...] * jax.nn.sigmoid(-forget_ref[...].astype(f32))
    query = gate(query_ref[...].astype(f32))
    values = value_ref[...].astype(f32)
    position = lax.broadcasted_iota(jnp.int32, (rows, rows), 0)
    earlier = lax.broadcasted_iota(jnp.int32, (rows, rows), 1)
    running = dot_hi((position >= earlier).astype(f32), jnp.log1p(-keys))
    ending = running[rows - 1 : rows]
    kept = keys * jnp.exp(ending - running)
    turned = values.T
    low = lax.broadcasted_iota(jnp.int32, (1, LANES), 1) < DK
    part_row = lax.broadcasted_iota(jnp.int32, (SUB, width), 0)

    def store_state(ref, state, decay):
        ref[0:DK] = state.astype(bf16)
        one = decay.astype(bf16).astype(f32)
        two = (decay - one).astype(bf16).astype(f32)
        three = decay - one - two
        parts = jnp.where(part_row == 1, two, jnp.where(part_row == 2, three, 0.0))
        ref[DK : DK + SUB] = jnp.where(part_row == 0, one, parts).astype(bf16)

    def load_state(ref):
        parts = ref[DK : DK + SUB].astype(f32)
        return ref[0:DK].astype(f32), parts[0:1] + parts[1:2] + parts[2:3]

    states = []
    for p in range(pairs):
        lanes = slice(p * LANES, (p + 1) * LANES)
        both = dot_hi(turned[lanes], kept[:, lanes])
        states.append(jnp.where(low, both[:DK], both[DK:]))
    store_state(st.at[i], jnp.concatenate(states, axis=1), jnp.exp(ending))
    for o in range(OUTER):
        main = slice(o * full, (o + 1) * full)
        up_in[o, :, 0:full] = value_weight_ref[:, main]
        up_in[o, :, full : 2 * full] = gate_weight_ref[:, main]
        dn_in[o, 0:full] = down_ref[main]
        if extra:
            start = OUTER * full + o * extra
            dn_in[o, full:chunk] = down_ref[start : start + extra]
    if extra:
        for o in range(0, OUTER, 2):
            start = OUTER * full + o * extra
            tile = slice(start, start + LANES)
            v = value_weight_ref[:, tile].astype(f32)
            g = gate_weight_ref[:, tile].astype(f32)
            end = slice(2 * full, 2 * full + LANES)
            up_in[o, :, end] = jnp.where(low, v, turn(g)).astype(bf16)
            up_in[o + 1, :, end] = jnp.where(low, turn(v), g).astype(bf16)

    pl.semaphore_wait(barrier, len(peers))
    for ii in (idg, iy, ic):
        send(st.at[i], st.at[i], st_r.at[i], at(z, ii))
    far = send_z(up_in, up_slot, z2, z == 3)
    near = send_z(up_in, up_slot, z1, z % 2 == 1)
    near_dn = send_z(dn_in, dn_slot, z1, z % 2 == 0)
    last_dn = send_z(dn_in, dn_slot, z3, z == 1)

    up[s] = up_in[z]
    dn[s, 0:chunk] = dn_in[z]
    spare = dn.shape[1] - chunk
    if spare:
        for b in range(INNER * OUTER):
            dn[b, chunk:] = jnp.zeros((spare, dn.shape[2]), bf16)
    start_buf[...] = query * jnp.exp(running)

    for ii in (ic, iy, idg):
        arrived(st.at[ii], st_r.at[ii])
    total = jnp.zeros((DK, width), f32)
    mine = jnp.zeros((DK, width), f32)
    total_decay = jnp.ones((1, width), f32)
    my_decay = jnp.ones((1, width), f32)
    for j in range(INNER):
        fresh, decay = load_state(st.at[j])
        mine = jnp.where(j < i, mine * decay + fresh, mine)
        my_decay = jnp.where(j < i, my_decay * decay, my_decay)
        total = total * decay + fresh
        total_decay = total_decay * decay
    store_state(zt.at[z], total, total_decay)
    totals = []
    for k in range(1, OUTER):
        totals.append(
            pltpu.make_async_remote_copy(
                src_ref=zt.at[z],
                dst_ref=zt.at[z],
                send_sem=zt_s.at[k],
                recv_sem=zt_r.at[z],
                device_id=at((z + k) % OUTER, i),
                device_id_type=MESH,
            )
        )
    for k in (3, 2, 1):
        pl.when(z + k < OUTER)(totals[k - 1].start)
    pl.when(z == 2)(near.start)
    forward_yc(up_slot, z, up_in.at[z])
    forward_yc(dn_slot, z, dn_in.at[z])

    cells = [[] for _ in range(pairs)]
    row_of = lax.broadcasted_iota(jnp.int32, (rows, width), 0)
    column = lax.broadcasted_iota(jnp.int32, (2 * SUB, rows), 1)
    stacked = lax.broadcasted_iota(jnp.int32, (2 * SUB, rows), 0) % SUB
    for n in range(rows // SUB):
        part = slice(n * SUB, (n + 1) * SUB)
        middle = running[n * SUB + SUB // 2 - 1 : n * SUB + SUB // 2]
        query_part = query[part] * jnp.exp(running[part] - middle)
        reach = jnp.where(row_of < (n + 1) * SUB, middle - running, -jnp.inf)
        key_part = keys * jnp.exp(reach)
        for p in range(pairs):
            lanes = slice(p * LANES, (p + 1) * LANES)
            piece = query_part[:, lanes]
            piece = jnp.concatenate(
                [jnp.where(low, piece, 0.0), jnp.where(low, 0.0, piece)], axis=0
            )
            score = dot_nt(piece, key_part[:, lanes])
            score = jnp.where(stacked + n * SUB >= column, score, 0.0)
            cells[p].append(score)
    for p in range(pairs):
        lanes = slice(p * LANES, (p + 1) * LANES)
        scores = jnp.concatenate(
            [cell[:SUB] for cell in cells[p]] + [cell[SUB:] for cell in cells[p]],
            axis=0,
        )
        result = dot_hi(scores, values[:, lanes])
        inner_buf[:, lanes] = jnp.where(low, result[:rows], result[rows:])

    for k, copy in enumerate(totals, 1):
        pl.when(z + k < OUTER)(copy.wait_send)

    @pl.when(z == 1)
    def _():
        pl.semaphore_signal(go, inc=1, device_id=at(z1, i), device_id_type=MESH)

    pl.when(z == 2)(far.start)
    gain = jnp.concatenate([head_gain_ref[...]] * (LANES // DK), axis=1)
    gating = gate(gate_ref[...].astype(f32))
    for k in range(1, OUTER):
        zz = (z + OUTER - k) % OUTER
        pl.when(z >= k)(functools.partial(arrived, zt.at[zz], zt_r.at[zz]))
    entering = jnp.zeros((DK, width), f32)
    for j in range(OUTER - 1):
        fresh, decay = load_state(zt.at[j])
        entering = jnp.where(j < z, entering * decay + fresh, entering)
    entering = entering * my_decay + mine
    same_head = (
        lax.broadcasted_iota(jnp.int32, (LANES, LANES), 0) // DK
        == lax.broadcasted_iota(jnp.int32, (LANES, LANES), 1) // DK
    ).astype(f32)
    for p in range(pairs):
        lanes = slice(p * LANES, (p + 1) * LANES)
        piece = entering[:, lanes]
        piece = jnp.concatenate(
            [jnp.where(low, piece, 0.0), jnp.where(low, 0.0, piece)], axis=0
        )
        recurrent = inner_buf[:, lanes] + dot_nt(start_buf[:, lanes], piece)
        squares = dot_hi(recurrent * recurrent, same_head) * (1.0 / DK)
        scaled = recurrent * lax.rsqrt(squares + epsilon) * gain
        ho[x, :, lanes] = (scaled * gating[:, lanes]).astype(bf16)
    send(ho.at[x], ho.at[x], misc_r.at[0], at(z, i, ox))

    @pl.when(z == 0)
    def _():
        pl.semaphore_wait(go, 1)
        far.start()


    arrived(ho.at[ox], misc_r.at[0])
    pl.when(z == 1)(far.start)
    heads = jnp.concatenate([ho[0], ho[1]], axis=1)
    stream[...] = residual_ref[...].astype(f32) + jnp.dot(
        heads, out_weight_ref[...], preferred_element_type=f32
    )
    partial = jnp.sum(stream[...] * stream[...], axis=1, keepdims=True)
    sq[x] = jnp.broadcast_to(partial, (rows, LANES))
    send(sq.at[x], sq.at[x], misc_r.at[1], at(z, i, ox))
    arrived(sq.at[ox], misc_r.at[1])
    channels = 2 * stream.shape[1]
    mean = (sq[0][:, 0:1] + sq[1][:, 0:1]) * (1.0 / channels)
    normed = stream[...] * lax.rsqrt(mean + epsilon) * norm_gain_ref[...]
    nb[z, x] = normed.astype(bf16)

    def nb_slot(zz, xx):
        return nb.at[zz, xx], nb_r.at[zz * 2 + xx]

    def share(zz, devices, first=None):
        dst, sem = nb_slot(zz, x)
        return [send(dst, dst, sem, device, first) for device in devices]

    share(z, [at(z2, i), at(z1, i), at(z, i, ox)])
    pl.when(z == 0)(near.start)
    cross = send_z(up_in, up_slot, z3, z > 0)
    pl.when(z % 2 == 1)(near_dn.start)
    forward_c(up_slot, z)
    forward_c(dn_slot, z)
    early_dn = prepare_yc(dn_slot, z1)
    pl.when(z % 2 == 1)(early_dn)
    forward_yc(up_slot, z2)

    pl.when(z == 1)(functools.partial(arrived, *nb_slot(z2, x)))
    passed = share(z2, [at(z1, i), at(z, i, ox)], z == 1)
    arrived(*nb_slot(z1, x))
    share(z1, [at(z, i, ox)])

    @pl.when(z != 1)
    def _():
        arrived(*nb_slot(z2, x))
        for copy in passed:
            copy.start()

    forward_yc(up_slot, z1)
    forward_c(up_slot, z2)
    arrived(*nb_slot(z3, x))
    share(z3, [at(z, i, ox)])
    pl.when(z == 0)(cross.start)
    forward_c(up_slot, z1)
    forward_yc(up_slot, z3)
    send_z(dn_in, dn_slot, z2)
    pl.when(z % 2 == 0)(early_dn)
    later_dn = prepare_yc(dn_slot, z2)
    pl.when(z % 3 == 0)(later_dn)
    forward_c(up_slot, z3)
    pl.when(z != 1)(last_dn.start)

    for zz in range(OUTER):
        arrived(*up_slot(zz, ic))
        arrived(*up_slot(zz, idg))
        arrived(*nb_slot(zz, ox))

    mine_at = pl.ds(pl.multiple_of(z * full, LANES), full)
    taps[:, 0:full] = value_taps_ref[:, mine_at]
    taps[:, full : 2 * full] = gate_taps_ref[:, mine_at]
    if extra:
        tile = pl.ds(pl.multiple_of(OUTER * full + z // 2 * LANES, LANES), LANES)
        v = value_taps_ref[:, tile]
        g = gate_taps_ref[:, tile]
        v = jnp.where(z % 2 == 0, v, turn(v))
        g = jnp.where(z % 2 == 0, turn(g), g)
        taps[:, 2 * full : 2 * full + LANES] = jnp.where(low, v, g)

    count = OUTER * rows
    half = nb.shape[3]
    deep = half // up.shape[1]
    first = nb[:, 0].reshape(count, half)
    second = nb[:, 1].reshape(count, half)
    span = up.shape[2]
    step = 2 * LANES
    for low_lane in range(0, span, step):
        lanes = slice(low_lane, min(span, low_lane + step))
        size = lanes.stop - lanes.start
        product = jnp.dot(
            first, up[0:deep, :, lanes].reshape(half, size), preferred_element_type=f32
        ) + jnp.dot(
            second,
            up[deep : 2 * deep, :, lanes].reshape(half, size),
            preferred_element_type=f32,
        )
        ubuf[:, 8:, lanes] = (
            product.astype(bf16).astype(f32).reshape(OUTER, rows, size)
        )
    for b in range(OUTER):
        tail_s[2 * b : 2 * b + 2] = ubuf[b, rows + 6 : rows + 8]
    after = z * INNER + (i + 1) % INNER
    send(tail_s, tail_r, misc_r.at[2], {"sp": after, "tp": x})

    forward_c(dn_slot, z1)
    pl.when(z % 3 != 0)(later_dn)
    forward_yc(dn_slot, z3)

    arrived(tail_r, misc_r.at[2])
    for b in range(OUTER):
        wrapped = tail_r[2 * b - 2 : 2 * b] if b else jnp.zeros((2, span), f32)
        ubuf[b, 6:8] = jnp.where(i == 0, wrapped, tail_r[2 * b : 2 * b + 2])

    def conv(b, lanes):
        return (
            taps[0:1, lanes] * ubuf[b, pl.ds(6, rows), lanes]
            + taps[1:2, lanes] * ubuf[b, pl.ds(7, rows), lanes]
            + taps[2:3, lanes] * ubuf[b, pl.ds(8, rows), lanes]
        )

    @pl.loop(0, OUTER)
    def _(b):
        for t in range(full // LANES):
            lanes = slice(t * LANES, (t + 1) * LANES)
            other = slice(full + t * LANES, full + (t + 1) * LANES)
            hid[b, :, lanes] = (gate(conv(b, other)) * conv(b, lanes)).astype(bf16)
        if extra:
            mixed = conv(b, slice(2 * full, 2 * full + LANES))
            turned_half = turn(mixed)
            last = jnp.where(low, gate(turned_half) * mixed, 0.0)
            hid[b, :, full : full + LANES] = last.astype(bf16)

    forward_c(dn_slot, z2)
    forward_c(dn_slot, z3)
    for zz in range(OUTER):
        arrived(*dn_slot(zz, ic))
        arrived(*dn_slot(zz, idg))

    def columns(zz, base, store, part):
        each = deep // 4
        for j in range(part * each, (part + 1) * each):
            weight = jnp.concatenate(
                [dn[base + 2 * j], dn[base + 2 * j + 1]], axis=1
            )
            product = jnp.dot(hid[zz], weight, preferred_element_type=f32)
            store[zz, :, j * step : (j + 1) * step] = product.astype(store.dtype)

    sides = [slice(0, half // 2), slice(half // 2, half)]

    def send_part(src, dst, sem, slot, part, device):
        side = sides[part]
        send(src.at[slot, :, side], dst.at[slot, :, side], sem.at[slot, part], device)

    phase = len(pending)
    order = [(z3, 0), (z2, 0), (z3, 1), (z2, 1), (z1, 0), (z1, 1), (z, 0), (z, 1)]
    for zz, part in order:
        columns(zz, ox * deep, xs, part)
        send_part(xs, xr, xr_r, zz, part, at(z, i, ox))

    for copy in pending[:phase]:
        copy.wait_send()

    def summed(zz, part):
        side = sides[part]
        columns(zz, x * deep, acc, part)
        arrived(xr.at[zz, :, side], xr_r.at[zz, part])
        return acc[zz, :, side] + xr[zz, :, side].astype(f32)

    def received(slot, part):
        side = sides[part]
        arrived(zr.at[slot, :, side], zr_r.at[slot, part])
        return zr[slot, :, side].astype(f32)

    def pass_on(slot, part, value, device):
        zs[slot, :, sides[part]] = value.astype(bf16)
        send_part(zs, zr, zr_r, slot, part, device)

    pass_on(0, 0, summed(z3, 0), at(z1, i))
    value = summed(z2, 0)
    pass_on(2, 0, value + received(0, 0), at(z2, i))
    pass_on(0, 1, summed(z3, 1), at(z1, i))
    value = summed(z2, 1)
    pass_on(2, 1, value + received(0, 1), at(z2, i))
    for part in range(2):
        pass_on(1, part, summed(z1, part), at(z1, i))
    for part in range(2):
        side = sides[part]
        own = summed(z, part) + received(1, part) + received(2, part)
        out_ref[:, side] = (stream[:, side] + own).astype(bf16)

    for copy in pending[phase:]:
        copy.wait_send()


def fused_layer(
    residual_in,
    query_pre,
    forget_pre,
    value_pre,
    gate_pre,
    floor_gap,
    head_gain,
    out_weight,
    norm_gain,
    value_weight,
    gate_weight,
    value_taps,
    gate_taps,
    down_weight,
):
    rows, my_width = residual_in.shape
    depth, half = value_weight.shape
    width = query_pre.shape[1]
    blocks = INNER * OUTER
    full = half // LANES // OUTER * LANES
    extra = half // OUTER - full
    chunk = full + extra
    padded = full + (LANES if extra else 0)

    dma = pltpu.SemaphoreType.DMA
    vmem = pl.BlockSpec(memory_space=pltpu.VMEM)
    span = 2 * chunk
    return pl.pallas_call(
        functools.partial(layer_kernel, full, extra),
        out_shape=jax.ShapeDtypeStruct((rows, my_width), bf16),
        in_specs=[vmem] * 14,
        out_specs=vmem,
        scratch_shapes=[
            pltpu.VMEM((OUTER, depth, span), bf16),
            pltpu.VMEM((OUTER, chunk, depth), bf16),
            pltpu.VMEM((value_taps.shape[0], span), f32),
            pltpu.VMEM((blocks, depth, span), bf16),
            pltpu.VMEM((blocks, padded, depth), bf16),
            pltpu.VMEM((INNER, DK + SUB, width), bf16),
            pltpu.VMEM((OUTER, DK + SUB, width), bf16),
            pltpu.VMEM((rows, width), f32),
            pltpu.VMEM((rows, width), f32),
            pltpu.VMEM((2, rows, width), bf16),
            pltpu.VMEM((2, rows, LANES), f32),
            pltpu.VMEM((rows, my_width), f32),
            pltpu.VMEM((OUTER, 2, rows, my_width), bf16),
            pltpu.VMEM((OUTER, rows + 8, span), f32),
            pltpu.VMEM((2 * OUTER, span), f32),
            pltpu.VMEM((2 * OUTER, span), f32),
            pltpu.VMEM((OUTER, rows, padded), bf16),
            pltpu.VMEM((OUTER, rows, my_width), f32),
            pltpu.VMEM((OUTER, rows, my_width), bf16),
            pltpu.VMEM((OUTER, rows, my_width), bf16),
            pltpu.VMEM((3, rows, my_width), bf16),
            pltpu.VMEM((3, rows, my_width), bf16),
            dma((80,)),
            dma((blocks,)),
            dma((blocks,)),
            dma((INNER,)),
            dma((OUTER,)),
            dma((OUTER,)),
            pltpu.SemaphoreType.REGULAR,
            dma((2 * OUTER,)),
            dma((OUTER, 2)),
            dma((3, 2)),
            dma((3,)),
        ],
        compiler_params=pltpu.CompilerParams(
            collective_id=0, has_side_effects=True, vmem_limit_bytes=56 * 2**20
        ),
        name="layer",
    )(
        residual_in,
        query_pre,
        forget_pre,
        value_pre,
        gate_pre,
        floor_gap[None],
        head_gain[None],
        out_weight,
        norm_gain[None],
        value_weight,
        gate_weight,
        value_taps,
        gate_taps,
        down_weight,
    )


def local_recurrence(query_pre, forget_pre, value_pre, floor_gap):
    rows, width = query_pre.shape
    heads = width // DK
    subs = rows // SUB
    keys = floor_gap * jax.nn.sigmoid(-forget_pre.astype(f32))
    log_decay = jnp.log1p(-keys)
    query = jax.nn.silu(query_pre.astype(f32))
    values = value_pre.astype(f32)
    position = lax.iota(jnp.int32, rows)
    lower = (position[:, None] >= position[None, :]).astype(f32)
    running = jnp.dot(lower, log_decay, precision=highest)
    middle = running.reshape(subs, SUB, width)[:, SUB // 2 - 1, :]
    query_part = query * jnp.exp(running - jnp.repeat(middle, SUB, axis=0))
    reach = (lax.iota(jnp.int32, subs) + 1) * SUB
    seen = position[None, :, None] < reach[:, None, None]
    key_part = keys[None] * jnp.exp(
        jnp.where(seen, middle[:, None, :] - running[None], -jnp.inf)
    )
    scores = jnp.einsum(
        "ithk,ishk->hits",
        query_part.reshape(subs, SUB, heads, DK),
        key_part.reshape(subs, rows, heads, DK),
        precision=highest,
    ).reshape(heads, rows, rows)
    scores = jnp.where(position[None, :, None] >= position[None, None, :], scores, 0.0)
    value_heads = values.reshape(rows, heads, DK)
    inner = jnp.einsum("hts,shv->htv", scores, value_heads, precision=highest)
    ending = running[-1]
    state = jnp.einsum(
        "shv,shk->vhk",
        value_heads,
        (keys * jnp.exp(ending - running)).reshape(rows, heads, DK),
        precision=highest,
    ).reshape(DK, width)
    from_start = (query * jnp.exp(running)).reshape(rows, heads, DK)
    return inner, state, jnp.exp(ending), from_start


def causal_taps(before, current, taps):
    padded = jnp.concatenate([before, current], axis=1).astype(f32)
    rows = current.shape[1]
    return (
        taps[0] * padded[:, 0:rows]
        + taps[1] * padded[:, 1 : rows + 1]
        + taps[2] * padded[:, 2 : rows + 2]
    )


def on_device(
    residual_in,
    query_pre,
    forget_pre,
    value_pre,
    gate_pre,
    floor_gap,
    head_gain,
    out_weight,
    norm_gain,
    value_weight,
    gate_weight,
    value_taps,
    gate_taps,
    down_weight,
):
    sp = lax.axis_size("sp")
    tp = lax.axis_size("tp")
    inner_size = 4 if sp % 4 == 0 else 1
    outer = sp // inner_size
    me = lax.axis_index("sp")
    my_outer = me // inner_size
    my_inner = me % inner_size
    outer_groups = [[o * inner_size + i for o in range(outer)] for i in range(inner_size)]
    inner_groups = [[o * inner_size + i for i in range(inner_size)] for o in range(outer)]
    rows, my_width = residual_in.shape
    width = my_width * tp
    depth, half = value_weight.shape
    chunk = half // outer

    wide_groups = [
        [s * tp + t for s in group for t in range(tp)] for group in outer_groups
    ]

    def exchange(array):
        return lax.all_to_all(
            array, "sp", 0, 0, axis_index_groups=outer_groups, tiled=True
        )

    def gather_inner(array):
        return lax.all_gather(array, "sp", axis_index_groups=inner_groups)

    def gather_wide(array):
        gathered = lax.all_gather(array, ("sp", "tp"), axis_index_groups=wide_groups)
        gathered = gathered.reshape(outer, tp, *array.shape)
        return [gathered[:, t].reshape(-1, array.shape[1]) for t in range(tp)]

    def reorder(pieces):
        span = pieces[0].shape[-1]
        blocks = []
        for i in range(inner_size):
            for o in range(outer):
                start = (o * inner_size + i) * depth
                low = start % span
                blocks.append(pieces[start // span][..., low : low + depth])
        return lax.optimization_barrier(jnp.concatenate(blocks, axis=-1))

    up_parts = jnp.stack(
        [
            jnp.concatenate(
                [
                    value_weight[:, o * chunk : (o + 1) * chunk],
                    gate_weight[:, o * chunk : (o + 1) * chunk],
                ],
                axis=1,
            )
            for o in range(outer)
        ]
    )
    up_chunk = gather_inner(exchange(up_parts)).reshape(width, 2 * chunk)
    down_parts = down_weight.reshape(outer, chunk, depth)
    down_mine = gather_inner(exchange(down_parts))
    down_chunk = down_mine.transpose(2, 1, 0, 3).reshape(chunk, width)

    out_full = reorder(list(lax.all_gather(out_weight, "tp")))
    gain_full = reorder(list(lax.all_gather(norm_gain, "tp")))
    residual_group = reorder(gather_wide(residual_in))

    inner, state, total_decay, from_start = local_recurrence(
        query_pre, forget_pre, value_pre, floor_gap
    )
    heads = inner.shape[0]
    first = total_decay.astype(bf16)
    rest = total_decay - first.astype(f32)
    second = rest.astype(bf16)
    third = (rest - second.astype(f32)).astype(bf16)
    spare = jnp.zeros((13, heads * DK), bf16)
    packed = jnp.concatenate(
        [state.astype(bf16), first[None], second[None], third[None], spare], axis=0
    )
    everyone = lax.all_gather(packed, "sp").astype(f32)
    decays = everyone[:, DK] + everyone[:, DK + 1] + everyone[:, DK + 2]
    entering = jnp.zeros_like(state)
    for j in range(sp - 1):
        advanced = entering * decays[j] + everyone[j, :DK]
        entering = jnp.where(j < me, advanced, entering)
    carried = jnp.einsum(
        "thk,vhk->htv", from_start, entering.reshape(DK, heads, DK), precision=highest
    )
    recurrent = (inner + carried).transpose(1, 0, 2)
    scaled = (
        recurrent
        * lax.rsqrt(jnp.mean(recurrent * recurrent, axis=-1, keepdims=True) + epsilon)
        * head_gain
    )
    gating = jax.nn.silu(gate_pre.astype(f32)).reshape(recurrent.shape)
    head_out = (scaled * gating).reshape(rows, heads * DK).astype(bf16)

    head_out, out_full = lax.optimization_barrier((head_out, out_full))
    head_group = jnp.concatenate(gather_wide(head_out), axis=1)
    stream = residual_group.astype(f32) + jnp.dot(
        head_group, out_full, preferred_element_type=f32
    )
    squares = jnp.mean(stream * stream, axis=1, keepdims=True)
    normed = (stream * lax.rsqrt(squares + epsilon) * gain_full).astype(bf16)
    up = jnp.dot(normed, up_chunk, preferred_element_type=f32).astype(bf16)
    up = up.reshape(outer, rows, 2 * chunk)
    tails = up[:, rows - 2 :]
    pairs = [
        (o * inner_size + i, o * inner_size + (i + 1) % inner_size)
        for o in range(outer)
        for i in range(inner_size)
    ]
    arrived = lax.ppermute(tails, "sp", pairs) if inner_size > 1 else tails
    wrapped = jnp.concatenate([jnp.zeros_like(arrived[:1]), arrived[:-1]], axis=0)
    before = jnp.where(my_inner == 0, wrapped, arrived)

    taps = jnp.concatenate(
        [
            lax.dynamic_slice_in_dim(value_taps, my_outer * chunk, chunk, axis=1),
            lax.dynamic_slice_in_dim(gate_taps, my_outer * chunk, chunk, axis=1),
        ],
        axis=1,
    )
    conv = causal_taps(before, up, taps)
    hidden = (jax.nn.silu(conv[:, :, chunk:]) * conv[:, :, :chunk]).astype(bf16)
    terms = jnp.dot(
        hidden.reshape(outer * rows, chunk), down_chunk, preferred_element_type=f32
    ).astype(bf16)
    summed = lax.psum_scatter(
        terms, "sp", scatter_dimension=0, tiled=True, axis_index_groups=outer_groups
    )
    summed = lax.psum_scatter(summed, "tp", scatter_dimension=1, tiled=True)
    my_heads = lax.dynamic_slice_in_dim(head_group, my_outer * rows, rows, axis=0)
    own = residual_in.astype(f32) + jnp.dot(
        my_heads, out_weight, preferred_element_type=f32
    )
    return (own + summed.astype(f32)).astype(bf16)


def fits(mesh, residual_in, query_pre, *arrays):
    depth, half = arrays[7].shape
    extra = half // OUTER % LANES
    return (
        mesh.shape["sp"] == INNER * OUTER
        and mesh.shape["tp"] == 2
        and depth == LANES
        and residual_in.shape == (LANES, depth * INNER * OUTER // 2)
        and query_pre.shape[1] % LANES == 0
        and half % LANES == 0
        and extra in (0, LANES // 2)
    )


def solution(mesh):
    rows = P(("grp", "sp"), "tp")

    def layer(*arrays):
        return (fused_layer if fits(mesh, *arrays) else on_device)(*arrays)

    return jax.shard_map(
        layer,
        mesh=mesh,
        in_specs=(
            rows,
            rows,
            rows,
            rows,
            rows,
            P("tp"),
            P(),
            P(None, "tp"),
            P("tp"),
            P("sp", "tp"),
            P("sp", "tp"),
            P(None, "tp"),
            P(None, "tp"),
            P("tp", "sp"),
        ),
        out_specs=rows,
        check_vma=False,
    )
```

```python
import functools

import jax
import jax.numpy as jnp
from jax import lax
from jax.experimental import pallas as pl
from jax.experimental.pallas import tpu as pltpu
from jax.sharding import PartitionSpec as P

DK = 64
SUB = 16
LANES = 128
INNER = 4
OUTER = 4
epsilon = 1e-06
highest = lax.Precision.HIGHEST
f32 = jnp.float32
bf16 = jnp.bfloat16
MESH = pl.DeviceIdType.MESH


def dot_nt(a, b):
    return lax.dot_general(
        a, b, (((1,), (1,)), ((), ())), precision=highest, preferred_element_type=f32
    )


def dot_hi(a, b):
    return jnp.dot(a, b, precision=highest, preferred_element_type=f32)


def gate(v):
    return v / (1.0 + jnp.exp(-v))


def turn(v):
    return jnp.concatenate([v[:, DK:], v[:, :DK]], axis=1)


def layer_kernel(
    full,
    extra,
    residual_ref,
    query_ref,
    forget_ref,
    value_ref,
    gate_ref,
    floor_ref,
    head_gain_ref,
    out_weight_ref,
    norm_gain_ref,
    value_weight_ref,
    gate_weight_ref,
    value_taps_ref,
    gate_taps_ref,
    down_ref,
    out_ref,
    up_in,
    dn_in,
    taps,
    up,
    dn,
    st,
    zt,
    inner_buf,
    start_buf,
    ho,
    sq,
    stream,
    nb,
    ubuf,
    tail_s,
    tail_r,
    hid,
    xs,
    xr,
    zs,
    zr,
    zbs,
    zbr,
    xbs,
    xbr,
    ssem,
    up_r,
    dn_r,
    st_r,
    zt_r,
    zt_s,
    go,
    nb_r,
    xr_r,
    zr_r,
    zb_r,
    misc_r,
):
    s = lax.axis_index("sp")
    x = lax.axis_index("tp")
    z = s // INNER
    i = s % INNER
    c = s % 2
    ox = 1 - x
    ic = i + 1 - 2 * c
    iy = (i + 2) % INNER
    idg = (ic + 2) % INNER
    z1 = z + 1 - 2 * (z % 2)
    z2 = (z + 2) % OUTER
    z3 = OUTER - 1 - z
    chunk = full + extra
    depth = up.shape[1]
    rows = query_ref.shape[0]
    width = query_ref.shape[1]
    pairs = width // LANES
    pending = []

    def at(zz, ii, xx=x):
        return {"sp": zz * INNER + ii, "tp": xx}

    def send(src, dst, rsem, device, first=None):
        copy = pltpu.make_async_remote_copy(
            src_ref=src,
            dst_ref=dst,
            send_sem=ssem.at[len(pending)],
            recv_sem=rsem,
            device_id=device,
            device_id_type=MESH,
        )
        pending.append(copy)
        if first is None:
            copy.start()
        elif first is not False:
            pl.when(first)(copy.start)
        return copy

    def arrived(dst, rsem):
        pltpu.make_async_remote_copy(
            src_ref=dst,
            dst_ref=dst,
            send_sem=ssem.at[0],
            recv_sem=rsem,
            device_id=at(z, ic),
            device_id_type=MESH,
        ).wait_recv()

    barrier = pltpu.get_barrier_semaphore()
    peers = [at((z + k) % OUTER, i) for k in range(1, OUTER)]
    peers += [at(z, ic), at(z, iy), at(z, idg), at(z, i, ox)]
    for peer in peers:
        pl.semaphore_signal(barrier, inc=1, device_id=peer, device_id_type=MESH)

    def up_slot(zz, ii):
        return up.at[zz * INNER + ii], up_r.at[zz * INNER + ii]

    def dn_slot(zz, ii):
        slot = dn.at[zz * INNER + ii, pl.ds(0, chunk)]
        return slot, dn_r.at[zz * INNER + ii]

    def send_z(source, slot, zz, first=None):
        dst, sem = slot(z, i)
        return send(source.at[zz], dst, sem, at(zz, i), first)

    def forward_yc(slot, zz, source=None):
        dst, sem = slot(zz, i)
        if source is None:
            arrived(dst, sem)
            source = dst
        send(source, dst, sem, at(z, iy))
        send(source, dst, sem, at(z, ic))

    def send_half(part, first):
        dst, sem = up_slot(z, i)
        part_rows = pl.ds(part * (depth // 2), depth // 2)
        src = up_in.at[z3, part_rows]
        return send(src, dst.at[part_rows], sem, at(z3, i), first)

    def prepare_yc(slot, zz):
        dst, sem = slot(zz, i)
        copies = [send(dst, dst, sem, at(z, ii), False) for ii in (iy, ic)]

        def run():
            arrived(dst, sem)
            for copy in copies:
                copy.start()

        return run

    def forward_c(slot, zz):
        dst, sem = slot(zz, iy)
        arrived(dst, sem)
        send(dst, dst, sem, at(z, ic))

    keys = floor_ref[...] * jax.nn.sigmoid(-forget_ref[...].astype(f32))
    query = gate(query_ref[...].astype(f32))
    values = value_ref[...].astype(f32)
    position = lax.broadcasted_iota(jnp.int32, (rows, rows), 0)
    earlier = lax.broadcasted_iota(jnp.int32, (rows, rows), 1)
    running = dot_hi((position >= earlier).astype(f32), jnp.log1p(-keys))
    ending = running[rows - 1 : rows]
    kept = keys * jnp.exp(ending - running)
    turned = values.T
    low = lax.broadcasted_iota(jnp.int32, (1, LANES), 1) < DK
    part_row = lax.broadcasted_iota(jnp.int32, (SUB, width), 0)

    def store_state(ref, state, decay):
        ref[0:DK] = state.astype(bf16)
        one = decay.astype(bf16).astype(f32)
        two = (decay - one).astype(bf16).astype(f32)
        three = decay - one - two
        parts = jnp.where(part_row == 1, two, jnp.where(part_row == 2, three, 0.0))
        ref[DK : DK + SUB] = jnp.where(part_row == 0, one, parts).astype(bf16)

    def load_state(ref):
        parts = ref[DK : DK + SUB].astype(f32)
        return ref[0:DK].astype(f32), parts[0:1] + parts[1:2] + parts[2:3]

    states = []
    for p in range(pairs):
        lanes = slice(p * LANES, (p + 1) * LANES)
        both = dot_hi(turned[lanes], kept[:, lanes])
        states.append(jnp.where(low, both[:DK], both[DK:]))
    store_state(st.at[i], jnp.concatenate(states, axis=1), jnp.exp(ending))
    for o in range(OUTER):
        main = slice(o * full, (o + 1) * full)
        up_in[o, :, 0:full] = value_weight_ref[:, main]
        up_in[o, :, full : 2 * full] = gate_weight_ref[:, main]
        dn_in[o, 0:full] = down_ref[main]
        if extra:
            start = OUTER * full + o * extra
            dn_in[o, full:chunk] = down_ref[start : start + extra]
    if extra:
        for o in range(0, OUTER, 2):
            start = OUTER * full + o * extra
            tile = slice(start, start + LANES)
            v = value_weight_ref[:, tile].astype(f32)
            g = gate_weight_ref[:, tile].astype(f32)
            end = slice(2 * full, 2 * full + LANES)
            up_in[o, :, end] = jnp.where(low, v, turn(g)).astype(bf16)
            up_in[o + 1, :, end] = jnp.where(low, turn(v), g).astype(bf16)

    pl.semaphore_wait(barrier, len(peers))
    for ii in (idg, iy, ic):
        send(st.at[i], st.at[i], st_r.at[i], at(z, ii))
    far = send_z(up_in, up_slot, z2, z == 3)
    near = send_z(up_in, up_slot, z1, z % 2 == 1)
    cross = send_half(0, z == 0)
    near_dn = send_z(dn_in, dn_slot, z1, z == 0)

    up[s] = up_in[z]
    dn[s, 0:chunk] = dn_in[z]
    spare = dn.shape[1] - chunk
    if spare:
        for b in range(INNER * OUTER):
            dn[b, chunk:] = jnp.zeros((spare, dn.shape[2]), bf16)
    start_buf[...] = query * jnp.exp(running)

    for ii in (ic, iy, idg):
        arrived(st.at[ii], st_r.at[ii])
    total = jnp.zeros((DK, width), f32)
    mine = jnp.zeros((DK, width), f32)
    total_decay = jnp.ones((1, width), f32)
    my_decay = jnp.ones((1, width), f32)
    for j in range(INNER):
        fresh, decay = load_state(st.at[j])
        mine = jnp.where(j < i, mine * decay + fresh, mine)
        my_decay = jnp.where(j < i, my_decay * decay, my_decay)
        total = total * decay + fresh
        total_decay = total_decay * decay
    store_state(zt.at[z], total, total_decay)
    totals = []
    for k in range(1, OUTER):
        totals.append(
            pltpu.make_async_remote_copy(
                src_ref=zt.at[z],
                dst_ref=zt.at[z],
                send_sem=zt_s.at[k],
                recv_sem=zt_r.at[z],
                device_id=at((z + k) % OUTER, i),
                device_id_type=MESH,
            )
        )
    for k in (3, 2, 1):
        pl.when(z + k < OUTER)(totals[k - 1].start)
    pl.when(z == 2)(near_dn.start)
    pl.when(z == 2)(near.start)
    forward_yc(up_slot, z, up_in.at[z])
    forward_yc(dn_slot, z, dn_in.at[z])

    cells = [[] for _ in range(pairs)]
    row_of = lax.broadcasted_iota(jnp.int32, (rows, width), 0)
    column = lax.broadcasted_iota(jnp.int32, (2 * SUB, rows), 1)
    stacked = lax.broadcasted_iota(jnp.int32, (2 * SUB, rows), 0) % SUB
    for n in range(rows // SUB):
        part = slice(n * SUB, (n + 1) * SUB)
        middle = running[n * SUB + SUB // 2 - 1 : n * SUB + SUB // 2]
        query_part = query[part] * jnp.exp(running[part] - middle)
        reach = jnp.where(row_of < (n + 1) * SUB, middle - running, -jnp.inf)
        key_part = keys * jnp.exp(reach)
        for p in range(pairs):
            lanes = slice(p * LANES, (p + 1) * LANES)
            piece = query_part[:, lanes]
            piece = jnp.concatenate(
                [jnp.where(low, piece, 0.0), jnp.where(low, 0.0, piece)], axis=0
            )
            score = dot_nt(piece, key_part[:, lanes])
            score = jnp.where(stacked + n * SUB >= column, score, 0.0)
            cells[p].append(score)
    for p in range(pairs):
        lanes = slice(p * LANES, (p + 1) * LANES)
        scores = jnp.concatenate(
            [cell[:SUB] for cell in cells[p]] + [cell[SUB:] for cell in cells[p]],
            axis=0,
        )
        result = dot_hi(scores, values[:, lanes])
        inner_buf[:, lanes] = jnp.where(low, result[:rows], result[rows:])

    for k, copy in enumerate(totals, 1):
        pl.when(z + k < OUTER)(copy.wait_send)

    @pl.when(z == 1)
    def _():
        pl.semaphore_signal(go, inc=1, device_id=at(z1, i), device_id_type=MESH)

    pl.when(z == 2)(far.start)
    gain = jnp.concatenate([head_gain_ref[...]] * (LANES // DK), axis=1)
    gating = gate(gate_ref[...].astype(f32))
    for k in range(1, OUTER):
        zz = (z + OUTER - k) % OUTER
        pl.when(z >= k)(functools.partial(arrived, zt.at[zz], zt_r.at[zz]))
    entering = jnp.zeros((DK, width), f32)
    for j in range(OUTER - 1):
        fresh, decay = load_state(zt.at[j])
        entering = jnp.where(j < z, entering * decay + fresh, entering)
    entering = entering * my_decay + mine
    same_head = (
        lax.broadcasted_iota(jnp.int32, (LANES, LANES), 0) // DK
        == lax.broadcasted_iota(jnp.int32, (LANES, LANES), 1) // DK
    ).astype(f32)
    for p in range(pairs):
        lanes = slice(p * LANES, (p + 1) * LANES)
        piece = entering[:, lanes]
        piece = jnp.concatenate(
            [jnp.where(low, piece, 0.0), jnp.where(low, 0.0, piece)], axis=0
        )
        recurrent = inner_buf[:, lanes] + dot_nt(start_buf[:, lanes], piece)
        squares = dot_hi(recurrent * recurrent, same_head) * (1.0 / DK)
        scaled = recurrent * lax.rsqrt(squares + epsilon) * gain
        ho[x, :, lanes] = (scaled * gating[:, lanes]).astype(bf16)
    send(ho.at[x], ho.at[x], misc_r.at[0], at(z, i, ox))

    @pl.when(z == 0)
    def _():
        pl.semaphore_wait(go, 1)
        far.start()


    arrived(ho.at[ox], misc_r.at[0])
    pl.when(z == 1)(far.start)
    heads = jnp.concatenate([ho[0], ho[1]], axis=1)
    stream[...] = residual_ref[...].astype(f32) + jnp.dot(
        heads, out_weight_ref[...], preferred_element_type=f32
    )
    partial = jnp.sum(stream[...] * stream[...], axis=1, keepdims=True)
    sq[x] = jnp.broadcast_to(partial, (rows, LANES))
    send(sq.at[x], sq.at[x], misc_r.at[1], at(z, i, ox))
    arrived(sq.at[ox], misc_r.at[1])
    channels = 2 * stream.shape[1]
    mean = (sq[0][:, 0:1] + sq[1][:, 0:1]) * (1.0 / channels)
    normed = stream[...] * lax.rsqrt(mean + epsilon) * norm_gain_ref[...]
    nb[z, x] = normed.astype(bf16)

    def nb_slot(zz, xx):
        return nb.at[zz, xx], nb_r.at[zz * 2 + xx]

    def share(zz, devices, first=None):
        dst, sem = nb_slot(zz, x)
        return [send(dst, dst, sem, device, first) for device in devices]

    share(z, [at(z2, i), at(z1, i), at(z, i, ox)])
    pl.when(z == 0)(near.start)
    pl.when(z > 0)(cross.start)
    cross_rest = send_half(1, z > 0)
    last_dn = send_z(dn_in, dn_slot, z3, False)
    pl.when(z % 2 == 1)(near_dn.start)
    forward_c(up_slot, z)
    forward_c(dn_slot, z)
    early_dn = prepare_yc(dn_slot, z1)
    pl.when(z % 2 == 1)(early_dn)
    forward_yc(up_slot, z2)

    pl.when(z == 1)(functools.partial(arrived, *nb_slot(z2, x)))
    passed = share(z2, [at(z1, i), at(z, i, ox)], z == 1)
    arrived(*nb_slot(z1, x))
    share(z1, [at(z, i, ox)])

    @pl.when(z != 1)
    def _():
        arrived(*nb_slot(z2, x))
        for copy in passed:
            copy.start()

    forward_yc(up_slot, z1)
    forward_c(up_slot, z2)
    arrived(*nb_slot(z3, x))
    share(z3, [at(z, i, ox)])
    pl.when(z == 0)(cross_rest.start)
    far_dn = send_z(dn_in, dn_slot, z2, z == 3)
    pl.when(z == 3)(last_dn.start)
    forward_c(up_slot, z1)
    forward_yc(up_slot, z3)
    pl.when(z < 3)(far_dn.start)
    pl.when(z % 2 == 0)(early_dn)
    later_dn = prepare_yc(dn_slot, z2)
    pl.when(z == 0)(later_dn)
    forward_c(up_slot, z3)
    pl.when(z < 3)(last_dn.start)

    for zz in range(OUTER):
        arrived(*up_slot(zz, ic))
        arrived(*up_slot(zz, idg))
        arrived(*nb_slot(zz, ox))

    mine_at = pl.ds(pl.multiple_of(z * full, LANES), full)
    taps[:, 0:full] = value_taps_ref[:, mine_at]
    taps[:, full : 2 * full] = gate_taps_ref[:, mine_at]
    if extra:
        tile = pl.ds(pl.multiple_of(OUTER * full + z // 2 * LANES, LANES), LANES)
        v = value_taps_ref[:, tile]
        g = gate_taps_ref[:, tile]
        v = jnp.where(z % 2 == 0, v, turn(v))
        g = jnp.where(z % 2 == 0, turn(g), g)
        taps[:, 2 * full : 2 * full + LANES] = jnp.where(low, v, g)

    count = OUTER * rows
    half = nb.shape[3]
    deep = half // up.shape[1]
    first = nb[:, 0].reshape(count, half)
    second = nb[:, 1].reshape(count, half)
    span = up.shape[2]
    step = 2 * LANES
    for low_lane in range(0, span, step):
        lanes = slice(low_lane, min(span, low_lane + step))
        size = lanes.stop - lanes.start
        product = jnp.dot(
            first, up[0:deep, :, lanes].reshape(half, size), preferred_element_type=f32
        ) + jnp.dot(
            second,
            up[deep : 2 * deep, :, lanes].reshape(half, size),
            preferred_element_type=f32,
        )
        ubuf[:, 8:, lanes] = (
            product.astype(bf16).astype(f32).reshape(OUTER, rows, size)
        )
    for b in range(OUTER):
        tail_s[2 * b : 2 * b + 2] = ubuf[b, rows + 6 : rows + 8]
    after = z * INNER + (i + 1) % INNER
    send(tail_s, tail_r, misc_r.at[2], {"sp": after, "tp": x})

    forward_c(dn_slot, z1)
    pl.when(z > 0)(later_dn)
    forward_yc(dn_slot, z3)

    arrived(tail_r, misc_r.at[2])
    for b in range(OUTER):
        wrapped = tail_r[2 * b - 2 : 2 * b] if b else jnp.zeros((2, span), f32)
        ubuf[b, 6:8] = jnp.where(i == 0, wrapped, tail_r[2 * b : 2 * b + 2])

    def conv(b, lanes):
        return (
            taps[0:1, lanes] * ubuf[b, pl.ds(6, rows), lanes]
            + taps[1:2, lanes] * ubuf[b, pl.ds(7, rows), lanes]
            + taps[2:3, lanes] * ubuf[b, pl.ds(8, rows), lanes]
        )

    @pl.loop(0, OUTER)
    def _(b):
        for t in range(full // LANES):
            lanes = slice(t * LANES, (t + 1) * LANES)
            other = slice(full + t * LANES, full + (t + 1) * LANES)
            hid[b, :, lanes] = (gate(conv(b, other)) * conv(b, lanes)).astype(bf16)
        if extra:
            mixed = conv(b, slice(2 * full, 2 * full + LANES))
            turned_half = turn(mixed)
            last = jnp.where(low, gate(turned_half) * mixed, 0.0)
            hid[b, :, full : full + LANES] = last.astype(bf16)

    forward_c(dn_slot, z2)
    forward_c(dn_slot, z3)
    for zz in range(OUTER):
        arrived(*dn_slot(zz, ic))
        arrived(*dn_slot(zz, idg))

    tiles = half // step
    keep = tiles - 1
    phase = len(pending)

    def tile(j):
        return slice(j * step, (j + 1) * step)

    def product(zz, base, j):
        weight = jnp.concatenate([dn[base + 2 * j], dn[base + 2 * j + 1]], axis=1)
        return jnp.dot(hid[zz], weight, preferred_element_type=f32)

    def both(zz):
        sides = [product(zz, side * deep, keep) for side in (x, ox)]
        return jnp.concatenate(sides, axis=1)

    def send_both(slot, value, device):
        zbs[slot] = value.astype(bf16)
        send(zbs.at[slot], zbr.at[slot], zb_r.at[slot], device)

    def got_both(slot):
        arrived(zbr.at[slot], zb_r.at[slot])
        return zbr[slot].astype(f32)

    def send_tile(src, dst, sem, slot, j, device):
        lanes = tile(j)
        send(src.at[slot, :, lanes], dst.at[slot, :, lanes], sem.at[slot, j], device)

    send_both(0, both(z3), at(z1, i))
    send_both(1, both(z1), at(z1, i))
    order = [(zz, j) for j in range(keep) for zz in (z3, z2)]
    order += [(zz, j) for zz in (z1, z) for j in range(keep)]
    for zz, j in order:
        xs[zz, :, tile(j)] = product(zz, ox * deep, j).astype(bf16)
        send_tile(xs, xr, xr_r, zz, j, at(z, i, ox))
    for copy in pending[:phase]:
        copy.wait_send()

    def summed(zz, j):
        value = product(zz, x * deep, j)
        arrived(xr.at[zz, :, tile(j)], xr_r.at[zz, j])
        return value + xr[zz, :, tile(j)].astype(f32)

    def received(slot, j):
        arrived(zr.at[slot, :, tile(j)], zr_r.at[slot, j])
        return zr[slot, :, tile(j)].astype(f32)

    def pass_on(slot, j, value, device):
        zs[slot, :, tile(j)] = value.astype(bf16)
        send_tile(zs, zr, zr_r, slot, j, device)

    pass_on(0, 0, summed(z3, 0), at(z1, i))
    send_both(2, both(z2) + got_both(0), at(z2, i))
    for j in range(1, keep):
        pass_on(0, j, summed(z3, j), at(z1, i))
    for j in range(keep):
        value = summed(z2, j)
        pass_on(2, j, value + received(0, j), at(z2, i))
    for j in range(keep):
        pass_on(1, j, summed(z1, j), at(z1, i))
    pair = both(z) + got_both(1)
    pair = pair + got_both(2)
    xbs[...] = pair[:, step:].astype(bf16)
    send(xbs, xbr, zb_r.at[3], at(z, i, ox))
    for j in range(keep):
        own = summed(z, j) + received(1, j) + received(2, j)
        out_ref[:, tile(j)] = (stream[:, tile(j)] + own).astype(bf16)
    arrived(xbr, zb_r.at[3])
    own = pair[:, :step] + xbr[...].astype(f32)
    out_ref[:, tile(keep)] = (stream[:, tile(keep)] + own).astype(bf16)

    for copy in pending[phase:]:
        copy.wait_send()


def fused_layer(
    residual_in,
    query_pre,
    forget_pre,
    value_pre,
    gate_pre,
    floor_gap,
    head_gain,
    out_weight,
    norm_gain,
    value_weight,
    gate_weight,
    value_taps,
    gate_taps,
    down_weight,
):
    rows, my_width = residual_in.shape
    depth, half = value_weight.shape
    width = query_pre.shape[1]
    blocks = INNER * OUTER
    full = half // LANES // OUTER * LANES
    extra = half // OUTER - full
    chunk = full + extra
    padded = full + (LANES if extra else 0)

    dma = pltpu.SemaphoreType.DMA
    vmem = pl.BlockSpec(memory_space=pltpu.VMEM)
    span = 2 * chunk
    return pl.pallas_call(
        functools.partial(layer_kernel, full, extra),
        out_shape=jax.ShapeDtypeStruct((rows, my_width), bf16),
        in_specs=[vmem] * 14,
        out_specs=vmem,
        scratch_shapes=[
            pltpu.VMEM((OUTER, depth, span), bf16),
            pltpu.VMEM((OUTER, chunk, depth), bf16),
            pltpu.VMEM((value_taps.shape[0], span), f32),
            pltpu.VMEM((blocks, depth, span), bf16),
            pltpu.VMEM((blocks, padded, depth), bf16),
            pltpu.VMEM((INNER, DK + SUB, width), bf16),
            pltpu.VMEM((OUTER, DK + SUB, width), bf16),
            pltpu.VMEM((rows, width), f32),
            pltpu.VMEM((rows, width), f32),
            pltpu.VMEM((2, rows, width), bf16),
            pltpu.VMEM((2, rows, LANES), f32),
            pltpu.VMEM((rows, my_width), f32),
            pltpu.VMEM((OUTER, 2, rows, my_width), bf16),
            pltpu.VMEM((OUTER, rows + 8, span), f32),
            pltpu.VMEM((2 * OUTER, span), f32),
            pltpu.VMEM((2 * OUTER, span), f32),
            pltpu.VMEM((OUTER, rows, padded), bf16),
            pltpu.VMEM((OUTER, rows, my_width), bf16),
            pltpu.VMEM((OUTER, rows, my_width), bf16),
            pltpu.VMEM((3, rows, my_width), bf16),
            pltpu.VMEM((3, rows, my_width), bf16),
            pltpu.VMEM((3, rows, 4 * LANES), bf16),
            pltpu.VMEM((3, rows, 4 * LANES), bf16),
            pltpu.VMEM((rows, 2 * LANES), bf16),
            pltpu.VMEM((rows, 2 * LANES), bf16),
            dma((96,)),
            dma((blocks,)),
            dma((blocks,)),
            dma((INNER,)),
            dma((OUTER,)),
            dma((OUTER,)),
            pltpu.SemaphoreType.REGULAR,
            dma((2 * OUTER,)),
            dma((OUTER, 4)),
            dma((3, 4)),
            dma((4,)),
            dma((3,)),
        ],
        compiler_params=pltpu.CompilerParams(
            collective_id=0, has_side_effects=True, vmem_limit_bytes=56 * 2**20
        ),
        name="layer",
    )(
        residual_in,
        query_pre,
        forget_pre,
        value_pre,
        gate_pre,
        floor_gap[None],
        head_gain[None],
        out_weight,
        norm_gain[None],
        value_weight,
        gate_weight,
        value_taps,
        gate_taps,
        down_weight,
    )


def local_recurrence(query_pre, forget_pre, value_pre, floor_gap):
    rows, width = query_pre.shape
    heads = width // DK
    subs = rows // SUB
    keys = floor_gap * jax.nn.sigmoid(-forget_pre.astype(f32))
    log_decay = jnp.log1p(-keys)
    query = jax.nn.silu(query_pre.astype(f32))
    values = value_pre.astype(f32)
    position = lax.iota(jnp.int32, rows)
    lower = (position[:, None] >= position[None, :]).astype(f32)
    running = jnp.dot(lower, log_decay, precision=highest)
    middle = running.reshape(subs, SUB, width)[:, SUB // 2 - 1, :]
    query_part = query * jnp.exp(running - jnp.repeat(middle, SUB, axis=0))
    reach = (lax.iota(jnp.int32, subs) + 1) * SUB
    seen = position[None, :, None] < reach[:, None, None]
    key_part = keys[None] * jnp.exp(
        jnp.where(seen, middle[:, None, :] - running[None], -jnp.inf)
    )
    scores = jnp.einsum(
        "ithk,ishk->hits",
        query_part.reshape(subs, SUB, heads, DK),
        key_part.reshape(subs, rows, heads, DK),
        precision=highest,
    ).reshape(heads, rows, rows)
    scores = jnp.where(position[None, :, None] >= position[None, None, :], scores, 0.0)
    value_heads = values.reshape(rows, heads, DK)
    inner = jnp.einsum("hts,shv->htv", scores, value_heads, precision=highest)
    ending = running[-1]
    state = jnp.einsum(
        "shv,shk->vhk",
        value_heads,
        (keys * jnp.exp(ending - running)).reshape(rows, heads, DK),
        precision=highest,
    ).reshape(DK, width)
    from_start = (query * jnp.exp(running)).reshape(rows, heads, DK)
    return inner, state, jnp.exp(ending), from_start


def causal_taps(before, current, taps):
    padded = jnp.concatenate([before, current], axis=1).astype(f32)
    rows = current.shape[1]
    return (
        taps[0] * padded[:, 0:rows]
        + taps[1] * padded[:, 1 : rows + 1]
        + taps[2] * padded[:, 2 : rows + 2]
    )


def on_device(
    residual_in,
    query_pre,
    forget_pre,
    value_pre,
    gate_pre,
    floor_gap,
    head_gain,
    out_weight,
    norm_gain,
    value_weight,
    gate_weight,
    value_taps,
    gate_taps,
    down_weight,
):
    sp = lax.axis_size("sp")
    tp = lax.axis_size("tp")
    inner_size = 4 if sp % 4 == 0 else 1
    outer = sp // inner_size
    me = lax.axis_index("sp")
    my_outer = me // inner_size
    my_inner = me % inner_size
    outer_groups = [[o * inner_size + i for o in range(outer)] for i in range(inner_size)]
    inner_groups = [[o * inner_size + i for i in range(inner_size)] for o in range(outer)]
    rows, my_width = residual_in.shape
    width = my_width * tp
    depth, half = value_weight.shape
    chunk = half // outer

    wide_groups = [
        [s * tp + t for s in group for t in range(tp)] for group in outer_groups
    ]

    def exchange(array):
        return lax.all_to_all(
            array, "sp", 0, 0, axis_index_groups=outer_groups, tiled=True
        )

    def gather_inner(array):
        return lax.all_gather(array, "sp", axis_index_groups=inner_groups)

    def gather_wide(array):
        gathered = lax.all_gather(array, ("sp", "tp"), axis_index_groups=wide_groups)
        gathered = gathered.reshape(outer, tp, *array.shape)
        return [gathered[:, t].reshape(-1, array.shape[1]) for t in range(tp)]

    def reorder(pieces):
        span = pieces[0].shape[-1]
        blocks = []
        for i in range(inner_size):
            for o in range(outer):
                start = (o * inner_size + i) * depth
                low = start % span
                blocks.append(pieces[start // span][..., low : low + depth])
        return lax.optimization_barrier(jnp.concatenate(blocks, axis=-1))

    up_parts = jnp.stack(
        [
            jnp.concatenate(
                [
                    value_weight[:, o * chunk : (o + 1) * chunk],
                    gate_weight[:, o * chunk : (o + 1) * chunk],
                ],
                axis=1,
            )
            for o in range(outer)
        ]
    )
    up_chunk = gather_inner(exchange(up_parts)).reshape(width, 2 * chunk)
    down_parts = down_weight.reshape(outer, chunk, depth)
    down_mine = gather_inner(exchange(down_parts))
    down_chunk = down_mine.transpose(2, 1, 0, 3).reshape(chunk, width)

    out_full = reorder(list(lax.all_gather(out_weight, "tp")))
    gain_full = reorder(list(lax.all_gather(norm_gain, "tp")))
    residual_group = reorder(gather_wide(residual_in))

    inner, state, total_decay, from_start = local_recurrence(
        query_pre, forget_pre, value_pre, floor_gap
    )
    heads = inner.shape[0]
    first = total_decay.astype(bf16)
    rest = total_decay - first.astype(f32)
    second = rest.astype(bf16)
    third = (rest - second.astype(f32)).astype(bf16)
    spare = jnp.zeros((13, heads * DK), bf16)
    packed = jnp.concatenate(
        [state.astype(bf16), first[None], second[None], third[None], spare], axis=0
    )
    everyone = lax.all_gather(packed, "sp").astype(f32)
    decays = everyone[:, DK] + everyone[:, DK + 1] + everyone[:, DK + 2]
    entering = jnp.zeros_like(state)
    for j in range(sp - 1):
        advanced = entering * decays[j] + everyone[j, :DK]
        entering = jnp.where(j < me, advanced, entering)
    carried = jnp.einsum(
        "thk,vhk->htv", from_start, entering.reshape(DK, heads, DK), precision=highest
    )
    recurrent = (inner + carried).transpose(1, 0, 2)
    scaled = (
        recurrent
        * lax.rsqrt(jnp.mean(recurrent * recurrent, axis=-1, keepdims=True) + epsilon)
        * head_gain
    )
    gating = jax.nn.silu(gate_pre.astype(f32)).reshape(recurrent.shape)
    head_out = (scaled * gating).reshape(rows, heads * DK).astype(bf16)

    head_out, out_full = lax.optimization_barrier((head_out, out_full))
    head_group = jnp.concatenate(gather_wide(head_out), axis=1)
    stream = residual_group.astype(f32) + jnp.dot(
        head_group, out_full, preferred_element_type=f32
    )
    squares = jnp.mean(stream * stream, axis=1, keepdims=True)
    normed = (stream * lax.rsqrt(squares + epsilon) * gain_full).astype(bf16)
    up = jnp.dot(normed, up_chunk, preferred_element_type=f32).astype(bf16)
    up = up.reshape(outer, rows, 2 * chunk)
    tails = up[:, rows - 2 :]
    pairs = [
        (o * inner_size + i, o * inner_size + (i + 1) % inner_size)
        for o in range(outer)
        for i in range(inner_size)
    ]
    arrived = lax.ppermute(tails, "sp", pairs) if inner_size > 1 else tails
    wrapped = jnp.concatenate([jnp.zeros_like(arrived[:1]), arrived[:-1]], axis=0)
    before = jnp.where(my_inner == 0, wrapped, arrived)

    taps = jnp.concatenate(
        [
            lax.dynamic_slice_in_dim(value_taps, my_outer * chunk, chunk, axis=1),
            lax.dynamic_slice_in_dim(gate_taps, my_outer * chunk, chunk, axis=1),
        ],
        axis=1,
    )
    conv = causal_taps(before, up, taps)
    hidden = (jax.nn.silu(conv[:, :, chunk:]) * conv[:, :, :chunk]).astype(bf16)
    terms = jnp.dot(
        hidden.reshape(outer * rows, chunk), down_chunk, preferred_element_type=f32
    ).astype(bf16)
    summed = lax.psum_scatter(
        terms, "sp", scatter_dimension=0, tiled=True, axis_index_groups=outer_groups
    )
    summed = lax.psum_scatter(summed, "tp", scatter_dimension=1, tiled=True)
    my_heads = lax.dynamic_slice_in_dim(head_group, my_outer * rows, rows, axis=0)
    own = residual_in.astype(f32) + jnp.dot(
        my_heads, out_weight, preferred_element_type=f32
    )
    return (own + summed.astype(f32)).astype(bf16)


def fits(mesh, residual_in, query_pre, *arrays):
    depth, half = arrays[7].shape
    extra = half // OUTER % LANES
    return (
        mesh.shape["sp"] == INNER * OUTER
        and mesh.shape["tp"] == 2
        and depth == LANES
        and residual_in.shape == (LANES, depth * INNER * OUTER // 2)
        and query_pre.shape[1] % LANES == 0
        and half % LANES == 0
        and extra in (0, LANES // 2)
    )


def solution(mesh):
    rows = P(("grp", "sp"), "tp")

    def layer(*arrays):
        return (fused_layer if fits(mesh, *arrays) else on_device)(*arrays)

    return jax.shard_map(
        layer,
        mesh=mesh,
        in_specs=(
            rows,
            rows,
            rows,
            rows,
            rows,
            P("tp"),
            P(),
            P(None, "tp"),
            P("tp"),
            P("sp", "tp"),
            P("sp", "tp"),
            P(None, "tp"),
            P(None, "tp"),
            P("tp", "sp"),
        ),
        out_specs=rows,
        check_vma=False,
    )
```

```python
import functools

import jax
import jax.numpy as jnp
from jax import lax
from jax.experimental import pallas as pl
from jax.experimental.pallas import tpu as pltpu
from jax.sharding import PartitionSpec as P

DK = 64
SUB = 16
LANES = 128
INNER = 4
OUTER = 4
epsilon = 1e-06
highest = lax.Precision.HIGHEST
f32 = jnp.float32
bf16 = jnp.bfloat16
MESH = pl.DeviceIdType.MESH


def dot_nt(a, b):
    return lax.dot_general(
        a, b, (((1,), (1,)), ((), ())), precision=highest, preferred_element_type=f32
    )


def dot_hi(a, b):
    return jnp.dot(a, b, precision=highest, preferred_element_type=f32)


def gate(v):
    return v / (1.0 + jnp.exp(-v))


def turn(v):
    return jnp.concatenate([v[:, DK:], v[:, :DK]], axis=1)


def layer_kernel(
    full,
    extra,
    residual_ref,
    query_ref,
    forget_ref,
    value_ref,
    gate_ref,
    floor_ref,
    head_gain_ref,
    out_weight_ref,
    norm_gain_ref,
    value_weight_ref,
    gate_weight_ref,
    value_taps_ref,
    gate_taps_ref,
    down_ref,
    out_ref,
    up_in,
    dn_in,
    taps,
    up,
    dn,
    st,
    zt,
    inner_buf,
    start_buf,
    ho,
    sq,
    stream,
    nb,
    ubuf,
    tail_s,
    tail_r,
    hid,
    xs,
    xr,
    zs,
    zr,
    zbs,
    zbr,
    xbs,
    xbr,
    ssem,
    up_r,
    dn_r,
    st_r,
    zt_r,
    zt_s,
    go,
    nb_r,
    xr_r,
    zr_r,
    zb_r,
    misc_r,
):
    s = lax.axis_index("sp")
    x = lax.axis_index("tp")
    z = s // INNER
    i = s % INNER
    c = s % 2
    ox = 1 - x
    ic = i + 1 - 2 * c
    iy = (i + 2) % INNER
    idg = (ic + 2) % INNER
    z1 = z + 1 - 2 * (z % 2)
    z2 = (z + 2) % OUTER
    z3 = OUTER - 1 - z
    chunk = full + extra
    depth = up.shape[1]
    rows = query_ref.shape[0]
    width = query_ref.shape[1]
    pairs = width // LANES
    pending = []

    def at(zz, ii, xx=x):
        return {"sp": zz * INNER + ii, "tp": xx}

    def send(src, dst, rsem, device, first=None):
        copy = pltpu.make_async_remote_copy(
            src_ref=src,
            dst_ref=dst,
            send_sem=ssem.at[len(pending)],
            recv_sem=rsem,
            device_id=device,
            device_id_type=MESH,
        )
        pending.append(copy)
        if first is None:
            copy.start()
        elif first is not False:
            pl.when(first)(copy.start)
        return copy

    def arrived(dst, rsem):
        pltpu.make_async_remote_copy(
            src_ref=dst,
            dst_ref=dst,
            send_sem=ssem.at[0],
            recv_sem=rsem,
            device_id=at(z, ic),
            device_id_type=MESH,
        ).wait_recv()

    barrier = pltpu.get_barrier_semaphore()
    peers = [at((z + k) % OUTER, i) for k in range(1, OUTER)]
    peers += [at(z, ic), at(z, iy), at(z, idg), at(z, i, ox)]
    for peer in peers:
        pl.semaphore_signal(barrier, inc=1, device_id=peer, device_id_type=MESH)

    def up_slot(zz, ii):
        return up.at[zz * INNER + ii], up_r.at[zz * INNER + ii]

    def dn_slot(zz, ii):
        slot = dn.at[zz * INNER + ii, pl.ds(0, chunk)]
        return slot, dn_r.at[zz * INNER + ii]

    def send_z(source, slot, zz, first=None):
        dst, sem = slot(z, i)
        return send(source.at[zz], dst, sem, at(zz, i), first)

    def forward_yc(slot, zz, source=None):
        dst, sem = slot(zz, i)
        if source is None:
            arrived(dst, sem)
            source = dst
        send(source, dst, sem, at(z, iy))
        send(source, dst, sem, at(z, ic))

    def send_half(part, first):
        dst, sem = up_slot(z, i)
        part_rows = pl.ds(part * (depth // 2), depth // 2)
        src = up_in.at[z3, part_rows]
        return send(src, dst.at[part_rows], sem, at(z3, i), first)

    def prepare_yc(slot, zz):
        dst, sem = slot(zz, i)
        copies = [send(dst, dst, sem, at(z, ii), False) for ii in (iy, ic)]

        def run():
            arrived(dst, sem)
            for copy in copies:
                copy.start()

        return run

    def forward_c(slot, zz):
        dst, sem = slot(zz, iy)
        arrived(dst, sem)
        send(dst, dst, sem, at(z, ic))

    keys = floor_ref[...] * jax.nn.sigmoid(-forget_ref[...].astype(f32))
    query = gate(query_ref[...].astype(f32))
    values = value_ref[...].astype(f32)
    position = lax.broadcasted_iota(jnp.int32, (rows, rows), 0)
    earlier = lax.broadcasted_iota(jnp.int32, (rows, rows), 1)
    running = dot_hi((position >= earlier).astype(f32), jnp.log1p(-keys))
    ending = running[rows - 1 : rows]
    kept = keys * jnp.exp(ending - running)
    turned = values.T
    low = lax.broadcasted_iota(jnp.int32, (1, LANES), 1) < DK
    part_row = lax.broadcasted_iota(jnp.int32, (SUB, width), 0)

    def store_state(ref, state, decay):
        ref[0:DK] = state.astype(bf16)
        one = decay.astype(bf16).astype(f32)
        two = (decay - one).astype(bf16).astype(f32)
        three = decay - one - two
        parts = jnp.where(part_row == 1, two, jnp.where(part_row == 2, three, 0.0))
        ref[DK : DK + SUB] = jnp.where(part_row == 0, one, parts).astype(bf16)

    def load_state(ref):
        parts = ref[DK : DK + SUB].astype(f32)
        return ref[0:DK].astype(f32), parts[0:1] + parts[1:2] + parts[2:3]

    states = []
    for p in range(pairs):
        lanes = slice(p * LANES, (p + 1) * LANES)
        both = dot_hi(turned[lanes], kept[:, lanes])
        states.append(jnp.where(low, both[:DK], both[DK:]))
    store_state(st.at[i], jnp.concatenate(states, axis=1), jnp.exp(ending))
    for o in range(OUTER):
        main = slice(o * full, (o + 1) * full)
        up_in[o, :, 0:full] = value_weight_ref[:, main]
        up_in[o, :, full : 2 * full] = gate_weight_ref[:, main]
        dn_in[o, 0:full] = down_ref[main]
        if extra:
            start = OUTER * full + o * extra
            dn_in[o, full:chunk] = down_ref[start : start + extra]
    if extra:
        for o in range(0, OUTER, 2):
            start = OUTER * full + o * extra
            tile = slice(start, start + LANES)
            v = value_weight_ref[:, tile].astype(f32)
            g = gate_weight_ref[:, tile].astype(f32)
            end = slice(2 * full, 2 * full + LANES)
            up_in[o, :, end] = jnp.where(low, v, turn(g)).astype(bf16)
            up_in[o + 1, :, end] = jnp.where(low, turn(v), g).astype(bf16)

    pl.semaphore_wait(barrier, len(peers))
    for ii in (idg, iy, ic):
        send(st.at[i], st.at[i], st_r.at[i], at(z, ii))
    far = send_z(up_in, up_slot, z2, z == 3)
    near = send_z(up_in, up_slot, z1, z % 2 == 1)
    cross = send_half(0, z == 0)
    near_dn = send_z(dn_in, dn_slot, z1, z == 0)

    up[s] = up_in[z]
    dn[s, 0:chunk] = dn_in[z]
    spare = dn.shape[1] - chunk
    if spare:
        for b in range(INNER * OUTER):
            dn[b, chunk:] = jnp.zeros((spare, dn.shape[2]), bf16)
    start_buf[...] = query * jnp.exp(running)

    for ii in (ic, iy, idg):
        arrived(st.at[ii], st_r.at[ii])
    total = jnp.zeros((DK, width), f32)
    mine = jnp.zeros((DK, width), f32)
    total_decay = jnp.ones((1, width), f32)
    my_decay = jnp.ones((1, width), f32)
    for j in range(INNER):
        fresh, decay = load_state(st.at[j])
        mine = jnp.where(j < i, mine * decay + fresh, mine)
        my_decay = jnp.where(j < i, my_decay * decay, my_decay)
        total = total * decay + fresh
        total_decay = total_decay * decay
    store_state(zt.at[z], total, total_decay)
    totals = []
    for k in range(1, OUTER):
        totals.append(
            pltpu.make_async_remote_copy(
                src_ref=zt.at[z],
                dst_ref=zt.at[z],
                send_sem=zt_s.at[k],
                recv_sem=zt_r.at[z],
                device_id=at((z + k) % OUTER, i),
                device_id_type=MESH,
            )
        )
    for k in (3, 2, 1):
        pl.when(z + k < OUTER)(totals[k - 1].start)
    pl.when(z == 2)(near_dn.start)
    pl.when(z == 2)(near.start)
    forward_yc(up_slot, z, up_in.at[z])
    forward_yc(dn_slot, z, dn_in.at[z])

    cells = [[] for _ in range(pairs)]
    row_of = lax.broadcasted_iota(jnp.int32, (rows, width), 0)
    column = lax.broadcasted_iota(jnp.int32, (2 * SUB, rows), 1)
    stacked = lax.broadcasted_iota(jnp.int32, (2 * SUB, rows), 0) % SUB
    for n in range(rows // SUB):
        part = slice(n * SUB, (n + 1) * SUB)
        middle = running[n * SUB + SUB // 2 - 1 : n * SUB + SUB // 2]
        query_part = query[part] * jnp.exp(running[part] - middle)
        reach = jnp.where(row_of < (n + 1) * SUB, middle - running, -jnp.inf)
        key_part = keys * jnp.exp(reach)
        for p in range(pairs):
            lanes = slice(p * LANES, (p + 1) * LANES)
            piece = query_part[:, lanes]
            piece = jnp.concatenate(
                [jnp.where(low, piece, 0.0), jnp.where(low, 0.0, piece)], axis=0
            )
            score = dot_nt(piece, key_part[:, lanes])
            score = jnp.where(stacked + n * SUB >= column, score, 0.0)
            cells[p].append(score)
    for p in range(pairs):
        lanes = slice(p * LANES, (p + 1) * LANES)
        scores = jnp.concatenate(
            [cell[:SUB] for cell in cells[p]] + [cell[SUB:] for cell in cells[p]],
            axis=0,
        )
        result = dot_hi(scores, values[:, lanes])
        inner_buf[:, lanes] = jnp.where(low, result[:rows], result[rows:])

    for k, copy in enumerate(totals, 1):
        pl.when(z + k < OUTER)(copy.wait_send)

    @pl.when(z == 1)
    def _():
        pl.semaphore_signal(go, inc=1, device_id=at(z1, i), device_id_type=MESH)

    pl.when(z == 2)(far.start)
    gain = jnp.concatenate([head_gain_ref[...]] * (LANES // DK), axis=1)
    gating = gate(gate_ref[...].astype(f32))
    for k in range(1, OUTER):
        zz = (z + OUTER - k) % OUTER
        pl.when(z >= k)(functools.partial(arrived, zt.at[zz], zt_r.at[zz]))
    entering = jnp.zeros((DK, width), f32)
    for j in range(OUTER - 1):
        fresh, decay = load_state(zt.at[j])
        entering = jnp.where(j < z, entering * decay + fresh, entering)
    entering = entering * my_decay + mine
    same_head = (
        lax.broadcasted_iota(jnp.int32, (LANES, LANES), 0) // DK
        == lax.broadcasted_iota(jnp.int32, (LANES, LANES), 1) // DK
    ).astype(f32)
    for p in range(pairs):
        lanes = slice(p * LANES, (p + 1) * LANES)
        piece = entering[:, lanes]
        piece = jnp.concatenate(
            [jnp.where(low, piece, 0.0), jnp.where(low, 0.0, piece)], axis=0
        )
        recurrent = inner_buf[:, lanes] + dot_nt(start_buf[:, lanes], piece)
        squares = dot_hi(recurrent * recurrent, same_head) * (1.0 / DK)
        scaled = recurrent * lax.rsqrt(squares + epsilon) * gain
        ho[x, :, lanes] = (scaled * gating[:, lanes]).astype(bf16)
    send(ho.at[x], ho.at[x], misc_r.at[0], at(z, i, ox))

    @pl.when(z == 0)
    def _():
        pl.semaphore_wait(go, 1)
        far.start()


    arrived(ho.at[ox], misc_r.at[0])
    pl.when(z == 1)(far.start)
    heads = jnp.concatenate([ho[0], ho[1]], axis=1)
    stream[...] = residual_ref[...].astype(f32) + jnp.dot(
        heads, out_weight_ref[...], preferred_element_type=f32
    )
    partial = jnp.sum(stream[...] * stream[...], axis=1, keepdims=True)
    sq[x] = jnp.broadcast_to(partial, (rows, LANES))
    send(sq.at[x], sq.at[x], misc_r.at[1], at(z, i, ox))
    arrived(sq.at[ox], misc_r.at[1])
    channels = 2 * stream.shape[1]
    mean = (sq[0][:, 0:1] + sq[1][:, 0:1]) * (1.0 / channels)
    normed = stream[...] * lax.rsqrt(mean + epsilon) * norm_gain_ref[...]
    nb[z, x] = normed.astype(bf16)

    def nb_slot(zz, xx):
        return nb.at[zz, xx], nb_r.at[zz * 2 + xx]

    def share(zz, devices, first=None):
        dst, sem = nb_slot(zz, x)
        return [send(dst, dst, sem, device, first) for device in devices]

    share(z, [at(z2, i), at(z1, i), at(z, i, ox)])
    pl.when(z == 0)(near.start)
    pl.when(z > 0)(cross.start)
    cross_rest = send_half(1, z > 0)
    last_dn = send_z(dn_in, dn_slot, z3, False)
    pl.when(z % 2 == 1)(near_dn.start)
    forward_c(up_slot, z)
    forward_c(dn_slot, z)
    early_dn = prepare_yc(dn_slot, z1)
    pl.when(z % 2 == 1)(early_dn)
    forward_yc(up_slot, z2)

    pl.when(z == 1)(functools.partial(arrived, *nb_slot(z2, x)))
    passed = share(z2, [at(z1, i), at(z, i, ox)], z == 1)
    arrived(*nb_slot(z1, x))
    share(z1, [at(z, i, ox)])

    @pl.when(z != 1)
    def _():
        arrived(*nb_slot(z2, x))
        for copy in passed:
            copy.start()

    forward_yc(up_slot, z1)
    forward_c(up_slot, z2)
    arrived(*nb_slot(z3, x))
    share(z3, [at(z, i, ox)])
    pl.when(z == 0)(cross_rest.start)
    far_dn = send_z(dn_in, dn_slot, z2, z == 3)
    pl.when(z == 3)(last_dn.start)
    forward_c(up_slot, z1)
    forward_yc(up_slot, z3)
    pl.when(z < 3)(far_dn.start)
    pl.when(z % 2 == 0)(early_dn)
    later_dn = prepare_yc(dn_slot, z2)
    forward_c(up_slot, z3)
    pl.when(z < 3)(last_dn.start)
    pl.when(z % 3 == 0)(later_dn)

    for zz in range(OUTER):
        arrived(*up_slot(zz, ic))
        arrived(*up_slot(zz, idg))
        arrived(*nb_slot(zz, ox))

    mine_at = pl.ds(pl.multiple_of(z * full, LANES), full)
    taps[:, 0:full] = value_taps_ref[:, mine_at]
    taps[:, full : 2 * full] = gate_taps_ref[:, mine_at]
    if extra:
        tile = pl.ds(pl.multiple_of(OUTER * full + z // 2 * LANES, LANES), LANES)
        v = value_taps_ref[:, tile]
        g = gate_taps_ref[:, tile]
        v = jnp.where(z % 2 == 0, v, turn(v))
        g = jnp.where(z % 2 == 0, turn(g), g)
        taps[:, 2 * full : 2 * full + LANES] = jnp.where(low, v, g)

    count = OUTER * rows
    half = nb.shape[3]
    deep = half // up.shape[1]
    first = nb[:, 0].reshape(count, half)
    second = nb[:, 1].reshape(count, half)
    span = up.shape[2]
    step = 2 * LANES
    for low_lane in range(0, span, step):
        lanes = slice(low_lane, min(span, low_lane + step))
        size = lanes.stop - lanes.start
        product = jnp.dot(
            first, up[0:deep, :, lanes].reshape(half, size), preferred_element_type=f32
        ) + jnp.dot(
            second,
            up[deep : 2 * deep, :, lanes].reshape(half, size),
            preferred_element_type=f32,
        )
        ubuf[:, 8:, lanes] = (
            product.astype(bf16).astype(f32).reshape(OUTER, rows, size)
        )
    for b in range(OUTER):
        tail_s[2 * b : 2 * b + 2] = ubuf[b, rows + 6 : rows + 8]
    after = z * INNER + (i + 1) % INNER
    send(tail_s, tail_r, misc_r.at[2], {"sp": after, "tp": x})

    forward_c(dn_slot, z1)
    pl.when(z % 3 != 0)(later_dn)
    forward_yc(dn_slot, z3)

    arrived(tail_r, misc_r.at[2])
    for b in range(OUTER):
        wrapped = tail_r[2 * b - 2 : 2 * b] if b else jnp.zeros((2, span), f32)
        ubuf[b, 6:8] = jnp.where(i == 0, wrapped, tail_r[2 * b : 2 * b + 2])

    def conv(b, lanes):
        return (
            taps[0:1, lanes] * ubuf[b, pl.ds(6, rows), lanes]
            + taps[1:2, lanes] * ubuf[b, pl.ds(7, rows), lanes]
            + taps[2:3, lanes] * ubuf[b, pl.ds(8, rows), lanes]
        )

    @pl.loop(0, OUTER)
    def _(b):
        for t in range(full // LANES):
            lanes = slice(t * LANES, (t + 1) * LANES)
            other = slice(full + t * LANES, full + (t + 1) * LANES)
            hid[b, :, lanes] = (gate(conv(b, other)) * conv(b, lanes)).astype(bf16)
        if extra:
            mixed = conv(b, slice(2 * full, 2 * full + LANES))
            turned_half = turn(mixed)
            last = jnp.where(low, gate(turned_half) * mixed, 0.0)
            hid[b, :, full : full + LANES] = last.astype(bf16)

    forward_c(dn_slot, z2)
    forward_c(dn_slot, z3)
    for zz in range(OUTER):
        arrived(*dn_slot(zz, ic))
        arrived(*dn_slot(zz, idg))

    tiles = half // step
    keep = tiles - 1
    phase = len(pending)

    def tile(j):
        return slice(j * step, (j + 1) * step)

    def product(zz, base, j):
        weight = jnp.concatenate([dn[base + 2 * j], dn[base + 2 * j + 1]], axis=1)
        return jnp.dot(hid[zz], weight, preferred_element_type=f32)

    def both(zz):
        sides = [product(zz, side * deep, keep) for side in (x, ox)]
        return jnp.concatenate(sides, axis=1)

    def send_both(slot, value, device):
        zbs[slot] = value.astype(bf16)
        send(zbs.at[slot], zbr.at[slot], zb_r.at[slot], device)

    def got_both(slot):
        arrived(zbr.at[slot], zb_r.at[slot])
        return zbr[slot].astype(f32)

    def send_tile(src, dst, sem, slot, j, device):
        lanes = tile(j)
        send(src.at[slot, :, lanes], dst.at[slot, :, lanes], sem.at[slot, j], device)

    send_both(0, both(z3), at(z1, i))
    send_both(1, both(z1), at(z1, i))
    order = [(zz, j) for j in range(keep) for zz in (z3, z2)]
    order += [(zz, j) for zz in (z1, z) for j in range(keep)]
    for zz, j in order:
        xs[zz, :, tile(j)] = product(zz, ox * deep, j).astype(bf16)
        send_tile(xs, xr, xr_r, zz, j, at(z, i, ox))
    for copy in pending[:phase]:
        copy.wait_send()

    def summed(zz, j):
        value = product(zz, x * deep, j)
        arrived(xr.at[zz, :, tile(j)], xr_r.at[zz, j])
        return value + xr[zz, :, tile(j)].astype(f32)

    def received(slot, j):
        arrived(zr.at[slot, :, tile(j)], zr_r.at[slot, j])
        return zr[slot, :, tile(j)].astype(f32)

    def pass_on(slot, j, value, device):
        zs[slot, :, tile(j)] = value.astype(bf16)
        send_tile(zs, zr, zr_r, slot, j, device)

    pass_on(0, 0, summed(z3, 0), at(z1, i))
    send_both(2, both(z2) + got_both(0), at(z2, i))
    for j in range(1, keep):
        pass_on(0, j, summed(z3, j), at(z1, i))
    for j in range(keep):
        value = summed(z2, j)
        pass_on(2, j, value + received(0, j), at(z2, i))
    for j in range(keep):
        pass_on(1, j, summed(z1, j), at(z1, i))
    pair = both(z) + got_both(1)
    pair = pair + got_both(2)
    xbs[...] = pair[:, step:].astype(bf16)
    send(xbs, xbr, zb_r.at[3], at(z, i, ox))
    for j in range(keep):
        own = summed(z, j) + received(1, j) + received(2, j)
        out_ref[:, tile(j)] = (stream[:, tile(j)] + own).astype(bf16)
    arrived(xbr, zb_r.at[3])
    own = pair[:, :step] + xbr[...].astype(f32)
    out_ref[:, tile(keep)] = (stream[:, tile(keep)] + own).astype(bf16)

    for copy in pending[phase:]:
        copy.wait_send()


def fused_layer(
    residual_in,
    query_pre,
    forget_pre,
    value_pre,
    gate_pre,
    floor_gap,
    head_gain,
    out_weight,
    norm_gain,
    value_weight,
    gate_weight,
    value_taps,
    gate_taps,
    down_weight,
):
    rows, my_width = residual_in.shape
    depth, half = value_weight.shape
    width = query_pre.shape[1]
    blocks = INNER * OUTER
    full = half // LANES // OUTER * LANES
    extra = half // OUTER - full
    chunk = full + extra
    padded = full + (LANES if extra else 0)

    dma = pltpu.SemaphoreType.DMA
    vmem = pl.BlockSpec(memory_space=pltpu.VMEM)
    span = 2 * chunk
    return pl.pallas_call(
        functools.partial(layer_kernel, full, extra),
        out_shape=pltpu.VMEM((rows, my_width), bf16),
        in_specs=[vmem] * 14,
        out_specs=vmem,
        scratch_shapes=[
            pltpu.VMEM((OUTER, depth, span), bf16),
            pltpu.VMEM((OUTER, chunk, depth), bf16),
            pltpu.VMEM((value_taps.shape[0], span), f32),
            pltpu.VMEM((blocks, depth, span), bf16),
            pltpu.VMEM((blocks, padded, depth), bf16),
            pltpu.VMEM((INNER, DK + SUB, width), bf16),
            pltpu.VMEM((OUTER, DK + SUB, width), bf16),
            pltpu.VMEM((rows, width), f32),
            pltpu.VMEM((rows, width), f32),
            pltpu.VMEM((2, rows, width), bf16),
            pltpu.VMEM((2, rows, LANES), f32),
            pltpu.VMEM((rows, my_width), f32),
            pltpu.VMEM((OUTER, 2, rows, my_width), bf16),
            pltpu.VMEM((OUTER, rows + 8, span), f32),
            pltpu.VMEM((2 * OUTER, span), f32),
            pltpu.VMEM((2 * OUTER, span), f32),
            pltpu.VMEM((OUTER, rows, padded), bf16),
            pltpu.VMEM((OUTER, rows, my_width), bf16),
            pltpu.VMEM((OUTER, rows, my_width), bf16),
            pltpu.VMEM((3, rows, my_width), bf16),
            pltpu.VMEM((3, rows, my_width), bf16),
            pltpu.VMEM((3, rows, 4 * LANES), bf16),
            pltpu.VMEM((3, rows, 4 * LANES), bf16),
            pltpu.VMEM((rows, 2 * LANES), bf16),
            pltpu.VMEM((rows, 2 * LANES), bf16),
            dma((96,)),
            dma((blocks,)),
            dma((blocks,)),
            dma((INNER,)),
            dma((OUTER,)),
            dma((OUTER,)),
            pltpu.SemaphoreType.REGULAR,
            dma((2 * OUTER,)),
            dma((OUTER, 4)),
            dma((3, 4)),
            dma((4,)),
            dma((3,)),
        ],
        compiler_params=pltpu.CompilerParams(
            collective_id=0, has_side_effects=True, vmem_limit_bytes=56 * 2**20
        ),
        name="layer",
    )(
        residual_in,
        query_pre,
        forget_pre,
        value_pre,
        gate_pre,
        floor_gap[None],
        head_gain[None],
        out_weight,
        norm_gain[None],
        value_weight,
        gate_weight,
        value_taps,
        gate_taps,
        down_weight,
    )


def local_recurrence(query_pre, forget_pre, value_pre, floor_gap):
    rows, width = query_pre.shape
    heads = width // DK
    subs = rows // SUB
    keys = floor_gap * jax.nn.sigmoid(-forget_pre.astype(f32))
    log_decay = jnp.log1p(-keys)
    query = jax.nn.silu(query_pre.astype(f32))
    values = value_pre.astype(f32)
    position = lax.iota(jnp.int32, rows)
    lower = (position[:, None] >= position[None, :]).astype(f32)
    running = jnp.dot(lower, log_decay, precision=highest)
    middle = running.reshape(subs, SUB, width)[:, SUB // 2 - 1, :]
    query_part = query * jnp.exp(running - jnp.repeat(middle, SUB, axis=0))
    reach = (lax.iota(jnp.int32, subs) + 1) * SUB
    seen = position[None, :, None] < reach[:, None, None]
    key_part = keys[None] * jnp.exp(
        jnp.where(seen, middle[:, None, :] - running[None], -jnp.inf)
    )
    scores = jnp.einsum(
        "ithk,ishk->hits",
        query_part.reshape(subs, SUB, heads, DK),
        key_part.reshape(subs, rows, heads, DK),
        precision=highest,
    ).reshape(heads, rows, rows)
    scores = jnp.where(position[None, :, None] >= position[None, None, :], scores, 0.0)
    value_heads = values.reshape(rows, heads, DK)
    inner = jnp.einsum("hts,shv->htv", scores, value_heads, precision=highest)
    ending = running[-1]
    state = jnp.einsum(
        "shv,shk->vhk",
        value_heads,
        (keys * jnp.exp(ending - running)).reshape(rows, heads, DK),
        precision=highest,
    ).reshape(DK, width)
    from_start = (query * jnp.exp(running)).reshape(rows, heads, DK)
    return inner, state, jnp.exp(ending), from_start


def causal_taps(before, current, taps):
    padded = jnp.concatenate([before, current], axis=1).astype(f32)
    rows = current.shape[1]
    return (
        taps[0] * padded[:, 0:rows]
        + taps[1] * padded[:, 1 : rows + 1]
        + taps[2] * padded[:, 2 : rows + 2]
    )


def on_device(
    residual_in,
    query_pre,
    forget_pre,
    value_pre,
    gate_pre,
    floor_gap,
    head_gain,
    out_weight,
    norm_gain,
    value_weight,
    gate_weight,
    value_taps,
    gate_taps,
    down_weight,
):
    sp = lax.axis_size("sp")
    tp = lax.axis_size("tp")
    inner_size = 4 if sp % 4 == 0 else 1
    outer = sp // inner_size
    me = lax.axis_index("sp")
    my_outer = me // inner_size
    my_inner = me % inner_size
    outer_groups = [[o * inner_size + i for o in range(outer)] for i in range(inner_size)]
    inner_groups = [[o * inner_size + i for i in range(inner_size)] for o in range(outer)]
    rows, my_width = residual_in.shape
    width = my_width * tp
    depth, half = value_weight.shape
    chunk = half // outer

    wide_groups = [
        [s * tp + t for s in group for t in range(tp)] for group in outer_groups
    ]

    def exchange(array):
        return lax.all_to_all(
            array, "sp", 0, 0, axis_index_groups=outer_groups, tiled=True
        )

    def gather_inner(array):
        return lax.all_gather(array, "sp", axis_index_groups=inner_groups)

    def gather_wide(array):
        gathered = lax.all_gather(array, ("sp", "tp"), axis_index_groups=wide_groups)
        gathered = gathered.reshape(outer, tp, *array.shape)
        return [gathered[:, t].reshape(-1, array.shape[1]) for t in range(tp)]

    def reorder(pieces):
        span = pieces[0].shape[-1]
        blocks = []
        for i in range(inner_size):
            for o in range(outer):
                start = (o * inner_size + i) * depth
                low = start % span
                blocks.append(pieces[start // span][..., low : low + depth])
        return lax.optimization_barrier(jnp.concatenate(blocks, axis=-1))

    up_parts = jnp.stack(
        [
            jnp.concatenate(
                [
                    value_weight[:, o * chunk : (o + 1) * chunk],
                    gate_weight[:, o * chunk : (o + 1) * chunk],
                ],
                axis=1,
            )
            for o in range(outer)
        ]
    )
    up_chunk = gather_inner(exchange(up_parts)).reshape(width, 2 * chunk)
    down_parts = down_weight.reshape(outer, chunk, depth)
    down_mine = gather_inner(exchange(down_parts))
    down_chunk = down_mine.transpose(2, 1, 0, 3).reshape(chunk, width)

    out_full = reorder(list(lax.all_gather(out_weight, "tp")))
    gain_full = reorder(list(lax.all_gather(norm_gain, "tp")))
    residual_group = reorder(gather_wide(residual_in))

    inner, state, total_decay, from_start = local_recurrence(
        query_pre, forget_pre, value_pre, floor_gap
    )
    heads = inner.shape[0]
    first = total_decay.astype(bf16)
    rest = total_decay - first.astype(f32)
    second = rest.astype(bf16)
    third = (rest - second.astype(f32)).astype(bf16)
    spare = jnp.zeros((13, heads * DK), bf16)
    packed = jnp.concatenate(
        [state.astype(bf16), first[None], second[None], third[None], spare], axis=0
    )
    everyone = lax.all_gather(packed, "sp").astype(f32)
    decays = everyone[:, DK] + everyone[:, DK + 1] + everyone[:, DK + 2]
    entering = jnp.zeros_like(state)
    for j in range(sp - 1):
        advanced = entering * decays[j] + everyone[j, :DK]
        entering = jnp.where(j < me, advanced, entering)
    carried = jnp.einsum(
        "thk,vhk->htv", from_start, entering.reshape(DK, heads, DK), precision=highest
    )
    recurrent = (inner + carried).transpose(1, 0, 2)
    scaled = (
        recurrent
        * lax.rsqrt(jnp.mean(recurrent * recurrent, axis=-1, keepdims=True) + epsilon)
        * head_gain
    )
    gating = jax.nn.silu(gate_pre.astype(f32)).reshape(recurrent.shape)
    head_out = (scaled * gating).reshape(rows, heads * DK).astype(bf16)

    head_out, out_full = lax.optimization_barrier((head_out, out_full))
    head_group = jnp.concatenate(gather_wide(head_out), axis=1)
    stream = residual_group.astype(f32) + jnp.dot(
        head_group, out_full, preferred_element_type=f32
    )
    squares = jnp.mean(stream * stream, axis=1, keepdims=True)
    normed = (stream * lax.rsqrt(squares + epsilon) * gain_full).astype(bf16)
    up = jnp.dot(normed, up_chunk, preferred_element_type=f32).astype(bf16)
    up = up.reshape(outer, rows, 2 * chunk)
    tails = up[:, rows - 2 :]
    pairs = [
        (o * inner_size + i, o * inner_size + (i + 1) % inner_size)
        for o in range(outer)
        for i in range(inner_size)
    ]
    arrived = lax.ppermute(tails, "sp", pairs) if inner_size > 1 else tails
    wrapped = jnp.concatenate([jnp.zeros_like(arrived[:1]), arrived[:-1]], axis=0)
    before = jnp.where(my_inner == 0, wrapped, arrived)

    taps = jnp.concatenate(
        [
            lax.dynamic_slice_in_dim(value_taps, my_outer * chunk, chunk, axis=1),
            lax.dynamic_slice_in_dim(gate_taps, my_outer * chunk, chunk, axis=1),
        ],
        axis=1,
    )
    conv = causal_taps(before, up, taps)
    hidden = (jax.nn.silu(conv[:, :, chunk:]) * conv[:, :, :chunk]).astype(bf16)
    terms = jnp.dot(
        hidden.reshape(outer * rows, chunk), down_chunk, preferred_element_type=f32
    ).astype(bf16)
    summed = lax.psum_scatter(
        terms, "sp", scatter_dimension=0, tiled=True, axis_index_groups=outer_groups
    )
    summed = lax.psum_scatter(summed, "tp", scatter_dimension=1, tiled=True)
    my_heads = lax.dynamic_slice_in_dim(head_group, my_outer * rows, rows, axis=0)
    own = residual_in.astype(f32) + jnp.dot(
        my_heads, out_weight, preferred_element_type=f32
    )
    return (own + summed.astype(f32)).astype(bf16)


def fits(mesh, residual_in, query_pre, *arrays):
    depth, half = arrays[7].shape
    extra = half // OUTER % LANES
    return (
        mesh.shape["sp"] == INNER * OUTER
        and mesh.shape["tp"] == 2
        and depth == LANES
        and residual_in.shape == (LANES, depth * INNER * OUTER // 2)
        and query_pre.shape[1] % LANES == 0
        and half % LANES == 0
        and extra in (0, LANES // 2)
    )


def solution(mesh):
    rows = P(("grp", "sp"), "tp")

    def layer(*arrays):
        return (fused_layer if fits(mesh, *arrays) else on_device)(*arrays)

    return jax.shard_map(
        layer,
        mesh=mesh,
        in_specs=(
            rows,
            rows,
            rows,
            rows,
            rows,
            P("tp"),
            P(),
            P(None, "tp"),
            P("tp"),
            P("sp", "tp"),
            P("sp", "tp"),
            P(None, "tp"),
            P(None, "tp"),
            P("tp", "sp"),
        ),
        out_specs=rows,
        check_vma=False,
    )
```

```python
import functools

import jax
import jax.numpy as jnp
from jax import lax
from jax.experimental import pallas as pl
from jax.experimental.pallas import tpu as pltpu
from jax.sharding import PartitionSpec as P

DK = 64
SUB = 16
LANES = 128
INNER = 4
OUTER = 4
epsilon = 1e-06
highest = lax.Precision.HIGHEST
f32 = jnp.float32
bf16 = jnp.bfloat16
MESH = pl.DeviceIdType.MESH


def dot_nt(a, b):
    return lax.dot_general(
        a, b, (((1,), (1,)), ((), ())), precision=highest, preferred_element_type=f32
    )


def dot_hi(a, b):
    return jnp.dot(a, b, precision=highest, preferred_element_type=f32)


def gate(v):
    return v / (1.0 + jnp.exp(-v))


def turn(v):
    return jnp.concatenate([v[:, DK:], v[:, :DK]], axis=1)


def layer_kernel(
    full,
    extra,
    residual_ref,
    query_ref,
    forget_ref,
    value_ref,
    gate_ref,
    floor_ref,
    head_gain_ref,
    out_weight_ref,
    norm_gain_ref,
    value_weight_ref,
    gate_weight_ref,
    value_taps_ref,
    gate_taps_ref,
    down_ref,
    out_ref,
    up_in,
    dn_in,
    taps,
    up,
    dn,
    st,
    zt,
    inner_buf,
    start_buf,
    ho,
    sq,
    stream,
    nb,
    ubuf,
    tail_s,
    tail_r,
    hid,
    xs,
    xr,
    zs,
    zr,
    zbs,
    zbr,
    xbs,
    xbr,
    ssem,
    up_r,
    dn_r,
    st_r,
    zt_r,
    zt_s,
    go,
    nb_r,
    xr_r,
    zr_r,
    zb_r,
    misc_r,
):
    s = lax.axis_index("sp")
    x = lax.axis_index("tp")
    z = s // INNER
    i = s % INNER
    c = s % 2
    ox = 1 - x
    ic = i + 1 - 2 * c
    iy = (i + 2) % INNER
    idg = (ic + 2) % INNER
    z1 = z + 1 - 2 * (z % 2)
    z2 = (z + 2) % OUTER
    z3 = OUTER - 1 - z
    chunk = full + extra
    depth = up.shape[1]
    rows = query_ref.shape[0]
    width = query_ref.shape[1]
    pairs = width // LANES
    pending = []

    def at(zz, ii, xx=x):
        return {"sp": zz * INNER + ii, "tp": xx}

    def send(src, dst, rsem, device, first=None):
        copy = pltpu.make_async_remote_copy(
            src_ref=src,
            dst_ref=dst,
            send_sem=ssem.at[len(pending)],
            recv_sem=rsem,
            device_id=device,
            device_id_type=MESH,
        )
        pending.append(copy)
        if first is None:
            copy.start()
        elif first is not False:
            pl.when(first)(copy.start)
        return copy

    def arrived(dst, rsem):
        pltpu.make_async_remote_copy(
            src_ref=dst,
            dst_ref=dst,
            send_sem=ssem.at[0],
            recv_sem=rsem,
            device_id=at(z, ic),
            device_id_type=MESH,
        ).wait_recv()

    barrier = pltpu.get_barrier_semaphore()
    peers = [at((z + k) % OUTER, i) for k in range(1, OUTER)]
    peers += [at(z, ic), at(z, iy), at(z, idg), at(z, i, ox)]
    for peer in peers:
        pl.semaphore_signal(barrier, inc=1, device_id=peer, device_id_type=MESH)

    def up_slot(zz, ii):
        return up.at[zz * INNER + ii], up_r.at[zz * INNER + ii]

    def dn_slot(zz, ii):
        slot = dn.at[zz * INNER + ii, pl.ds(0, chunk)]
        return slot, dn_r.at[zz * INNER + ii]

    def send_z(source, slot, zz, first=None):
        dst, sem = slot(z, i)
        return send(source.at[zz], dst, sem, at(zz, i), first)

    def forward_yc(slot, zz, source=None):
        dst, sem = slot(zz, i)
        if source is None:
            arrived(dst, sem)
            source = dst
        send(source, dst, sem, at(z, iy))
        send(source, dst, sem, at(z, ic))

    def send_half(part, first):
        dst, sem = up_slot(z, i)
        part_rows = pl.ds(part * (depth // 2), depth // 2)
        src = up_in.at[z3, part_rows]
        return send(src, dst.at[part_rows], sem, at(z3, i), first)

    def prepare_yc(slot, zz):
        dst, sem = slot(zz, i)
        copies = [send(dst, dst, sem, at(z, ii), False) for ii in (iy, ic)]

        def run():
            arrived(dst, sem)
            for copy in copies:
                copy.start()

        return run

    def forward_c(slot, zz):
        dst, sem = slot(zz, iy)
        arrived(dst, sem)
        send(dst, dst, sem, at(z, ic))

    keys = floor_ref[...] * jax.nn.sigmoid(-forget_ref[...].astype(f32))
    query = gate(query_ref[...].astype(f32))
    values = value_ref[...].astype(f32)
    position = lax.broadcasted_iota(jnp.int32, (rows, rows), 0)
    earlier = lax.broadcasted_iota(jnp.int32, (rows, rows), 1)
    running = dot_hi((position >= earlier).astype(f32), jnp.log1p(-keys))
    ending = running[rows - 1 : rows]
    kept = keys * jnp.exp(ending - running)
    turned = values.T
    low = lax.broadcasted_iota(jnp.int32, (1, LANES), 1) < DK
    part_row = lax.broadcasted_iota(jnp.int32, (SUB, width), 0)

    def store_state(ref, state, decay):
        ref[0:DK] = state.astype(bf16)
        one = decay.astype(bf16).astype(f32)
        two = (decay - one).astype(bf16).astype(f32)
        three = decay - one - two
        parts = jnp.where(part_row == 1, two, jnp.where(part_row == 2, three, 0.0))
        ref[DK : DK + SUB] = jnp.where(part_row == 0, one, parts).astype(bf16)

    def load_state(ref):
        parts = ref[DK : DK + SUB].astype(f32)
        return ref[0:DK].astype(f32), parts[0:1] + parts[1:2] + parts[2:3]

    states = []
    for p in range(pairs):
        lanes = slice(p * LANES, (p + 1) * LANES)
        both = dot_hi(turned[lanes], kept[:, lanes])
        states.append(jnp.where(low, both[:DK], both[DK:]))
    store_state(st.at[i], jnp.concatenate(states, axis=1), jnp.exp(ending))
    for o in range(OUTER):
        main = slice(o * full, (o + 1) * full)
        up_in[o, :, 0:full] = value_weight_ref[:, main]
        up_in[o, :, full : 2 * full] = gate_weight_ref[:, main]
        dn_in[o, 0:full] = down_ref[main]
        if extra:
            start = OUTER * full + o * extra
            dn_in[o, full:chunk] = down_ref[start : start + extra]
    if extra:
        for o in range(0, OUTER, 2):
            start = OUTER * full + o * extra
            tile = slice(start, start + LANES)
            v = value_weight_ref[:, tile].astype(f32)
            g = gate_weight_ref[:, tile].astype(f32)
            end = slice(2 * full, 2 * full + LANES)
            up_in[o, :, end] = jnp.where(low, v, turn(g)).astype(bf16)
            up_in[o + 1, :, end] = jnp.where(low, turn(v), g).astype(bf16)

    pl.semaphore_wait(barrier, len(peers))
    for ii in (idg, iy, ic):
        send(st.at[i], st.at[i], st_r.at[i], at(z, ii))
    far = send_z(up_in, up_slot, z2, z == 3)
    near = send_z(up_in, up_slot, z1, z % 2 == 1)
    cross = send_half(0, z == 0)
    near_dn = send_z(dn_in, dn_slot, z1, z == 0)

    up[s] = up_in[z]
    dn[s, 0:chunk] = dn_in[z]
    spare = dn.shape[1] - chunk
    if spare:
        for b in range(INNER * OUTER):
            dn[b, chunk:] = jnp.zeros((spare, dn.shape[2]), bf16)
    start_buf[...] = query * jnp.exp(running)

    for ii in (ic, iy, idg):
        arrived(st.at[ii], st_r.at[ii])
    total = jnp.zeros((DK, width), f32)
    mine = jnp.zeros((DK, width), f32)
    total_decay = jnp.ones((1, width), f32)
    my_decay = jnp.ones((1, width), f32)
    for j in range(INNER):
        fresh, decay = load_state(st.at[j])
        mine = jnp.where(j < i, mine * decay + fresh, mine)
        my_decay = jnp.where(j < i, my_decay * decay, my_decay)
        total = total * decay + fresh
        total_decay = total_decay * decay
    store_state(zt.at[z], total, total_decay)
    totals = []
    for k in range(1, OUTER):
        totals.append(
            pltpu.make_async_remote_copy(
                src_ref=zt.at[z],
                dst_ref=zt.at[z],
                send_sem=zt_s.at[k],
                recv_sem=zt_r.at[z],
                device_id=at((z + k) % OUTER, i),
                device_id_type=MESH,
            )
        )
    for k in (3, 2, 1):
        pl.when(z + k < OUTER)(totals[k - 1].start)
    pl.when(z == 2)(near_dn.start)
    pl.when(z == 2)(near.start)
    forward_yc(up_slot, z, up_in.at[z])
    forward_yc(dn_slot, z, dn_in.at[z])

    cells = [[] for _ in range(pairs)]
    row_of = lax.broadcasted_iota(jnp.int32, (rows, width), 0)
    column = lax.broadcasted_iota(jnp.int32, (2 * SUB, rows), 1)
    stacked = lax.broadcasted_iota(jnp.int32, (2 * SUB, rows), 0) % SUB
    for n in range(rows // SUB):
        part = slice(n * SUB, (n + 1) * SUB)
        middle = running[n * SUB + SUB // 2 - 1 : n * SUB + SUB // 2]
        query_part = query[part] * jnp.exp(running[part] - middle)
        reach = jnp.where(row_of < (n + 1) * SUB, middle - running, -jnp.inf)
        key_part = keys * jnp.exp(reach)
        for p in range(pairs):
            lanes = slice(p * LANES, (p + 1) * LANES)
            piece = query_part[:, lanes]
            piece = jnp.concatenate(
                [jnp.where(low, piece, 0.0), jnp.where(low, 0.0, piece)], axis=0
            )
            score = dot_nt(piece, key_part[:, lanes])
            score = jnp.where(stacked + n * SUB >= column, score, 0.0)
            cells[p].append(score)
    for p in range(pairs):
        lanes = slice(p * LANES, (p + 1) * LANES)
        scores = jnp.concatenate(
            [cell[:SUB] for cell in cells[p]] + [cell[SUB:] for cell in cells[p]],
            axis=0,
        )
        result = dot_hi(scores, values[:, lanes])
        inner_buf[:, lanes] = jnp.where(low, result[:rows], result[rows:])

    for k, copy in enumerate(totals, 1):
        pl.when(z + k < OUTER)(copy.wait_send)

    @pl.when(z == 1)
    def _():
        pl.semaphore_signal(go, inc=1, device_id=at(z1, i), device_id_type=MESH)

    pl.when(z == 2)(far.start)
    gain = jnp.concatenate([head_gain_ref[...]] * (LANES // DK), axis=1)
    gating = gate(gate_ref[...].astype(f32))
    for k in range(1, OUTER):
        zz = (z + OUTER - k) % OUTER
        pl.when(z >= k)(functools.partial(arrived, zt.at[zz], zt_r.at[zz]))
    entering = jnp.zeros((DK, width), f32)
    for j in range(OUTER - 1):
        fresh, decay = load_state(zt.at[j])
        entering = jnp.where(j < z, entering * decay + fresh, entering)
    entering = entering * my_decay + mine
    same_head = (
        lax.broadcasted_iota(jnp.int32, (LANES, LANES), 0) // DK
        == lax.broadcasted_iota(jnp.int32, (LANES, LANES), 1) // DK
    ).astype(f32)
    for p in range(pairs):
        lanes = slice(p * LANES, (p + 1) * LANES)
        piece = entering[:, lanes]
        piece = jnp.concatenate(
            [jnp.where(low, piece, 0.0), jnp.where(low, 0.0, piece)], axis=0
        )
        recurrent = inner_buf[:, lanes] + dot_nt(start_buf[:, lanes], piece)
        squares = dot_hi(recurrent * recurrent, same_head) * (1.0 / DK)
        scaled = recurrent * lax.rsqrt(squares + epsilon) * gain
        ho[x, :, lanes] = (scaled * gating[:, lanes]).astype(bf16)
    send(ho.at[x], ho.at[x], misc_r.at[0], at(z, i, ox))

    @pl.when(z == 0)
    def _():
        pl.semaphore_wait(go, 1)
        far.start()


    arrived(ho.at[ox], misc_r.at[0])
    pl.when(z == 1)(far.start)
    heads = jnp.concatenate([ho[0], ho[1]], axis=1)
    stream[...] = residual_ref[...].astype(f32) + jnp.dot(
        heads, out_weight_ref[...], preferred_element_type=f32
    )
    partial = jnp.sum(stream[...] * stream[...], axis=1, keepdims=True)
    sq[x] = jnp.broadcast_to(partial, (rows, LANES))
    send(sq.at[x], sq.at[x], misc_r.at[1], at(z, i, ox))
    arrived(sq.at[ox], misc_r.at[1])
    channels = 2 * stream.shape[1]
    mean = (sq[0][:, 0:1] + sq[1][:, 0:1]) * (1.0 / channels)
    normed = stream[...] * lax.rsqrt(mean + epsilon) * norm_gain_ref[...]
    nb[z, x] = normed.astype(bf16)

    def nb_slot(zz, xx):
        return nb.at[zz, xx], nb_r.at[zz * 2 + xx]

    def share(zz, devices, first=None):
        dst, sem = nb_slot(zz, x)
        return [send(dst, dst, sem, device, first) for device in devices]

    share(z, [at(z2, i), at(z1, i), at(z, i, ox)])
    pl.when(z == 0)(near.start)
    pl.when(z > 0)(cross.start)
    cross_rest = send_half(1, z > 0)
    last_dn = send_z(dn_in, dn_slot, z3, False)
    pl.when(z % 2 == 1)(near_dn.start)
    forward_c(up_slot, z)
    forward_c(dn_slot, z)
    early_dn = prepare_yc(dn_slot, z1)
    pl.when(z % 2 == 1)(early_dn)
    forward_yc(up_slot, z2)

    pl.when(z == 1)(functools.partial(arrived, *nb_slot(z2, x)))
    passed = share(z2, [at(z1, i), at(z, i, ox)], z == 1)
    arrived(*nb_slot(z1, x))
    share(z1, [at(z, i, ox)])

    @pl.when(z != 1)
    def _():
        arrived(*nb_slot(z2, x))
        for copy in passed:
            copy.start()

    forward_yc(up_slot, z1)
    forward_c(up_slot, z2)
    arrived(*nb_slot(z3, x))
    share(z3, [at(z, i, ox)])
    pl.when(z == 0)(cross_rest.start)
    far_dn = send_z(dn_in, dn_slot, z2, z == 3)
    pl.when(z == 3)(last_dn.start)
    forward_c(up_slot, z1)
    forward_yc(up_slot, z3)
    pl.when(z < 3)(far_dn.start)
    pl.when(z % 2 == 0)(early_dn)
    later_dn = prepare_yc(dn_slot, z2)
    forward_c(up_slot, z3)
    pl.when(z < 3)(last_dn.start)
    pl.when(z % 3 == 0)(later_dn)

    for zz in range(OUTER):
        arrived(*up_slot(zz, ic))
        arrived(*up_slot(zz, idg))
        arrived(*nb_slot(zz, ox))

    mine_at = pl.ds(pl.multiple_of(z * full, LANES), full)
    taps[:, 0:full] = value_taps_ref[:, mine_at]
    taps[:, full : 2 * full] = gate_taps_ref[:, mine_at]
    if extra:
        tile = pl.ds(pl.multiple_of(OUTER * full + z // 2 * LANES, LANES), LANES)
        v = value_taps_ref[:, tile]
        g = gate_taps_ref[:, tile]
        v = jnp.where(z % 2 == 0, v, turn(v))
        g = jnp.where(z % 2 == 0, turn(g), g)
        taps[:, 2 * full : 2 * full + LANES] = jnp.where(low, v, g)

    count = OUTER * rows
    half = nb.shape[3]
    deep = half // up.shape[1]
    first = nb[:, 0].reshape(count, half)
    second = nb[:, 1].reshape(count, half)
    span = up.shape[2]
    step = 2 * LANES
    for low_lane in range(0, span, step):
        lanes = slice(low_lane, min(span, low_lane + step))
        size = lanes.stop - lanes.start
        product = jnp.dot(
            first, up[0:deep, :, lanes].reshape(half, size), preferred_element_type=f32
        ) + jnp.dot(
            second,
            up[deep : 2 * deep, :, lanes].reshape(half, size),
            preferred_element_type=f32,
        )
        ubuf[:, 8:, lanes] = (
            product.astype(bf16).astype(f32).reshape(OUTER, rows, size)
        )
    for b in range(OUTER):
        tail_s[2 * b : 2 * b + 2] = ubuf[b, rows + 6 : rows + 8]
    after = z * INNER + (i + 1) % INNER
    send(tail_s, tail_r, misc_r.at[2], {"sp": after, "tp": x})

    forward_c(dn_slot, z1)
    pl.when(z % 3 != 0)(later_dn)
    forward_yc(dn_slot, z3)

    arrived(tail_r, misc_r.at[2])
    for b in range(OUTER):
        wrapped = tail_r[2 * b - 2 : 2 * b] if b else jnp.zeros((2, span), f32)
        ubuf[b, 6:8] = jnp.where(i == 0, wrapped, tail_r[2 * b : 2 * b + 2])

    def conv(b, lanes):
        return (
            taps[0:1, lanes] * ubuf[b, pl.ds(6, rows), lanes]
            + taps[1:2, lanes] * ubuf[b, pl.ds(7, rows), lanes]
            + taps[2:3, lanes] * ubuf[b, pl.ds(8, rows), lanes]
        )

    @pl.loop(0, OUTER)
    def _(b):
        for t in range(full // LANES):
            lanes = slice(t * LANES, (t + 1) * LANES)
            other = slice(full + t * LANES, full + (t + 1) * LANES)
            hid[b, :, lanes] = (gate(conv(b, other)) * conv(b, lanes)).astype(bf16)
        if extra:
            mixed = conv(b, slice(2 * full, 2 * full + LANES))
            turned_half = turn(mixed)
            last = jnp.where(low, gate(turned_half) * mixed, 0.0)
            hid[b, :, full : full + LANES] = last.astype(bf16)

    forward_c(dn_slot, z2)
    forward_c(dn_slot, z3)
    for zz in range(OUTER):
        arrived(*dn_slot(zz, ic))
        arrived(*dn_slot(zz, idg))

    tiles = half // step
    keep = tiles - 1
    phase = len(pending)

    def tile(j):
        return slice(j * step, (j + 1) * step)

    def product(zz, base, j):
        weight = jnp.concatenate([dn[base + 2 * j], dn[base + 2 * j + 1]], axis=1)
        return jnp.dot(hid[zz], weight, preferred_element_type=f32)

    def both(zz):
        sides = [product(zz, side * deep, keep) for side in (x, ox)]
        return jnp.concatenate(sides, axis=1)

    def send_both(slot, value, device):
        zbs[slot] = value.astype(bf16)
        send(zbs.at[slot], zbr.at[slot], zb_r.at[slot], device)

    def got_both(slot):
        arrived(zbr.at[slot], zb_r.at[slot])
        return zbr[slot].astype(f32)

    def send_tile(src, dst, sem, slot, j, device):
        lanes = tile(j)
        send(src.at[slot, :, lanes], dst.at[slot, :, lanes], sem.at[slot, j], device)

    send_both(0, both(z3), at(z1, i))
    send_both(1, both(z1), at(z1, i))
    order = [(zz, j) for j in range(keep) for zz in (z3, z2)]
    order += [(zz, j) for zz in (z1, z) for j in range(keep)]
    for zz, j in order:
        xs[zz, :, tile(j)] = product(zz, ox * deep, j).astype(bf16)
        send_tile(xs, xr, xr_r, zz, j, at(z, i, ox))
    for copy in pending[:phase]:
        copy.wait_send()

    def summed(zz, j):
        value = product(zz, x * deep, j)
        arrived(xr.at[zz, :, tile(j)], xr_r.at[zz, j])
        return value + xr[zz, :, tile(j)].astype(f32)

    def received(slot, j):
        arrived(zr.at[slot, :, tile(j)], zr_r.at[slot, j])
        return zr[slot, :, tile(j)].astype(f32)

    def pass_on(slot, j, value, device):
        zs[slot, :, tile(j)] = value.astype(bf16)
        send_tile(zs, zr, zr_r, slot, j, device)

    pass_on(0, 0, summed(z3, 0), at(z1, i))
    for j in range(1, keep):
        pass_on(0, j, summed(z3, j), at(z1, i))
    send_both(2, both(z2) + got_both(0), at(z2, i))
    for j in range(keep):
        value = summed(z2, j)
        pass_on(2, j, value + received(0, j), at(z2, i))
    for j in range(keep):
        pass_on(1, j, summed(z1, j), at(z1, i))
    pair = both(z) + got_both(1)
    pair = pair + got_both(2)
    xbs[...] = pair[:, step:].astype(bf16)
    send(xbs, xbr, zb_r.at[3], at(z, i, ox))
    for j in range(keep):
        own = summed(z, j) + received(1, j) + received(2, j)
        out_ref[:, tile(j)] = (stream[:, tile(j)] + own).astype(bf16)
    arrived(xbr, zb_r.at[3])
    own = pair[:, :step] + xbr[...].astype(f32)
    out_ref[:, tile(keep)] = (stream[:, tile(keep)] + own).astype(bf16)

    for copy in pending[phase:]:
        copy.wait_send()


def fused_layer(
    residual_in,
    query_pre,
    forget_pre,
    value_pre,
    gate_pre,
    floor_gap,
    head_gain,
    out_weight,
    norm_gain,
    value_weight,
    gate_weight,
    value_taps,
    gate_taps,
    down_weight,
):
    rows, my_width = residual_in.shape
    depth, half = value_weight.shape
    width = query_pre.shape[1]
    blocks = INNER * OUTER
    full = half // LANES // OUTER * LANES
    extra = half // OUTER - full
    chunk = full + extra
    padded = full + (LANES if extra else 0)

    dma = pltpu.SemaphoreType.DMA
    vmem = pl.BlockSpec(memory_space=pltpu.VMEM)
    span = 2 * chunk
    return pl.pallas_call(
        functools.partial(layer_kernel, full, extra),
        out_shape=pltpu.VMEM((rows, my_width), bf16),
        in_specs=[vmem] * 14,
        out_specs=vmem,
        scratch_shapes=[
            pltpu.VMEM((OUTER, depth, span), bf16),
            pltpu.VMEM((OUTER, chunk, depth), bf16),
            pltpu.VMEM((value_taps.shape[0], span), f32),
            pltpu.VMEM((blocks, depth, span), bf16),
            pltpu.VMEM((blocks, padded, depth), bf16),
            pltpu.VMEM((INNER, DK + SUB, width), bf16),
            pltpu.VMEM((OUTER, DK + SUB, width), bf16),
            pltpu.VMEM((rows, width), f32),
            pltpu.VMEM((rows, width), f32),
            pltpu.VMEM((2, rows, width), bf16),
            pltpu.VMEM((2, rows, LANES), f32),
            pltpu.VMEM((rows, my_width), f32),
            pltpu.VMEM((OUTER, 2, rows, my_width), bf16),
            pltpu.VMEM((OUTER, rows + 8, span), f32),
            pltpu.VMEM((2 * OUTER, span), f32),
            pltpu.VMEM((2 * OUTER, span), f32),
            pltpu.VMEM((OUTER, rows, padded), bf16),
            pltpu.VMEM((OUTER, rows, my_width), bf16),
            pltpu.VMEM((OUTER, rows, my_width), bf16),
            pltpu.VMEM((3, rows, my_width), bf16),
            pltpu.VMEM((3, rows, my_width), bf16),
            pltpu.VMEM((3, rows, 4 * LANES), bf16),
            pltpu.VMEM((3, rows, 4 * LANES), bf16),
            pltpu.VMEM((rows, 2 * LANES), bf16),
            pltpu.VMEM((rows, 2 * LANES), bf16),
            dma((96,)),
            dma((blocks,)),
            dma((blocks,)),
            dma((INNER,)),
            dma((OUTER,)),
            dma((OUTER,)),
            pltpu.SemaphoreType.REGULAR,
            dma((2 * OUTER,)),
            dma((OUTER, 4)),
            dma((3, 4)),
            dma((4,)),
            dma((3,)),
        ],
        compiler_params=pltpu.CompilerParams(
            collective_id=0, has_side_effects=True, vmem_limit_bytes=56 * 2**20
        ),
        name="layer",
    )(
        residual_in,
        query_pre,
        forget_pre,
        value_pre,
        gate_pre,
        floor_gap[None],
        head_gain[None],
        out_weight,
        norm_gain[None],
        value_weight,
        gate_weight,
        value_taps,
        gate_taps,
        down_weight,
    )


def local_recurrence(query_pre, forget_pre, value_pre, floor_gap):
    rows, width = query_pre.shape
    heads = width // DK
    subs = rows // SUB
    keys = floor_gap * jax.nn.sigmoid(-forget_pre.astype(f32))
    log_decay = jnp.log1p(-keys)
    query = jax.nn.silu(query_pre.astype(f32))
    values = value_pre.astype(f32)
    position = lax.iota(jnp.int32, rows)
    lower = (position[:, None] >= position[None, :]).astype(f32)
    running = jnp.dot(lower, log_decay, precision=highest)
    middle = running.reshape(subs, SUB, width)[:, SUB // 2 - 1, :]
    query_part = query * jnp.exp(running - jnp.repeat(middle, SUB, axis=0))
    reach = (lax.iota(jnp.int32, subs) + 1) * SUB
    seen = position[None, :, None] < reach[:, None, None]
    key_part = keys[None] * jnp.exp(
        jnp.where(seen, middle[:, None, :] - running[None], -jnp.inf)
    )
    scores = jnp.einsum(
        "ithk,ishk->hits",
        query_part.reshape(subs, SUB, heads, DK),
        key_part.reshape(subs, rows, heads, DK),
        precision=highest,
    ).reshape(heads, rows, rows)
    scores = jnp.where(position[None, :, None] >= position[None, None, :], scores, 0.0)
    value_heads = values.reshape(rows, heads, DK)
    inner = jnp.einsum("hts,shv->htv", scores, value_heads, precision=highest)
    ending = running[-1]
    state = jnp.einsum(
        "shv,shk->vhk",
        value_heads,
        (keys * jnp.exp(ending - running)).reshape(rows, heads, DK),
        precision=highest,
    ).reshape(DK, width)
    from_start = (query * jnp.exp(running)).reshape(rows, heads, DK)
    return inner, state, jnp.exp(ending), from_start


def causal_taps(before, current, taps):
    padded = jnp.concatenate([before, current], axis=1).astype(f32)
    rows = current.shape[1]
    return (
        taps[0] * padded[:, 0:rows]
        + taps[1] * padded[:, 1 : rows + 1]
        + taps[2] * padded[:, 2 : rows + 2]
    )


def on_device(
    residual_in,
    query_pre,
    forget_pre,
    value_pre,
    gate_pre,
    floor_gap,
    head_gain,
    out_weight,
    norm_gain,
    value_weight,
    gate_weight,
    value_taps,
    gate_taps,
    down_weight,
):
    sp = lax.axis_size("sp")
    tp = lax.axis_size("tp")
    inner_size = 4 if sp % 4 == 0 else 1
    outer = sp // inner_size
    me = lax.axis_index("sp")
    my_outer = me // inner_size
    my_inner = me % inner_size
    outer_groups = [[o * inner_size + i for o in range(outer)] for i in range(inner_size)]
    inner_groups = [[o * inner_size + i for i in range(inner_size)] for o in range(outer)]
    rows, my_width = residual_in.shape
    width = my_width * tp
    depth, half = value_weight.shape
    chunk = half // outer

    wide_groups = [
        [s * tp + t for s in group for t in range(tp)] for group in outer_groups
    ]

    def exchange(array):
        return lax.all_to_all(
            array, "sp", 0, 0, axis_index_groups=outer_groups, tiled=True
        )

    def gather_inner(array):
        return lax.all_gather(array, "sp", axis_index_groups=inner_groups)

    def gather_wide(array):
        gathered = lax.all_gather(array, ("sp", "tp"), axis_index_groups=wide_groups)
        gathered = gathered.reshape(outer, tp, *array.shape)
        return [gathered[:, t].reshape(-1, array.shape[1]) for t in range(tp)]

    def reorder(pieces):
        span = pieces[0].shape[-1]
        blocks = []
        for i in range(inner_size):
            for o in range(outer):
                start = (o * inner_size + i) * depth
                low = start % span
                blocks.append(pieces[start // span][..., low : low + depth])
        return lax.optimization_barrier(jnp.concatenate(blocks, axis=-1))

    up_parts = jnp.stack(
        [
            jnp.concatenate(
                [
                    value_weight[:, o * chunk : (o + 1) * chunk],
                    gate_weight[:, o * chunk : (o + 1) * chunk],
                ],
                axis=1,
            )
            for o in range(outer)
        ]
    )
    up_chunk = gather_inner(exchange(up_parts)).reshape(width, 2 * chunk)
    down_parts = down_weight.reshape(outer, chunk, depth)
    down_mine = gather_inner(exchange(down_parts))
    down_chunk = down_mine.transpose(2, 1, 0, 3).reshape(chunk, width)

    out_full = reorder(list(lax.all_gather(out_weight, "tp")))
    gain_full = reorder(list(lax.all_gather(norm_gain, "tp")))
    residual_group = reorder(gather_wide(residual_in))

    inner, state, total_decay, from_start = local_recurrence(
        query_pre, forget_pre, value_pre, floor_gap
    )
    heads = inner.shape[0]
    first = total_decay.astype(bf16)
    rest = total_decay - first.astype(f32)
    second = rest.astype(bf16)
    third = (rest - second.astype(f32)).astype(bf16)
    spare = jnp.zeros((13, heads * DK), bf16)
    packed = jnp.concatenate(
        [state.astype(bf16), first[None], second[None], third[None], spare], axis=0
    )
    everyone = lax.all_gather(packed, "sp").astype(f32)
    decays = everyone[:, DK] + everyone[:, DK + 1] + everyone[:, DK + 2]
    entering = jnp.zeros_like(state)
    for j in range(sp - 1):
        advanced = entering * decays[j] + everyone[j, :DK]
        entering = jnp.where(j < me, advanced, entering)
    carried = jnp.einsum(
        "thk,vhk->htv", from_start, entering.reshape(DK, heads, DK), precision=highest
    )
    recurrent = (inner + carried).transpose(1, 0, 2)
    scaled = (
        recurrent
        * lax.rsqrt(jnp.mean(recurrent * recurrent, axis=-1, keepdims=True) + epsilon)
        * head_gain
    )
    gating = jax.nn.silu(gate_pre.astype(f32)).reshape(recurrent.shape)
    head_out = (scaled * gating).reshape(rows, heads * DK).astype(bf16)

    head_out, out_full = lax.optimization_barrier((head_out, out_full))
    head_group = jnp.concatenate(gather_wide(head_out), axis=1)
    stream = residual_group.astype(f32) + jnp.dot(
        head_group, out_full, preferred_element_type=f32
    )
    squares = jnp.mean(stream * stream, axis=1, keepdims=True)
    normed = (stream * lax.rsqrt(squares + epsilon) * gain_full).astype(bf16)
    up = jnp.dot(normed, up_chunk, preferred_element_type=f32).astype(bf16)
    up = up.reshape(outer, rows, 2 * chunk)
    tails = up[:, rows - 2 :]
    pairs = [
        (o * inner_size + i, o * inner_size + (i + 1) % inner_size)
        for o in range(outer)
        for i in range(inner_size)
    ]
    arrived = lax.ppermute(tails, "sp", pairs) if inner_size > 1 else tails
    wrapped = jnp.concatenate([jnp.zeros_like(arrived[:1]), arrived[:-1]], axis=0)
    before = jnp.where(my_inner == 0, wrapped, arrived)

    taps = jnp.concatenate(
        [
            lax.dynamic_slice_in_dim(value_taps, my_outer * chunk, chunk, axis=1),
            lax.dynamic_slice_in_dim(gate_taps, my_outer * chunk, chunk, axis=1),
        ],
        axis=1,
    )
    conv = causal_taps(before, up, taps)
    hidden = (jax.nn.silu(conv[:, :, chunk:]) * conv[:, :, :chunk]).astype(bf16)
    terms = jnp.dot(
        hidden.reshape(outer * rows, chunk), down_chunk, preferred_element_type=f32
    ).astype(bf16)
    summed = lax.psum_scatter(
        terms, "sp", scatter_dimension=0, tiled=True, axis_index_groups=outer_groups
    )
    summed = lax.psum_scatter(summed, "tp", scatter_dimension=1, tiled=True)
    my_heads = lax.dynamic_slice_in_dim(head_group, my_outer * rows, rows, axis=0)
    own = residual_in.astype(f32) + jnp.dot(
        my_heads, out_weight, preferred_element_type=f32
    )
    return (own + summed.astype(f32)).astype(bf16)


def fits(mesh, residual_in, query_pre, *arrays):
    depth, half = arrays[7].shape
    extra = half // OUTER % LANES
    return (
        mesh.shape["sp"] == INNER * OUTER
        and mesh.shape["tp"] == 2
        and depth == LANES
        and residual_in.shape == (LANES, depth * INNER * OUTER // 2)
        and query_pre.shape[1] % LANES == 0
        and half % LANES == 0
        and extra in (0, LANES // 2)
    )


def solution(mesh):
    rows = P(("grp", "sp"), "tp")

    def layer(*arrays):
        return (fused_layer if fits(mesh, *arrays) else on_device)(*arrays)

    return jax.shard_map(
        layer,
        mesh=mesh,
        in_specs=(
            rows,
            rows,
            rows,
            rows,
            rows,
            P("tp"),
            P(),
            P(None, "tp"),
            P("tp"),
            P("sp", "tp"),
            P("sp", "tp"),
            P(None, "tp"),
            P(None, "tp"),
            P("tp", "sp"),
        ),
        out_specs=rows,
        check_vma=False,
    )
```
